32 devices in a mesh: kv: 8 (over y, x, core), tp: 4 (over z).
Axes of the slice: x: 2, y: 2, z: 4, core: 2. Of those that a mesh axis runs over, the one named last changes fastest.
Arguments:
- tokens: bfloat16 [64, 4, 4096], P(None, None, ('kv', 'tp')), may hold values from -36 to 36
- lengths: int32 [64], replicated, may hold values from 1 to 4, 112 in all
- state: float32 [64, 128, 4096], P('kv', None, 'tp'), may hold values from -0.6 to 0.6
- attn_gain: float32 [4096], P('kv'), may hold values from 0.1 to 1.9
- w_query: bfloat16 [4096, 4096], P('kv', 'tp'), may hold values from -0.09375 to 0.09375
- w_key: bfloat16 [4096, 4096], P('kv', 'tp'), may hold values from -0.09375 to 0.09375
- w_value: bfloat16 [4096, 4096], P('kv', 'tp'), may hold values from -0.09375 to 0.09375
- w_beta: bfloat16 [4096, 32], replicated, may hold values from -0.09375 to 0.09375
- w_alpha: bfloat16 [4096, 32], replicated, may hold values from -0.09375 to 0.09375
- decay_rate: float32 [32], replicated, may hold values from 0.05 to 3
- decay_bias: float32 [32], replicated, may hold values from -3 to 3
- out_gain: float32 [128], replicated, may hold values from 0.1 to 1.9
- w_out: bfloat16 [4096, 4096], P('tp', 'kv'), may hold values from -0.09375 to 0.09375
- mix_gain: float32 [4096], P('kv'), may hold values from 0.1 to 1.9
- w_gate: bfloat16 [4096, 11008], P('kv', 'tp'), may hold values from -0.09375 to 0.09375
- w_up: bfloat16 [4096, 11008], P('kv', 'tp'), may hold values from -0.09375 to 0.09375
- w_down: bfloat16 [11008, 4096], P('tp', 'kv'), may hold values from -0.0546875 to 0.0546875
Outputs:
- mixed: bfloat16 [64, 4, 4096], P(None, None, ('kv', 'tp'))
- new_state: float32 [64, 128, 4096], P('kv', None, 'tp')
The draws below stay inside these ranges and needn't reach their ends.
Inputs may be any that keep to these rules, and one draw needn't show every extreme that they name: Each sequence has 1 to 4 live tokens, the first ones of its block, and the lengths sum to 112.
All inputs are finite; a program needn't handle non-finite values.
Results may differ from the reference program's by a relative error of at most 0.015.
Values may be sent and summed in bfloat16 or wider, within the bound.
A program may use at most 64 MiB of HBM per device.

```python
import math
import jax
import jax.numpy as jnp
import numpy as np
from jax import lax

D = 4096
HEADS = 32
HEAD_DIM = 128
FF = 11008
SPAN = 4
BATCH = 64
VALUE_WIDTH = 4096
N_KV = 8


def draw_tokens(key, part):
    key_base = jax.random.fold_in(key, 0)
    columns = jnp.arange(D, dtype=jnp.float32)
    block_size = D // N_KV
    within = (jnp.arange(D) % block_size).astype(jnp.float32) / block_size
    col_scale = 3.0 ** (columns / D) * 3.0 ** within
    base_draw = jnp.clip(jax.random.normal(key_base, (BATCH, SPAN, D), jnp.float32), -4.0, 4.0)
    return (base_draw * col_scale).astype(jnp.bfloat16)


def level_of(own_key, extent, pieces, low, high):
    factor_of = 1.0
    for axis_at, blocks in pieces:
        draws = jax.random.uniform(jax.random.fold_in(jax.random.fold_in(own_key, 6), axis_at), (blocks,), jnp.float32, low / len(pieces), high / len(pieces))
        factor_of = factor_of * jnp.repeat(jnp.exp(draws), extent[axis_at] // blocks).reshape((-1,) + (1,) * (len(extent) - 1 - axis_at))
    return factor_of


def split_up(amount, total, reach, lean):
    portions = [(1 << 20) // math.isqrt(grade ** lean) + 1 for grade in range(2, amount + 1)]
    spare, holding = total - reach - (amount - 1), [1] * (amount - 1)
    while spare > 0:
        movable = [i for i in range(amount - 1) if holding[i] < reach]
        mass, left = sum([portions[i] for i in movable]), spare
        for i in movable:
            addition = min(reach - holding[i], max(1, left * portions[i] // mass), spare)
            holding[i] = holding[i] + addition
            spare = spare - addition
    return np.array([reach] + holding)


def uneven(stream_key, amount, total, limit, lean):
    if amount == 2:
        one = jax.random.randint(stream_key, (), max(1, total - limit), min(limit, total - 1) + 1)
        return jnp.stack([one, total - one])
    sizes = jnp.asarray(split_up(amount, total, limit, lean), jnp.int32)
    pairs = (amount - 1) // 2
    source_of, taker = sizes[1:1 + 2 * pairs:2], sizes[2:2 + 2 * pairs:2]
    room = jnp.minimum(source_of - 1, limit - taker)
    moved = jax.random.randint(jax.random.fold_in(stream_key, 1), (pairs,), 0, 1 << 20) % (room + 1)
    sizes = sizes.at[1:1 + 2 * pairs:2].set(source_of - moved).at[2:2 + 2 * pairs:2].set(taker + moved)
    return sizes[jax.random.permutation(jax.random.fold_in(stream_key, 2), amount)]


def normal_values(own_key, extent, deviation, most, shards=(), held_as=jnp.bfloat16):
    entries = deviation * jax.random.normal(own_key, extent, jnp.float32)
    if shards:
        entries = entries * level_of(own_key, extent, shards, -0.22, 0.18)
    return jnp.clip(entries, -most, most).astype(held_as)


def setup_inputs(seed: int = 0) -> dict:
    arg_keys = jax.random.split(jax.random.key(seed), 18)
    tokens = draw_tokens(jax.random.fold_in(arg_keys[17], 71), 0)
    lengths = uneven(arg_keys[1], BATCH, BATCH * 7 // 4, SPAN, 2).astype(jnp.int32)
    state = normal_values(arg_keys[2], (BATCH, HEAD_DIM, VALUE_WIDTH), 0.1, 0.6, ((0, 8), (2, 4)), jnp.float32)
    attn_gain = jnp.clip(1.0 + 0.18 * jax.random.normal(arg_keys[3], (D,), jnp.float32), 0.1, 1.9)
    w_query = normal_values(arg_keys[4], (D, VALUE_WIDTH), D ** -0.5, 0.09375, ((0, 8), (1, 4)))
    w_key = normal_values(arg_keys[5], (D, VALUE_WIDTH), D ** -0.5, 0.09375, ((0, 8), (1, 4)))
    w_value = normal_values(arg_keys[6], (D, VALUE_WIDTH), D ** -0.5, 0.09375, ((0, 8), (1, 4)))
    w_beta = normal_values(arg_keys[7], (D, HEADS), D ** -0.5, 0.09375)
    w_alpha = normal_values(arg_keys[8], (D, HEADS), D ** -0.5, 0.09375)
    decay_rate = jnp.clip(jnp.exp(jax.random.uniform(arg_keys[9], (HEADS,), jnp.float32, math.log(0.05), math.log(3.0))), 0.05, 3.0)
    decay_bias = normal_values(arg_keys[10], (HEADS,), 1.0, 3.0, (), jnp.float32)
    out_gain = jnp.clip(1.0 + 0.18 * jax.random.normal(arg_keys[11], (HEAD_DIM,), jnp.float32), 0.1, 1.9)
    w_out = normal_values(arg_keys[12], (VALUE_WIDTH, D), VALUE_WIDTH ** -0.5, 0.09375, ((0, 4), (1, 8)))
    mix_gain = jnp.clip(1.0 + 0.18 * jax.random.normal(arg_keys[13], (D,), jnp.float32), 0.1, 1.9)
    w_gate = normal_values(arg_keys[14], (D, FF), D ** -0.5, 0.09375, ((0, 8), (1, 4)))
    w_up = normal_values(arg_keys[15], (D, FF), D ** -0.5, 0.09375, ((0, 8), (1, 4)))
    w_down = normal_values(arg_keys[16], (FF, D), FF ** -0.5, 0.0546875, ((0, 4), (1, 8)))
    return {"tokens": tokens, "lengths": lengths, "state": state, "attn_gain": attn_gain, "w_query": w_query, "w_key": w_key, "w_value": w_value, "w_beta": w_beta, "w_alpha": w_alpha, "decay_rate": decay_rate, "decay_bias": decay_bias, "out_gain": out_gain, "w_out": w_out, "mix_gain": mix_gain, "w_gate": w_gate, "w_up": w_up, "w_down": w_down}


EPSILON = 1e-06

def unit_rows(vectors):
    return vectors * lax.rsqrt(lax.optimization_barrier(jnp.sum(vectors * vectors, axis=-1, keepdims=True)) + EPSILON)

def reference(tokens, lengths, state, attn_gain, w_query, w_key, w_value, w_beta, w_alpha, decay_rate, decay_bias, out_gain, w_out, mix_gain, w_gate, w_up, w_down):
    row_total = BATCH * SPAN
    highest = lax.Precision.HIGHEST
    flat_rows = tokens.reshape(row_total, D).astype(jnp.float32)
    sq_in = lax.optimization_barrier(jnp.sum(flat_rows * flat_rows, axis=1))
    normed_in = (flat_rows * attn_gain).astype(jnp.bfloat16)
    row_scale = lax.rsqrt(sq_in / D + EPSILON)[:, None]
    query_raw = jnp.dot(normed_in, w_query, preferred_element_type=jnp.float32) * row_scale
    key_raw = jnp.dot(normed_in, w_key, preferred_element_type=jnp.float32) * row_scale
    value_rows = jnp.dot(normed_in, w_value, preferred_element_type=jnp.float32) * row_scale
    live_mask = (jnp.arange(SPAN, dtype=jnp.int32)[None, :] < lengths[:, None]).reshape(row_total, 1)
    beta = jnp.where(live_mask, jax.nn.sigmoid(jnp.dot(normed_in, w_beta, preferred_element_type=jnp.float32) * row_scale), 0.0)
    alpha_pre = jnp.dot(normed_in, w_alpha, preferred_element_type=jnp.float32) * row_scale + decay_bias
    log_decay = jnp.where(live_mask, -decay_rate * jax.nn.softplus(alpha_pre), 0.0)
    queries = unit_rows(query_raw.reshape(BATCH, SPAN, HEADS, HEAD_DIM)) * HEAD_DIM ** (-0.5)
    unit_keys = unit_rows(key_raw.reshape(BATCH, SPAN, HEADS, HEAD_DIM))
    values_split = value_rows.reshape(BATCH, SPAN, HEADS, HEAD_DIM)
    beta = beta.reshape(BATCH, SPAN, HEADS)
    log_decay = log_decay.reshape(BATCH, SPAN, HEADS)
    carried = state.reshape(BATCH, HEAD_DIM, HEADS, HEAD_DIM)
    outputs = []
    for step in range(SPAN):
        carried = carried * jnp.exp(log_decay[:, step])[:, None, :, None]
        predicted = jnp.einsum('bhd,bdhe->bhe', unit_keys[:, step], carried, precision=highest)
        update = beta[:, step][..., None] * (values_split[:, step] - predicted)
        carried = carried + jnp.einsum('bhd,bhe->bdhe', unit_keys[:, step], update, precision=highest)
        outputs.append(jnp.einsum('bhd,bdhe->bhe', queries[:, step], carried, precision=highest))
    attended = jnp.stack(outputs, axis=1)
    head_out = attended * lax.rsqrt(lax.optimization_barrier(jnp.mean(attended * attended, axis=-1, keepdims=True)) + EPSILON) * out_gain
    head_out = head_out.astype(jnp.bfloat16).reshape(row_total, VALUE_WIDTH)
    middle = (flat_rows + jnp.dot(head_out, w_out, preferred_element_type=jnp.float32)).astype(jnp.bfloat16)
    middle_f = middle.astype(jnp.float32)
    sq_mid = lax.optimization_barrier(jnp.sum(middle_f * middle_f, axis=1))
    normed_mid = (middle_f * mix_gain).astype(jnp.bfloat16)
    mid_scale = lax.rsqrt(sq_mid / D + EPSILON)[:, None]
    gate_rows = jnp.dot(normed_mid, w_gate, preferred_element_type=jnp.float32) * mid_scale
    up_rows = jnp.dot(normed_mid, w_up, preferred_element_type=jnp.float32) * mid_scale
    hidden = (jax.nn.silu(gate_rows) * up_rows).astype(jnp.bfloat16)
    result_rows = middle_f + jnp.dot(hidden, w_down, preferred_element_type=jnp.float32)
    mixed = jnp.where(live_mask, result_rows, 0.0).astype(jnp.bfloat16).reshape(BATCH, SPAN, D)
    return (mixed, carried.reshape(BATCH, HEAD_DIM, VALUE_WIDTH))
```

```python
import jax
import jax.numpy as jnp
from jax import lax
from jax.experimental import pallas as pl
from jax.experimental.pallas import tpu as pltpu
from jax.sharding import PartitionSpec as P

MESH = pl.DeviceIdType.MESH
F32 = jnp.float32
BF16 = jnp.bfloat16

D = 4096
HEAD_DIM = 128


EPSILON = 1e-06


def unit_rows(vectors):
    return vectors * lax.rsqrt(jnp.sum(vectors * vectors, axis=-1, keepdims=True) + EPSILON)


def delta_block(queries, unit_keys, values_split, beta, log_decay, carried):
    highest = lax.Precision.HIGHEST
    seq_count, span_len, heads_here = beta.shape
    cumulative = jnp.cumsum(log_decay, axis=1)
    position = jnp.arange(span_len)
    inclusive = (position[:, None] >= position[None, :])[None, :, :, None]
    strict = (position[:, None] > position[None, :])[None, :, :, None]
    gap_matrix = cumulative[:, :, None, :] - cumulative[:, None, :, :]
    decay_matrix = jnp.where(inclusive, jnp.exp(jnp.where(inclusive, gap_matrix, 0.0)), 0.0)
    key_dots = jnp.einsum("nihd,njhd->nijh", unit_keys, unit_keys, precision=highest)
    query_dots = jnp.einsum("nihd,njhd->nijh", queries, unit_keys, precision=highest) * decay_matrix
    lower_part = jnp.where(strict, key_dots * decay_matrix * beta[:, :, None, :], 0.0)
    identity = jnp.eye(span_len, dtype=jnp.float32)
    inverse_rows = []
    for step in range(span_len):
        row_now = jnp.broadcast_to(identity[step][None, :, None], (seq_count, span_len, heads_here))
        for prior in range(step):
            row_now = row_now - lower_part[:, step, prior, :][:, None, :] * inverse_rows[prior]
        inverse_rows.append(row_now)
    inverse = jnp.stack(inverse_rows, axis=1)
    beta_value = beta[..., None] * values_split
    beta_key = (beta * jnp.exp(cumulative))[..., None] * unit_keys
    base_update = jnp.einsum("nich,nche->nihe", inverse, beta_value, precision=highest)
    key_weights = jnp.einsum("nich,nchd->nihd", inverse, beta_key, precision=highest)
    corrected = base_update - jnp.einsum("nihd,ndhe->nihe", key_weights, carried, precision=highest)
    decayed_queries = queries * jnp.exp(cumulative)[..., None]
    attended = jnp.einsum("nihd,ndhe->nihe", decayed_queries, carried, precision=highest)
    attended = attended + jnp.einsum("nijh,njhe->nihe", query_dots, corrected, precision=highest)
    block_total = cumulative[:, -1, :]
    key_tail = unit_keys * jnp.exp(block_total[:, None, :] - cumulative)[..., None]
    updated = carried * jnp.exp(block_total)[:, None, :, None]
    updated = updated + jnp.einsum("nihd,nihe->ndhe", key_tail, corrected, precision=highest)
    return (attended, updated)


def body(
    tokens,
    lengths,
    state,
    attn_gain,
    w_query,
    w_key,
    w_value,
    w_beta,
    w_alpha,
    decay_rate,
    decay_bias,
    out_gain,
    w_out,
    mix_gain,
    w_gate,
    w_up,
    w_down,
):
    kv_index = lax.axis_index("kv")
    tp_index = lax.axis_index("tp")
    kv_count = lax.axis_size("kv")
    batch_all, span_len, own_cols = tokens.shape
    row_count = batch_all * span_len
    seq_count = state.shape[0]
    local_rows = seq_count * span_len
    head_size = state.shape[1]
    heads_here = state.shape[2] // head_size
    block_width = attn_gain.shape[0]
    flat_rows = tokens.reshape(row_count, own_cols)
    live_all = (jnp.arange(span_len, dtype=jnp.int32)[None, :] < lengths[:, None]).reshape(
        row_count, 1
    )
    gathered = lax.all_gather(flat_rows, "tp", axis=1, tiled=True).astype(jnp.float32)
    squares_in = jnp.sum(gathered * gathered, axis=1)
    normed_in = (gathered * attn_gain).astype(jnp.bfloat16)
    beta_rows = lax.dynamic_slice_in_dim(w_beta, kv_index * block_width, block_width, 0)
    alpha_rows = lax.dynamic_slice_in_dim(w_alpha, kv_index * block_width, block_width, 0)
    query_part = jnp.dot(normed_in, w_query, preferred_element_type=jnp.float32)
    key_part = jnp.dot(normed_in, w_key, preferred_element_type=jnp.float32)
    value_part = jnp.dot(normed_in, w_value, preferred_element_type=jnp.float32)
    beta_part = jnp.dot(normed_in, beta_rows, preferred_element_type=jnp.float32)
    alpha_part = jnp.dot(normed_in, alpha_rows, preferred_element_type=jnp.float32)
    squares_all = lax.psum(squares_in, "kv")
    squares_own = lax.dynamic_slice_in_dim(squares_all, kv_index * local_rows, local_rows, 0)
    query_sum, key_sum, value_sum, beta_sum, alpha_sum = (
        lax.psum_scatter(
            query_part.astype(jnp.bfloat16), "kv", scatter_dimension=0, tiled=True
        ).astype(jnp.float32),
        lax.psum_scatter(
            key_part.astype(jnp.bfloat16), "kv", scatter_dimension=0, tiled=True
        ).astype(jnp.float32),
        lax.psum_scatter(
            value_part.astype(jnp.bfloat16), "kv", scatter_dimension=0, tiled=True
        ).astype(jnp.float32),
        lax.psum_scatter(
            beta_part.astype(jnp.bfloat16), "kv", scatter_dimension=0, tiled=True
        ).astype(jnp.float32),
        lax.psum_scatter(
            alpha_part.astype(jnp.bfloat16), "kv", scatter_dimension=0, tiled=True
        ).astype(jnp.float32),
    )
    row_scale = lax.rsqrt(squares_own / D + EPSILON)[:, None]
    head_start = tp_index * heads_here
    lengths_own = lax.dynamic_slice_in_dim(lengths, kv_index * seq_count, seq_count, 0)
    live_own = (jnp.arange(span_len, dtype=jnp.int32)[None, :] < lengths_own[:, None])[..., None]
    beta_heads = lax.dynamic_slice_in_dim(beta_sum, head_start, heads_here, 1) * row_scale
    alpha_heads = lax.dynamic_slice_in_dim(alpha_sum, head_start, heads_here, 1) * row_scale
    rate_here = lax.dynamic_slice_in_dim(decay_rate, head_start, heads_here, 0)
    bias_here = lax.dynamic_slice_in_dim(decay_bias, head_start, heads_here, 0)
    beta = jnp.where(
        live_own, jax.nn.sigmoid(beta_heads).reshape(seq_count, span_len, heads_here), 0.0
    )
    log_decay = -rate_here * jax.nn.softplus(alpha_heads + bias_here)
    log_decay = jnp.where(live_own, log_decay.reshape(seq_count, span_len, heads_here), 0.0)
    split_shape = (seq_count, span_len, heads_here, head_size)
    queries = unit_rows((query_sum * row_scale).reshape(split_shape)) * HEAD_DIM ** (-0.5)
    unit_keys = unit_rows((key_sum * row_scale).reshape(split_shape))
    values_split = (value_sum * row_scale).reshape(split_shape)
    carried = state.reshape(seq_count, head_size, heads_here, head_size)
    attended, updated = delta_block(queries, unit_keys, values_split, beta, log_decay, carried)
    head_out = (
        attended
        * lax.rsqrt(jnp.mean(attended * attended, axis=-1, keepdims=True) + EPSILON)
        * out_gain
    )
    head_out = head_out.astype(jnp.bfloat16).reshape(local_rows, heads_here * head_size)
    pack_rows = min((batch_all * 7 // 4 + kv_count - 1) // kv_count * kv_count, row_count)
    live_flat = live_all.reshape(row_count).astype(jnp.int32)
    slot_index = jnp.cumsum(live_flat) - 1
    picker = (
        (slot_index[None, :] == jnp.arange(pack_rows, dtype=jnp.int32)[:, None])
        & (live_flat[None, :] > 0)
    ).astype(jnp.bfloat16)
    heads_every = lax.all_gather(head_out, "kv", axis=0, tiled=True)
    packed_heads = jnp.dot(picker, heads_every, preferred_element_type=jnp.float32).astype(
        jnp.bfloat16
    )
    attn_part = jnp.dot(packed_heads, w_out, preferred_element_type=jnp.float32)
    base_rows = jnp.dot(picker, flat_rows, preferred_element_type=jnp.float32)
    attn_own = lax.psum_scatter(
        attn_part.astype(jnp.bfloat16), "tp", scatter_dimension=1, tiled=True
    ).astype(jnp.float32)
    middle = (base_rows + attn_own).astype(jnp.bfloat16)
    middle_rows = lax.all_gather(middle, "tp", axis=1, tiled=True).astype(jnp.float32)
    squares_mid = jnp.sum(middle_rows * middle_rows, axis=1)
    normed_mid = (middle_rows * mix_gain).astype(jnp.bfloat16)
    gate_part = jnp.dot(normed_mid, w_gate, preferred_element_type=jnp.float32)
    up_part = jnp.dot(normed_mid, w_up, preferred_element_type=jnp.float32)
    squares_total = lax.psum(squares_mid, "kv")
    gate_sum, up_sum = (
        lax.psum(gate_part.astype(jnp.bfloat16), "kv").astype(jnp.float32),
        lax.psum(up_part.astype(jnp.bfloat16), "kv").astype(jnp.float32),
    )
    mid_scale = lax.rsqrt(squares_total / D + EPSILON)[:, None]
    hidden = (jax.nn.silu(gate_sum * mid_scale) * (up_sum * mid_scale)).astype(jnp.bfloat16)
    down_part = jnp.dot(hidden, w_down, preferred_element_type=jnp.float32)
    down_own = lax.psum_scatter(
        down_part.astype(jnp.bfloat16), "tp", scatter_dimension=1, tiled=True
    ).astype(jnp.float32)
    result_rows = middle.astype(jnp.float32) + down_own
    result_rows = jnp.dot(
        picker.astype(jnp.float32).T,
        result_rows,
        precision=lax.Precision.HIGHEST,
        preferred_element_type=jnp.float32,
    )
    mixed = (
        jnp.where(live_all, result_rows, 0.0)
        .astype(jnp.bfloat16)
        .reshape(batch_all, span_len, own_cols)
    )
    return (mixed, updated.reshape(seq_count, head_size, heads_here * head_size))


def iota(shape, axis):
    return lax.broadcasted_iota(jnp.int32, shape, axis)


def dot(a, b):
    return jnp.dot(a, b, preferred_element_type=F32)


def dot_t(a, b):
    return lax.dot_general(a, b, (((1,), (1,)), ((), ())), preferred_element_type=F32)


def dot_exact(a, b):
    return jnp.dot(a, b, precision=lax.Precision.HIGHEST, preferred_element_type=F32)


def head_sum(x, heads, size):
    pieces = []
    for h in range(heads):
        total = jnp.sum(x[:, h * size : (h + 1) * size], axis=1, keepdims=True)
        pieces.append(jnp.broadcast_to(total, (x.shape[0], size)))
    return jnp.concatenate(pieces, axis=1)


def high_low(x):
    high = x.astype(BF16)
    return high.astype(F32), x - high.astype(F32)


def layer_kernel(
    dims,
    tokens_hbm,
    lengths_hbm,
    state_hbm,
    attn_gain_hbm,
    wq_hbm,
    wk_hbm,
    wv_hbm,
    wb_hbm,
    wa_hbm,
    rate_hbm,
    bias_hbm,
    out_gain_hbm,
    wo_hbm,
    mix_gain_hbm,
    wg_hbm,
    wu_hbm,
    wd_hbm,
    mixed_ref,
    state,
    tokens_ref,
    lengths_ref,
    attn_gain_ref,
    rate_ref,
    bias_ref,
    out_gain_ref,
    mix_gain_ref,
    w_qkv,
    w_beta,
    w_alpha,
    w_out,
    w_gate,
    w_up,
    w_down,
    tok_all,
    qkv_part,
    qkv_pair,
    qkv_red,
    qkv_recv,
    head_all,
    attn_part,
    attn_recv,
    mid_all,
    gu_part,
    gu_pair,
    gu_red,
    gu_recv,
    hid_first,
    hid_second,
    down_part,
    down_recv,
    placed_ref,
    square_ref,
    normed_ref,
    side_ref,
    load_sem,
    small_sem,
    tp_send,
    tp_recv,
    pair_send,
    pair_recv,
    chip_send,
    chip_recv,
    fwd_send,
    fwd_recv,
):
    n_kv, n_tp, batch, span, seqs, heads, size, width, ff, rows, packs, unit = dims
    chips = n_kv // 2
    kv = lax.axis_index("kv")
    tp = lax.axis_index("tp")
    core = lax.rem(kv, 2)
    chip = kv // 2
    other = 1 - core
    partner = chip * 2 + other
    slots = batch * span
    local = seqs * span
    vw = heads * size

    def chip_at(d):
        return lax.rem(chip + d, chips)

    def chip_from(d):
        return lax.rem(chip + chips - d, chips)

    barrier = pltpu.get_barrier_semaphore()
    pl.semaphore_signal(barrier, inc=1, device_id={"kv": partner}, device_id_type=MESH)
    for d in range(1, chips):
        pl.semaphore_signal(
            barrier, inc=1, device_id={"kv": chip_at(d) * 2 + core}, device_id_type=MESH
        )
    for d in range(1, n_tp):
        pl.semaphore_signal(
            barrier, inc=1, device_id={"tp": lax.rem(tp + d, n_tp)}, device_id_type=MESH
        )

    smalls = [
        pltpu.make_async_copy(source, dest, small_sem.at[i])
        for i, (source, dest) in enumerate(
            (
                (tokens_hbm, tokens_ref),
                (lengths_hbm, lengths_ref),
                (attn_gain_hbm, attn_gain_ref),
                (rate_hbm, rate_ref),
                (bias_hbm, bias_ref),
                (out_gain_hbm, out_gain_ref),
                (mix_gain_hbm, mix_gain_ref),
            )
        )
    ]
    for load in smalls:
        load.start()
    loads = [
        pltpu.make_async_copy(wq_hbm, w_qkv.at[0], load_sem.at[0]),
        pltpu.make_async_copy(wk_hbm, w_qkv.at[1], load_sem.at[1]),
        pltpu.make_async_copy(wv_hbm, w_qkv.at[2], load_sem.at[2]),
        pltpu.make_async_copy(
            wb_hbm.at[:, pl.ds(pl.multiple_of(kv * width, width), width)], w_beta, load_sem.at[3]
        ),
        pltpu.make_async_copy(
            wa_hbm.at[:, pl.ds(pl.multiple_of(kv * width, width), width)], w_alpha, load_sem.at[4]
        ),
        pltpu.make_async_copy(state_hbm, state, load_sem.at[5]),
        pltpu.make_async_copy(wo_hbm, w_out, load_sem.at[6]),
        pltpu.make_async_copy(wg_hbm, w_gate, load_sem.at[7]),
        pltpu.make_async_copy(wu_hbm, w_up, load_sem.at[8]),
        pltpu.make_async_copy(wd_hbm, w_down, load_sem.at[9]),
    ]
    for load in loads:
        load.start()

    for load in smalls:
        load.wait()
    lengths_row = lengths_ref[...].astype(F32)
    spread = (iota((batch, slots), 1) // span == iota((batch, slots), 0)).astype(BF16)
    length_of = dot(jnp.broadcast_to(lengths_row, (8, batch)).astype(BF16), spread)
    live_row = (lax.rem(iota((8, slots), 1), span).astype(F32) < length_of).astype(F32)
    before = (iota((slots, slots), 0) < iota((slots, slots), 1)).astype(BF16)
    slot_row = dot(live_row.astype(BF16), before)
    slot_row = jnp.where(live_row > 0.0, slot_row, -1.0)[0:1, :]
    picker = (iota((packs, slots), 0).astype(F32) == slot_row).astype(BF16)
    position = iota((slots, slots), 1) // local
    inner = lax.rem(iota((slots, slots), 1), local)
    from_slot = (
        (lax.rem(position, chips) * 2 + position // chips) * seqs + lax.rem(inner, seqs)
    ) * span + inner // seqs
    order = (iota((slots, slots), 0) == from_slot).astype(BF16)
    picker_kv = dot(picker, order).astype(BF16)

    own_tokens = dot(picker, tokens_ref[...])
    tok_all[tp] = own_tokens.astype(BF16)
    pl.semaphore_wait(barrier, 1 + (chips - 1) + (n_tp - 1))

    def tp_copies(phase, source_at, dest_at):
        copies = []
        for d in range(1, n_tp):
            peer = lax.rem(tp + d, n_tp)
            copies.append(
                pltpu.make_async_remote_copy(
                    src_ref=source_at(peer, d),
                    dst_ref=dest_at(peer, d),
                    send_sem=tp_send.at[phase, d - 1],
                    recv_sem=tp_recv.at[phase, d - 1],
                    device_id={"tp": peer},
                    device_id_type=MESH,
                )
            )
        return copies

    def exchange_start(copies):
        for copy in copies:
            copy.start()

    def exchange_wait(copies):
        for copy in copies:
            copy.wait()

    copies = tp_copies(0, lambda peer, d: tok_all.at[tp], lambda peer, d: tok_all.at[tp])
    exchange_start(copies)
    exchange_wait(copies)
    gathered = jnp.concatenate([tok_all[j] for j in range(n_tp)], axis=1).astype(F32)
    squares = jnp.sum(gathered * gathered, axis=1, keepdims=True)
    normed = (gathered * attn_gain_ref[...]).astype(BF16)
    square_high, square_low = high_low(squares)
    square_pair = jnp.concatenate([square_high, square_low], axis=1).astype(BF16)

    def place(rows_packed):
        return lax.dot_general(
            picker_kv, rows_packed, (((0,), (0,)), ((), ())), preferred_element_type=F32
        ).astype(BF16)

    placed = place(normed)
    square_placed = place(square_pair)
    half = chips * local
    n_heads_all = wb_hbm.shape[0]
    qkv_width = 3 * vw + 128
    first = 128 + vw
    chunks = ((0, first), (first, first + vw), (first + vw, qkv_width))

    def halves(c, size_of):
        return pl.ds(pl.multiple_of(c * size_of, size_of), size_of)

    def pair_start(index, source, dest):
        copy = pltpu.make_async_remote_copy(
            src_ref=source,
            dst_ref=dest,
            send_sem=pair_send.at[index],
            recv_sem=pair_recv.at[index],
            device_id={"kv": partner},
            device_id_type=MESH,
        )
        copy.start()
        return copy

    def chip_start(index, d, source, dest):
        copy = pltpu.make_async_remote_copy(
            src_ref=source,
            dst_ref=dest,
            send_sem=chip_send.at[index, d - 1],
            recv_sem=chip_recv.at[index, d - 1],
            device_id={"kv": chip_at(d) * 2 + core},
            device_id_type=MESH,
        )
        copy.start()
        return copy

    placed_ref[...] = placed
    square_ref[...] = square_placed

    def qkv_chunk(m, c):
        part = halves(c, half)
        here = placed_ref[part, :]
        low, high = chunks[m]
        if m == 0:
            extra = jnp.concatenate(
                [
                    dot_t(here, w_beta[...]),
                    dot_t(here, w_alpha[...]),
                    square_ref[part, :].astype(F32),
                    jnp.zeros((half, 128 - 2 * n_heads_all - 2), F32),
                ],
                axis=1,
            )
            qkv_part[part, 0:128] = extra.astype(BF16)
            low = 128
        qkv_part[part, low:high] = dot(here, w_qkv[(1, 0, 2)[m]]).astype(BF16)

    def qkv_finish(m):
        pair_copies[m].wait()
        cols = slice(*chunks[m])
        for d in range(1, chips):
            dest = chip_at(d)
            at = halves(dest, local)
            mine = pl.ds(pl.multiple_of(core * half + dest * local, local), local)
            qkv_red[d - 1, :, cols] = (
                qkv_part[mine, cols].astype(F32) + qkv_pair[at, cols].astype(F32)
            ).astype(BF16)
            qkv_far[m].append(
                chip_start(m, d, qkv_red.at[d - 1, :, cols], qkv_recv.at[d - 1, :, cols])
            )

    pair_copies = []
    qkv_far = [[], [], []]
    for m in range(3):
        loads[(1, 0, 2)[m]].wait()
        if m == 0:
            loads[3].wait()
            loads[4].wait()
        qkv_chunk(m, other)
        cols = slice(*chunks[m])
        pair_copies.append(
            pair_start(m, qkv_part.at[halves(other, half), cols], qkv_pair.at[:, cols])
        )
        qkv_chunk(m, core)
        if m > 0:
            qkv_finish(m - 1)
    qkv_finish(2)

    loads[5].wait()
    state_low = state[...].reshape(seqs * size, vw).astype(BF16)

    def own_sum(m):
        exchange_wait(qkv_far[m])
        cols = slice(*chunks[m])
        at = halves(chip, local)
        mine = pl.ds(pl.multiple_of(core * half + chip * local, local), local)
        total = qkv_part[mine, cols].astype(F32) + qkv_pair[at, cols].astype(F32)
        for d in range(1, chips):
            total = total + qkv_recv[d - 1, :, cols].astype(F32)
        return total

    extra_keys = own_sum(0)
    extra = extra_keys[:, 0:128]
    lane = iota((local, 128), 1)
    sq_lane = (lane == 2 * n_heads_all) | (lane == 2 * n_heads_all + 1)
    sq_own = jnp.sum(jnp.where(sq_lane, extra, 0.0), axis=1, keepdims=True)
    row_scale = lax.rsqrt(sq_own / D + EPSILON)
    scaled_extra = jnp.where(sq_lane, 0.0, extra * row_scale)
    lane_of = iota((128, vw), 0)
    head_of = iota((128, vw), 1) // size + tp * heads
    beta_pre = dot_exact(scaled_extra, (lane_of == head_of).astype(F32))
    alpha_pre = dot_exact(scaled_extra, (lane_of == head_of + n_heads_all).astype(F32))
    per_head = (iota((n_heads_all, vw), 0) == iota((n_heads_all, vw), 1) // size + tp * heads).astype(F32)
    rate = dot_exact(jnp.broadcast_to(rate_ref[...], (8, n_heads_all)), per_head)[0:1, :]
    bias = dot_exact(jnp.broadcast_to(bias_ref[...], (8, n_heads_all)), per_head)[0:1, :]
    row_id = iota((local, batch), 0)
    seq_hit = iota((local, batch), 1) == kv * seqs + lax.rem(row_id, seqs)
    own_len = jnp.sum(jnp.where(seq_hit, lengths_row, 0.0), axis=1, keepdims=True)
    live = (iota((local, 1), 0) // seqs).astype(F32) < own_len
    beta = jnp.where(live, 1.0 / (1.0 + jnp.exp(-beta_pre)), 0.0)
    pre = alpha_pre + bias
    softplus = jnp.maximum(pre, 0.0) + jnp.log(1.0 + jnp.exp(-jnp.abs(pre)))
    log_decay = jnp.where(live, -rate * softplus, 0.0)

    k_raw = extra_keys[:, 128:] * row_scale
    keys = k_raw * lax.rsqrt(head_sum(k_raw * k_raw, heads, size) + EPSILON)
    q_raw = own_sum(1) * row_scale
    queries = q_raw * lax.rsqrt(head_sum(q_raw * q_raw, heads, size) + EPSILON) * size ** (-0.5)

    def token(x, t):
        return x[t * seqs : (t + 1) * seqs, :]

    cumulative = [token(log_decay, 0)]
    for t in range(1, span):
        cumulative.append(cumulative[-1] + token(log_decay, t))

    def blocked(x):
        keep = lax.rem(iota(x.shape, 0), seqs)
        return jnp.concatenate(
            [jnp.where(keep == n, x, 0.0).astype(BF16) for n in range(seqs)], axis=1
        )

    products = []
    for h in range(heads):
        cols = slice(h * size, (h + 1) * size)
        both = jnp.concatenate([keys[:, cols], queries[:, cols]], axis=0)
        products.append(dot(blocked(both), state_low[:, cols]))
    products = jnp.concatenate(products, axis=1)
    values = own_sum(2) * row_scale
    updates, attended = [], []
    for t in range(span):
        grown = jnp.exp(cumulative[t])
        update = token(values, t) - grown * token(products, t)
        for p in range(t):
            weight = jnp.exp(cumulative[t] - cumulative[p]) * head_sum(
                token(keys, t) * token(keys, p), heads, size
            )
            update = update - weight * updates[p]
        updates.append(token(beta, t) * update)
        result = grown * token(products, span + t)
        for p in range(t + 1):
            weight = jnp.exp(cumulative[t] - cumulative[p]) * head_sum(
                token(queries, t) * token(keys, p), heads, size
            )
            result = result + weight * updates[p]
        attended.append(result)
    attended = jnp.concatenate(attended, axis=0)
    gain = jnp.concatenate([out_gain_ref[...]] * heads, axis=1)
    head_out = attended * lax.rsqrt(head_sum(attended * attended, heads, size) / size + EPSILON) * gain

    def kv_gather_start(phase, buffer):
        spot = core * chips + chip
        own = pltpu.make_async_remote_copy(
            src_ref=buffer.at[spot],
            dst_ref=buffer.at[spot],
            send_sem=fwd_send.at[phase, 0],
            recv_sem=fwd_recv.at[phase, 0],
            device_id={"kv": partner},
            device_id_type=MESH,
        )
        far = [
            pltpu.make_async_remote_copy(
                src_ref=buffer.at[spot],
                dst_ref=buffer.at[spot],
                send_sem=chip_send.at[8 + phase, d - 1],
                recv_sem=chip_recv.at[8 + phase, d - 1],
                device_id={"kv": chip_at(d) * 2 + core},
                device_id_type=MESH,
            )
            for d in range(1, chips)
        ]
        exchange_start(far)
        own.start()
        return own, far

    def kv_gather_finish(phase, buffer, own, far):
        forwards = []
        for d in range(1, chips):
            far[d - 1].wait_recv()
            spot = core * chips + chip_from(d)
            forwards.append(
                pltpu.make_async_remote_copy(
                    src_ref=buffer.at[spot],
                    dst_ref=buffer.at[spot],
                    send_sem=fwd_send.at[phase, d],
                    recv_sem=fwd_recv.at[phase, d],
                    device_id={"kv": partner},
                    device_id_type=MESH,
                )
            )
            forwards[-1].start()
        own.wait()
        exchange_wait(forwards)
        for copy in far:
            copy.wait_send()

    head_all[core * chips + chip] = head_out.astype(BF16)
    own, far = kv_gather_start(0, head_all)

    final = cumulative[-1]
    tails = jnp.concatenate(
        [token(keys, t) * jnp.exp(final - cumulative[t]) for t in range(span)], axis=0
    )
    all_updates = jnp.concatenate(updates, axis=0).astype(BF16)
    decay_all = jnp.exp(final)
    for h in range(heads):
        cols = slice(h * size, (h + 1) * size)
        rank = lax.dot_general(
            blocked(tails[:, cols]),
            all_updates[:, cols],
            (((0,), (0,)), ((), ())),
            preferred_element_type=F32,
        )
        for n in range(seqs):
            state[n, :, cols] = (
                state[n, :, cols] * decay_all[n : n + 1, cols] + rank[n * size : (n + 1) * size, :]
            )

    kv_gather_finish(0, head_all, own, far)
    heads_every = head_all[...].reshape(slots, vw)
    packed = dot(picker_kv, heads_every).astype(BF16)
    loads[6].wait()
    part = dot(packed, w_out[...])
    own_cols = tokens_ref.shape[1]

    def tp_scatter_start(phase, part, part_ref, recv_ref, group):
        for j in range(n_tp):
            part_ref[j, group, :] = part[group, j * own_cols : (j + 1) * own_cols].astype(BF16)
        copies = tp_copies(
            phase,
            lambda peer, d: part_ref.at[peer, group, :],
            lambda peer, d: recv_ref.at[d - 1, group, :],
        )
        exchange_start(copies)
        return copies

    def tp_scatter_finish(copies, part_ref, recv_ref, group):
        exchange_wait(copies)
        total = part_ref[tp, group, :].astype(F32)
        for d in range(1, n_tp):
            total = total + recv_ref[d - 1, group, :].astype(F32)
        return total

    cut = packs // 32 * 16
    groups = (slice(0, cut), slice(cut, packs))
    scatters = [
        tp_scatter_start((1, 4)[i], part, attn_part, attn_recv, group)
        for i, group in enumerate(groups)
    ]
    gathers = []
    for i, group in enumerate(groups):
        middle = (
            own_tokens[group, :] + tp_scatter_finish(scatters[i], attn_part, attn_recv, group)
        ).astype(BF16)
        mid_all[tp, group, :] = middle
        gathers.append(
            tp_copies(
                (2, 5)[i],
                lambda peer, d: mid_all.at[tp, group, :],
                lambda peer, d: mid_all.at[tp, group, :],
            )
        )
        exchange_start(gathers[-1])
    for copies in gathers:
        exchange_wait(copies)
    middle_rows = jnp.concatenate([mid_all[j] for j in range(n_tp)], axis=1).astype(F32)
    squares = jnp.sum(middle_rows * middle_rows, axis=1, keepdims=True)
    normed_mid = (middle_rows * mix_gain_ref[...]).astype(BF16)
    ff_pad = gu_part.shape[2]
    pad = ff_pad - ff
    empty = rows - packs
    if empty:
        normed_mid = jnp.concatenate([normed_mid, jnp.zeros((empty, width), BF16)], axis=0)
        squares = jnp.concatenate([squares, jnp.zeros((empty, 1), F32)], axis=0)
    square_high, square_low = high_low(squares)
    half = chips * unit
    normed_ref[...] = normed_mid
    side_ref[...] = jnp.concatenate(
        [square_high, square_low, jnp.zeros((rows, pad - 2), F32)], axis=1
    )
    middle_col = ff_pad // 256 * 128
    last_col = ff // 128 * 128
    gu_chunks = (
        (0, last_col, ff_pad),
        (0, 0, middle_col),
        (1, 0, middle_col),
        (0, middle_col, last_col),
        (1, middle_col, ff_pad),
    )

    def gu_chunk(index, c):
        m, low, high = gu_chunks[index]
        part = halves(c, half)
        stop = min(high, ff)
        weights = (w_gate, w_up)[m]
        if stop > low:
            gu_part[m, part, low:stop] = dot_t(normed_ref[part, :], weights[low:stop, :]).astype(
                BF16
            )
        if high > ff:
            side = side_ref[part, :] if m == 0 else jnp.zeros((half, pad), F32)
            gu_part[m, part, ff:high] = side.astype(BF16)

    def gu_finish(index):
        gu_pairs[index].wait()
        m, low, high = gu_chunks[index]
        cols = slice(low, high)
        for d in range(1, chips):
            dest = chip_at(d)
            at = halves(dest, unit)
            mine = pl.ds(pl.multiple_of(core * half + dest * unit, unit), unit)
            gu_red[m, d - 1, :, cols] = (
                gu_part[m, mine, cols].astype(F32) + gu_pair[m, at, cols].astype(F32)
            ).astype(BF16)
            gu_far[index].append(
                chip_start(
                    3 + index, d, gu_red.at[m, d - 1, :, cols], gu_recv.at[m, d - 1, :, cols]
                )
            )

    gu_pairs, gu_far = [], [[] for _ in gu_chunks]
    loads[7].wait()
    loads[8].wait()
    for index, (m, low, high) in enumerate(gu_chunks):
        gu_chunk(index, other)
        gu_pairs.append(
            pair_start(
                3 + index,
                gu_part.at[m, halves(other, half), slice(low, high)],
                gu_pair.at[m, :, slice(low, high)],
            )
        )
        gu_chunk(index, core)
        if index > 0:
            gu_finish(index - 1)
    gu_finish(len(gu_chunks) - 1)
    at = halves(chip, unit)
    mine = pl.ds(pl.multiple_of(core * half + chip * unit, unit), unit)

    def gu_sum(index):
        exchange_wait(gu_far[index])
        m, low, high = gu_chunks[index]
        cols = slice(low, high)
        total = gu_part[m, mine, cols].astype(F32) + gu_pair[m, at, cols].astype(F32)
        for d in range(1, chips):
            total = total + gu_recv[m, d - 1, :, cols].astype(F32)
        return total

    spot = core * chips + chip
    gate_last = gu_sum(0)
    lane = iota(gate_last.shape, 1) + last_col
    sq_mid = jnp.sum(
        jnp.where((lane == ff) | (lane == ff + 1), gate_last, 0.0), axis=1, keepdims=True
    )
    mid_scale = lax.rsqrt(sq_mid / D + EPSILON)
    gate_last = jnp.where(lane < ff, gate_last, 0.0)

    def hidden_of(gate, up):
        gate = gate * mid_scale
        return (gate / (1.0 + jnp.exp(-gate)) * (up * mid_scale)).astype(BF16)

    hid_first[spot] = hidden_of(gu_sum(1), gu_sum(2))
    own_first, far_first = kv_gather_start(1, hid_first)
    gate = jnp.concatenate([gu_sum(3), gate_last], axis=1)
    hid_second[spot] = hidden_of(gate, gu_sum(4))
    own_second, far_second = kv_gather_start(2, hid_second)
    kv_gather_finish(1, hid_first, own_first, far_first)
    loads[9].wait()
    hidden_all = hid_first[...].reshape(rows, middle_col)[0:packs, :]
    part = dot(hidden_all, w_down[0:middle_col, :])
    kv_gather_finish(2, hid_second, own_second, far_second)
    hidden_all = hid_second[...].reshape(rows, ff_pad - middle_col)[0:packs, 0 : ff - middle_col]
    part = part + dot(hidden_all, w_down[middle_col:ff, :])
    every = slice(0, packs)
    copies = tp_scatter_start(3, part, down_part, down_recv, every)
    down = tp_scatter_finish(copies, down_part, down_recv, every)
    result = (mid_all[tp].astype(F32) + down).astype(BF16)
    mixed_ref[...] = lax.dot_general(
        picker, result, (((0,), (0,)), ((), ())), preferred_element_type=F32
    ).astype(BF16)


def fused_layer(n_kv, n_tp, *args):
    tokens, lengths, state, attn_gain, w_query = args[:5]
    w_beta, w_out, w_gate = args[7], args[12], args[14]
    batch, span, own_cols = tokens.shape
    seqs, size, vw = state.shape
    heads = vw // size
    width = attn_gain.shape[0]
    ff = w_gate.shape[1]
    pack = min(batch * 7 // 4, batch * span)
    unit = (pack + n_kv - 1) // n_kv
    unit = (unit + 15) // 16 * 16
    packs = (pack + 15) // 16 * 16
    rows = unit * n_kv
    local = seqs * span
    chips = n_kv // 2
    ff_pad = (ff + 2 + 127) // 128 * 128
    qkv_width = 3 * vw + 128
    dims = (n_kv, n_tp, batch, span, seqs, heads, size, width, ff, rows, packs, unit)
    operands = list(args)
    operands[0] = tokens.reshape(batch * span, own_cols)
    for at in (1, 3, 9, 10, 11, 13):
        operands[at] = operands[at].reshape(1, -1)
    for at in (7, 8, 14, 15):
        operands[at] = operands[at].T
    in_vmem = pl.BlockSpec(memory_space=pltpu.VMEM)
    in_hbm = pl.BlockSpec(memory_space=pltpu.HBM)
    dma = pltpu.SemaphoreType.DMA

    def buf(*shape):
        return pltpu.VMEM(shape, BF16)

    mixed, new_state = pl.pallas_call(
        lambda *refs: layer_kernel(dims, *refs),
        out_shape=(
            pltpu.VMEM((batch * span, own_cols), BF16),
            pltpu.VMEM(state.shape, F32),
        ),
        in_specs=[in_hbm] * len(operands),
        out_specs=(in_vmem, in_vmem),
        scratch_shapes=[
            buf(batch * span, own_cols),
            pltpu.VMEM((1, batch), jnp.int32),
            pltpu.VMEM((1, width), F32),
            pltpu.VMEM((1, args[9].shape[0]), F32),
            pltpu.VMEM((1, args[10].shape[0]), F32),
            pltpu.VMEM((1, size), F32),
            pltpu.VMEM((1, width), F32),
            buf(3, width, vw),
            buf(w_beta.shape[1], width),
            buf(w_beta.shape[1], width),
            buf(*w_out.shape),
            buf(ff, width),
            buf(ff, width),
            buf(ff, w_out.shape[1]),
            buf(n_tp, packs, own_cols),
            buf(n_kv * local, qkv_width),
            buf(chips * local, qkv_width),
            buf(chips - 1, local, qkv_width),
            buf(chips - 1, local, qkv_width),
            buf(n_kv, local, vw),
            buf(n_tp, packs, own_cols),
            buf(n_tp - 1, packs, own_cols),
            buf(n_tp, packs, own_cols),
            buf(2, rows, ff_pad),
            buf(2, chips * unit, ff_pad),
            buf(2, chips - 1, unit, ff_pad),
            buf(2, chips - 1, unit, ff_pad),
            buf(n_kv, unit, ff_pad // 256 * 128),
            buf(n_kv, unit, ff_pad - ff_pad // 256 * 128),
            buf(n_tp, packs, own_cols),
            buf(n_tp - 1, packs, own_cols),
            buf(n_kv * local, width),
            buf(n_kv * local, 2),
            buf(rows, width),
            pltpu.VMEM((rows, ff_pad - ff), F32),
            dma((10,)),
            dma((7,)),
            dma((6, n_tp - 1)),
            dma((6, n_tp - 1)),
            dma((8,)),
            dma((8,)),
            dma((11, chips - 1)),
            dma((11, chips - 1)),
            dma((3, chips)),
            dma((3, chips)),
        ],
        compiler_params=pltpu.CompilerParams(
            collective_id=0, has_side_effects=True, vmem_limit_bytes=52 * 1024 * 1024
        ),
    )(*operands)
    count = state.shape[0]
    return pl.pallas_call(
        finish_kernel,
        out_shape=(
            jax.ShapeDtypeStruct(tokens.shape, BF16),
            jax.ShapeDtypeStruct(state.shape, F32),
        ),
        in_specs=[in_vmem, in_vmem],
        out_specs=(in_hbm, in_hbm),
        scratch_shapes=[pltpu.VMEM(tokens.shape, BF16), dma((count + 1,))],
        compiler_params=pltpu.CompilerParams(vmem_limit_bytes=8 * 1024 * 1024),
    )(mixed, new_state)


def finish_kernel(mixed_ref, state_ref, mixed_out, state_out, mixed_rows, write_sem):
    count = state_ref.shape[0]
    writes = [
        pltpu.make_async_copy(state_ref.at[n], state_out.at[n], write_sem.at[n])
        for n in range(count)
    ]
    for write in writes:
        write.start()
    mixed_rows[...] = mixed_ref[...].astype(F32).reshape(mixed_rows.shape).astype(BF16)
    writes.append(pltpu.make_async_copy(mixed_rows, mixed_out, write_sem.at[count]))
    writes[-1].start()
    for write in writes:
        write.wait()


def layer(*args):
    n_kv, n_tp = lax.axis_size("kv"), lax.axis_size("tp")
    tokens, state = args[0], args[2]
    batch, span, own_cols = tokens.shape
    seqs, size, vw = state.shape
    aligned = own_cols % 128 == 0 and size % 128 == 0 and seqs == 8
    aligned = aligned and n_kv % 2 == 0 and 2 * args[7].shape[1] + 2 <= 128
    if aligned:
        return fused_layer(n_kv, n_tp, *args)
    return body(*args)


def solution(mesh):
    return jax.shard_map(
        layer,
        mesh=mesh,
        in_specs=(
            P(None, None, ("kv", "tp")),
            P(),
            P("kv", None, "tp"),
            P("kv"),
            P("kv", "tp"),
            P("kv", "tp"),
            P("kv", "tp"),
            P(),
            P(),
            P(),
            P(),
            P(),
            P("tp", "kv"),
            P("kv"),
            P("kv", "tp"),
            P("kv", "tp"),
            P("tp", "kv"),
        ),
        out_specs=(P(None, None, ("kv", "tp")), P("kv", None, "tp")),
        check_vma=False,
    )
```

```python
import jax
import jax.numpy as jnp
from jax import lax
from jax.experimental import pallas as pl
from jax.experimental.pallas import tpu as pltpu
from jax.sharding import PartitionSpec as P

MESH = pl.DeviceIdType.MESH
F32 = jnp.float32
BF16 = jnp.bfloat16

D = 4096
HEAD_DIM = 128


EPSILON = 1e-06


def unit_rows(vectors):
    return vectors * lax.rsqrt(jnp.sum(vectors * vectors, axis=-1, keepdims=True) + EPSILON)


def delta_block(queries, unit_keys, values_split, beta, log_decay, carried):
    highest = lax.Precision.HIGHEST
    seq_count, span_len, heads_here = beta.shape
    cumulative = jnp.cumsum(log_decay, axis=1)
    position = jnp.arange(span_len)
    inclusive = (position[:, None] >= position[None, :])[None, :, :, None]
    strict = (position[:, None] > position[None, :])[None, :, :, None]
    gap_matrix = cumulative[:, :, None, :] - cumulative[:, None, :, :]
    decay_matrix = jnp.where(inclusive, jnp.exp(jnp.where(inclusive, gap_matrix, 0.0)), 0.0)
    key_dots = jnp.einsum("nihd,njhd->nijh", unit_keys, unit_keys, precision=highest)
    query_dots = jnp.einsum("nihd,njhd->nijh", queries, unit_keys, precision=highest) * decay_matrix
    lower_part = jnp.where(strict, key_dots * decay_matrix * beta[:, :, None, :], 0.0)
    identity = jnp.eye(span_len, dtype=jnp.float32)
    inverse_rows = []
    for step in range(span_len):
        row_now = jnp.broadcast_to(identity[step][None, :, None], (seq_count, span_len, heads_here))
        for prior in range(step):
            row_now = row_now - lower_part[:, step, prior, :][:, None, :] * inverse_rows[prior]
        inverse_rows.append(row_now)
    inverse = jnp.stack(inverse_rows, axis=1)
    beta_value = beta[..., None] * values_split
    beta_key = (beta * jnp.exp(cumulative))[..., None] * unit_keys
    base_update = jnp.einsum("nich,nche->nihe", inverse, beta_value, precision=highest)
    key_weights = jnp.einsum("nich,nchd->nihd", inverse, beta_key, precision=highest)
    corrected = base_update - jnp.einsum("nihd,ndhe->nihe", key_weights, carried, precision=highest)
    decayed_queries = queries * jnp.exp(cumulative)[..., None]
    attended = jnp.einsum("nihd,ndhe->nihe", decayed_queries, carried, precision=highest)
    attended = attended + jnp.einsum("nijh,njhe->nihe", query_dots, corrected, precision=highest)
    block_total = cumulative[:, -1, :]
    key_tail = unit_keys * jnp.exp(block_total[:, None, :] - cumulative)[..., None]
    updated = carried * jnp.exp(block_total)[:, None, :, None]
    updated = updated + jnp.einsum("nihd,nihe->ndhe", key_tail, corrected, precision=highest)
    return (attended, updated)


def body(
    tokens,
    lengths,
    state,
    attn_gain,
    w_query,
    w_key,
    w_value,
    w_beta,
    w_alpha,
    decay_rate,
    decay_bias,
    out_gain,
    w_out,
    mix_gain,
    w_gate,
    w_up,
    w_down,
):
    kv_index = lax.axis_index("kv")
    tp_index = lax.axis_index("tp")
    kv_count = lax.axis_size("kv")
    batch_all, span_len, own_cols = tokens.shape
    row_count = batch_all * span_len
    seq_count = state.shape[0]
    local_rows = seq_count * span_len
    head_size = state.shape[1]
    heads_here = state.shape[2] // head_size
    block_width = attn_gain.shape[0]
    flat_rows = tokens.reshape(row_count, own_cols)
    live_all = (jnp.arange(span_len, dtype=jnp.int32)[None, :] < lengths[:, None]).reshape(
        row_count, 1
    )
    gathered = lax.all_gather(flat_rows, "tp", axis=1, tiled=True).astype(jnp.float32)
    squares_in = jnp.sum(gathered * gathered, axis=1)
    normed_in = (gathered * attn_gain).astype(jnp.bfloat16)
    beta_rows = lax.dynamic_slice_in_dim(w_beta, kv_index * block_width, block_width, 0)
    alpha_rows = lax.dynamic_slice_in_dim(w_alpha, kv_index * block_width, block_width, 0)
    query_part = jnp.dot(normed_in, w_query, preferred_element_type=jnp.float32)
    key_part = jnp.dot(normed_in, w_key, preferred_element_type=jnp.float32)
    value_part = jnp.dot(normed_in, w_value, preferred_element_type=jnp.float32)
    beta_part = jnp.dot(normed_in, beta_rows, preferred_element_type=jnp.float32)
    alpha_part = jnp.dot(normed_in, alpha_rows, preferred_element_type=jnp.float32)
    squares_all = lax.psum(squares_in, "kv")
    squares_own = lax.dynamic_slice_in_dim(squares_all, kv_index * local_rows, local_rows, 0)
    query_sum, key_sum, value_sum, beta_sum, alpha_sum = (
        lax.psum_scatter(
            query_part.astype(jnp.bfloat16), "kv", scatter_dimension=0, tiled=True
        ).astype(jnp.float32),
        lax.psum_scatter(
            key_part.astype(jnp.bfloat16), "kv", scatter_dimension=0, tiled=True
        ).astype(jnp.float32),
        lax.psum_scatter(
            value_part.astype(jnp.bfloat16), "kv", scatter_dimension=0, tiled=True
        ).astype(jnp.float32),
        lax.psum_scatter(
            beta_part.astype(jnp.bfloat16), "kv", scatter_dimension=0, tiled=True
        ).astype(jnp.float32),
        lax.psum_scatter(
            alpha_part.astype(jnp.bfloat16), "kv", scatter_dimension=0, tiled=True
        ).astype(jnp.float32),
    )
    row_scale = lax.rsqrt(squares_own / D + EPSILON)[:, None]
    head_start = tp_index * heads_here
    lengths_own = lax.dynamic_slice_in_dim(lengths, kv_index * seq_count, seq_count, 0)
    live_own = (jnp.arange(span_len, dtype=jnp.int32)[None, :] < lengths_own[:, None])[..., None]
    beta_heads = lax.dynamic_slice_in_dim(beta_sum, head_start, heads_here, 1) * row_scale
    alpha_heads = lax.dynamic_slice_in_dim(alpha_sum, head_start, heads_here, 1) * row_scale
    rate_here = lax.dynamic_slice_in_dim(decay_rate, head_start, heads_here, 0)
    bias_here = lax.dynamic_slice_in_dim(decay_bias, head_start, heads_here, 0)
    beta = jnp.where(
        live_own, jax.nn.sigmoid(beta_heads).reshape(seq_count, span_len, heads_here), 0.0
    )
    log_decay = -rate_here * jax.nn.softplus(alpha_heads + bias_here)
    log_decay = jnp.where(live_own, log_decay.reshape(seq_count, span_len, heads_here), 0.0)
    split_shape = (seq_count, span_len, heads_here, head_size)
    queries = unit_rows((query_sum * row_scale).reshape(split_shape)) * HEAD_DIM ** (-0.5)
    unit_keys = unit_rows((key_sum * row_scale).reshape(split_shape))
    values_split = (value_sum * row_scale).reshape(split_shape)
    carried = state.reshape(seq_count, head_size, heads_here, head_size)
    attended, updated = delta_block(queries, unit_keys, values_split, beta, log_decay, carried)
    head_out = (
        attended
        * lax.rsqrt(jnp.mean(attended * attended, axis=-1, keepdims=True) + EPSILON)
        * out_gain
    )
    head_out = head_out.astype(jnp.bfloat16).reshape(local_rows, heads_here * head_size)
    pack_rows = min((batch_all * 7 // 4 + kv_count - 1) // kv_count * kv_count, row_count)
    live_flat = live_all.reshape(row_count).astype(jnp.int32)
    slot_index = jnp.cumsum(live_flat) - 1
    picker = (
        (slot_index[None, :] == jnp.arange(pack_rows, dtype=jnp.int32)[:, None])
        & (live_flat[None, :] > 0)
    ).astype(jnp.bfloat16)
    heads_every = lax.all_gather(head_out, "kv", axis=0, tiled=True)
    packed_heads = jnp.dot(picker, heads_every, preferred_element_type=jnp.float32).astype(
        jnp.bfloat16
    )
    attn_part = jnp.dot(packed_heads, w_out, preferred_element_type=jnp.float32)
    base_rows = jnp.dot(picker, flat_rows, preferred_element_type=jnp.float32)
    attn_own = lax.psum_scatter(
        attn_part.astype(jnp.bfloat16), "tp", scatter_dimension=1, tiled=True
    ).astype(jnp.float32)
    middle = (base_rows + attn_own).astype(jnp.bfloat16)
    middle_rows = lax.all_gather(middle, "tp", axis=1, tiled=True).astype(jnp.float32)
    squares_mid = jnp.sum(middle_rows * middle_rows, axis=1)
    normed_mid = (middle_rows * mix_gain).astype(jnp.bfloat16)
    gate_part = jnp.dot(normed_mid, w_gate, preferred_element_type=jnp.float32)
    up_part = jnp.dot(normed_mid, w_up, preferred_element_type=jnp.float32)
    squares_total = lax.psum(squares_mid, "kv")
    gate_sum, up_sum = (
        lax.psum(gate_part.astype(jnp.bfloat16), "kv").astype(jnp.float32),
        lax.psum(up_part.astype(jnp.bfloat16), "kv").astype(jnp.float32),
    )
    mid_scale = lax.rsqrt(squares_total / D + EPSILON)[:, None]
    hidden = (jax.nn.silu(gate_sum * mid_scale) * (up_sum * mid_scale)).astype(jnp.bfloat16)
    down_part = jnp.dot(hidden, w_down, preferred_element_type=jnp.float32)
    down_own = lax.psum_scatter(
        down_part.astype(jnp.bfloat16), "tp", scatter_dimension=1, tiled=True
    ).astype(jnp.float32)
    result_rows = middle.astype(jnp.float32) + down_own
    result_rows = jnp.dot(
        picker.astype(jnp.float32).T,
        result_rows,
        precision=lax.Precision.HIGHEST,
        preferred_element_type=jnp.float32,
    )
    mixed = (
        jnp.where(live_all, result_rows, 0.0)
        .astype(jnp.bfloat16)
        .reshape(batch_all, span_len, own_cols)
    )
    return (mixed, updated.reshape(seq_count, head_size, heads_here * head_size))


def iota(shape, axis):
    return lax.broadcasted_iota(jnp.int32, shape, axis)


def dot(a, b):
    return jnp.dot(a, b, preferred_element_type=F32)


def dot_t(a, b):
    return lax.dot_general(a, b, (((1,), (1,)), ((), ())), preferred_element_type=F32)


def dot_exact(a, b):
    return jnp.dot(a, b, precision=lax.Precision.HIGHEST, preferred_element_type=F32)


def head_sum(x, size):
    pieces = []
    for h in range(x.shape[1] // size):
        total = jnp.sum(x[:, h * size : (h + 1) * size], axis=1, keepdims=True)
        pieces.append(jnp.broadcast_to(total, (x.shape[0], size)))
    return jnp.concatenate(pieces, axis=1)


def high_low(x):
    high = x.astype(BF16)
    return high.astype(F32), x - high.astype(F32)


class Phases:
    def __init__(self):
        self.scope = None

    def __call__(self, name):
        if self.scope is not None:
            self.scope.__exit__(None, None, None)
            self.scope = None
        if name:
            self.scope = jax.named_scope(name)
            self.scope.__enter__()


GROUPS = 4
KINDS = (0, 1, 0, 1)
STRIP = 64


def strip_groups(per):
    sizes = [per // GROUPS] * GROUPS
    for at in range(per % GROUPS):
        sizes[at] += 1
    return sizes


def layer_kernel(
    dims,
    tokens_hbm,
    lengths_hbm,
    state_hbm,
    attn_gain_hbm,
    wq_hbm,
    wk_hbm,
    wv_hbm,
    wb_hbm,
    wa_hbm,
    rate_hbm,
    bias_hbm,
    out_gain_hbm,
    wo_hbm,
    mix_gain_hbm,
    wg_hbm,
    wu_hbm,
    wd_hbm,
    mixed_ref,
    state_keep,
    state_back,
    state_far,
    tokens_ref,
    lengths_ref,
    attn_gain_ref,
    rate_ref,
    bias_ref,
    out_gain_ref,
    mix_gain_ref,
    w_qkv,
    w_beta,
    w_alpha,
    w_out,
    w_gu,
    w_down,
    tok_all,
    qkv_send,
    qkv_own,
    qkv_pair,
    qkv_near,
    qkv_near_in,
    qkv_last,
    qkv_last_in,
    head_all,
    attn_part,
    attn_recv,
    mid_all,
    sq_all,
    gu_send,
    gu_own,
    gu_pair,
    gu_near,
    gu_near_in,
    gu_last,
    gu_last_in,
    hid_all,
    down_part,
    down_recv,
    small_sem,
    load_sem,
    state_sem,
    tp_send,
    tp_recv,
    qkv_out_sem,
    qkv_in_sem,
    gu_out_sem,
    gu_in_sem,
    far_send,
    far_recv,
    fwd_send,
    fwd_recv,
    sq_sem,
):
    n_kv, n_tp, batch, span, seqs, heads, size, width, ff, packs, cap = dims
    phase = Phases()
    phase("loads")
    kv = lax.axis_index("kv")
    tp = lax.axis_index("tp")
    core = lax.rem(kv, 2)
    chip = kv // 2
    other = 1 - core
    x = lax.rem(chip, 2)
    y = chip // 2
    partner = chip * 2 + other
    chips = n_kv // 2
    slots = batch * span
    group_seqs = 2 * seqs
    local = group_seqs * span
    vw = heads * size
    half_vw = vw // 2
    pair = 2 * size
    hops = (y * 2 + 1 - x, (1 - y) * 2 + x, (1 - y) * 2 + 1 - x)
    peers = [hop * 2 + core for hop in hops]
    upper = tp // 2
    tp_peers = (3 - 3 * upper, 2 - upper, tp + 1 - 2 * lax.rem(tp, 2))

    barrier = pltpu.get_barrier_semaphore()
    for peer in [partner, *peers]:
        pl.semaphore_signal(barrier, inc=1, device_id={"kv": peer}, device_id_type=MESH)
    for peer in tp_peers:
        pl.semaphore_signal(barrier, inc=1, device_id={"tp": peer}, device_id_type=MESH)

    def move(source, dest, sem):
        copy = pltpu.make_async_copy(source, dest, sem)
        copy.start()
        return copy

    def send(source, dest, out_sem, in_sem, device):
        pltpu.make_async_remote_copy(
            src_ref=source,
            dst_ref=dest,
            send_sem=out_sem,
            recv_sem=in_sem,
            device_id=device,
            device_id_type=MESH,
        ).start()

    def drain(ref, sem):
        pltpu.make_async_copy(ref, ref, sem).wait()

    smalls = [
        move(source, dest, small_sem.at[i])
        for i, (source, dest) in enumerate(
            (
                (tokens_hbm, tokens_ref),
                (lengths_hbm, lengths_ref),
                (attn_gain_hbm, attn_gain_ref),
                (rate_hbm, rate_ref),
                (bias_hbm, bias_ref),
                (out_gain_hbm, out_gain_ref),
                (mix_gain_hbm, mix_gain_ref),
            )
        )
    ]

    for load in smalls:
        load.wait()

    phase("pick")
    lengths_row = lengths_ref[...].astype(F32)
    spread = (iota((batch, slots), 1) // span == iota((batch, slots), 0)).astype(BF16)
    length_of = dot(jnp.broadcast_to(lengths_row, (8, batch)).astype(BF16), spread)
    slot_chip = iota((8, slots), 1) // (group_seqs * span)
    slot_x, slot_y = lax.rem(slot_chip, 2), slot_chip // 2
    live_all = lax.rem(iota((8, slots), 1), span).astype(F32) < length_of
    row = iota((8, slots), 0)
    chosen = (
        (row == 0)
        | ((row == 1) & (slot_x == x))
        | ((row == 2) & (slot_x != x))
        | ((row == 3) & (slot_y == y))
        | ((row == 4) & (slot_y != y))
    )
    members = (live_all & chosen).astype(F32)
    before = (iota((slots, slots), 0) < iota((slots, slots), 1)).astype(BF16)
    ranks = jnp.where(members > 0.0, dot(members.astype(BF16), before), -1.0)
    picker = (iota((packs, slots), 0).astype(F32) == ranks[0:1, :]).astype(BF16)
    tok_all[tp] = dot(picker, tokens_ref[...]).astype(BF16)
    phase("barrier")
    pl.semaphore_wait(barrier, 1 + len(peers) + (n_tp - 1))

    def tp_start(index, source_at, dest_at):
        for peer in tp_peers:
            d = lax.rem(peer - tp + n_tp, n_tp)
            send(source_at(peer), dest_at(d), tp_send.at[index], tp_recv.at[index], {"tp": peer})

    def tp_finish(index, sent, received):
        drain(received, tp_recv.at[index])
        drain(sent, tp_send.at[index])

    rest = n_tp - 1
    phase("token_send")
    tp_start(0, lambda peer: tok_all.at[tp], lambda d: tok_all.at[tp])
    phase("big_loads")
    def block(index, extent):
        return pl.ds(pl.multiple_of(index * extent, extent), extent)

    loads = [
        move(wk_hbm, w_qkv.at[1], load_sem.at[1]),
        move(wq_hbm, w_qkv.at[0], load_sem.at[0]),
        move(wv_hbm, w_qkv.at[2], load_sem.at[2]),
        move(wb_hbm.at[:, block(kv, width)], w_beta, load_sem.at[3]),
        move(wa_hbm.at[:, block(kv, width)], w_alpha, load_sem.at[4]),
        move(state_hbm.at[:, :, block(core, half_vw)], state_keep, state_sem.at[0]),
        move(wo_hbm, w_out, load_sem.at[5]),
    ]
    strips = ff // STRIP
    per = (strips + 3) // 4
    sizes = strip_groups(per)
    starts = [sum(sizes[:g]) for g in range(GROUPS)]
    for c in range(2):
        for g in range(GROUPS):
            for yy in range(2):
                source = (c * 2 + yy) * per + starts[g]
                count = min(sizes[g], strips - source)
                dest = c * 2 * per + 2 * starts[g] + yy * sizes[g]
                if count > 0:
                    move(wg_hbm.at[source : source + count], w_gu.at[dest : dest + count, 0], load_sem.at[6])
                    move(wu_hbm.at[source : source + count], w_gu.at[dest : dest + count, 1], load_sem.at[7])
    lead = sizes[0] + sizes[1]
    piece = (lead * STRIP + 127) // 128 * 128
    for i in range(4):
        low = i * per * STRIP
        for k, (begin, end) in enumerate(((0, lead * STRIP), (lead * STRIP, per * STRIP))):
            stop = min(low + end, ff)
            count = stop - low - begin
            dest = (k * 4 + i) * piece
            if count > 0:
                move(wd_hbm.at[low + begin : stop, :], w_down.at[dest : dest + count, :], load_sem.at[8])
            if count < piece:
                fill = max(count, 0)
                w_down[dest + fill : dest + piece, :] = jnp.zeros((piece - fill, w_down.shape[1]), BF16)
    for at in range(strips, 4 * per):
        w_gu[at] = jnp.zeros(w_gu.shape[1:], BF16)
    phase("state_send")
    send(
        state_hbm.at[:, :, block(other, half_vw)],
        state_far,
        state_sem.at[1],
        state_sem.at[2],
        {"kv": partner},
    )
    half_rows = [
        (iota((cap, slots), 0).astype(F32) == ranks[1 + i : 2 + i, :]).astype(BF16) for i in range(4)
    ]
    keep_rows, give_rows = half_rows[0::2], half_rows[1::2]
    give = [dot_t(rows, picker).astype(BF16) for rows in give_rows]

    def slot_of(q, c, shape, axis):
        r = iota(shape, axis)
        s = lax.rem(r, group_seqs)
        seq = q * group_seqs + lax.rem(c + s // seqs, 2) * seqs + lax.rem(s, seqs)
        return seq * span + r // group_seqs

    def place(q):
        return (iota((local, slots), 1) == slot_of(q, core, (local, slots), 0)).astype(BF16)

    own_place = place(chip)
    settle = []
    for kind in range(2):
        both = jnp.concatenate([own_place, place(hops[1 - kind])], axis=0)
        known = jnp.concatenate([picker, keep_rows[kind]], axis=0)
        settle.append(dot_t(both, known).astype(BF16))

    def order(c):
        column = iota((slots, slots), 1)
        r = lax.rem(column, local)
        s = lax.rem(r, group_seqs)
        seq = column // local * group_seqs + lax.rem(c + s // seqs, 2) * seqs + lax.rem(s, seqs)
        return (iota((slots, slots), 0) == seq * span + r // group_seqs).astype(BF16)

    pick_heads = [dot(picker, order(c)).astype(BF16) for c in range(2)]
    n_heads_all = wb_hbm.shape[0]
    core_heads = heads // 2
    first_head = tp * heads + core * core_heads
    per_head = (
        iota((n_heads_all, half_vw), 0) == iota((n_heads_all, half_vw), 1) // size + first_head
    ).astype(F32)
    rate = dot_exact(jnp.broadcast_to(rate_ref[...], (8, n_heads_all)), per_head)[0:1, :]
    bias = dot_exact(jnp.broadcast_to(bias_ref[...], (8, n_heads_all)), per_head)[0:1, :]
    slot_seq = slot_of(chip, core, (local, batch), 0) // span
    own_len = jnp.sum(
        jnp.where(iota((local, batch), 1) == slot_seq, lengths_row, 0.0), axis=1, keepdims=True
    )
    live = (iota((local, 1), 0) // group_seqs).astype(F32) < own_len
    for load in loads[0:5]:
        load.wait()

    phase("token_wait")
    tp_finish(0, tok_all.at[0:rest], tok_all.at[0:rest])
    phase("norm")
    gathered = jnp.concatenate([tok_all[j] for j in range(n_tp)], axis=1).astype(F32)
    squares = jnp.sum(gathered * gathered, axis=1, keepdims=True)
    normed = (gathered * attn_gain_ref[...]).astype(BF16)
    square_high, square_low = high_low(squares)
    extra = jnp.concatenate(
        [
            dot_t(normed, w_beta[...]),
            dot_t(normed, w_alpha[...]),
            square_high,
            square_low,
            jnp.zeros((packs, 128 - 2 * n_heads_all - 2), F32),
        ],
        axis=1,
    )

    widths = (128 + 2 * pair, 2 * pair, pair, pair)
    offsets = [sum(widths[:g]) for g in range(GROUPS + 1)]

    def qkv_cols(g):
        return slice(offsets[g], offsets[g + 1])

    def qkv_compute(g, c, dest):
        lanes = block(c * 2 + KINDS[g], pair)
        at = offsets[g]
        if g == 0:
            dest[:, 0:128] = extra.astype(BF16)
            at = 128
        for m in (1, 0) if g < 2 else (2,):
            dest[:, at : at + pair] = dot(normed, w_qkv[m, :, lanes]).astype(BF16)
            at += pair

    def qkv_give(g):
        phase(f"qkv_give{g}")
        qkv_compute(g, other, qkv_send)
        cols = qkv_cols(g)
        send(
            qkv_send.at[:, cols],
            qkv_pair.at[:, cols],
            qkv_out_sem.at[0],
            qkv_in_sem.at[0, g],
            {"kv": partner},
        )

    def qkv_near_step(g):
        phase(f"qkv_near{g}")
        cols, kind = qkv_cols(g), KINDS[g]
        drain(qkv_pair.at[:, cols], qkv_in_sem.at[0, g])
        both = (qkv_own[:, cols].astype(F32) + qkv_pair[:, cols].astype(F32)).astype(BF16)
        qkv_own[:, cols] = both
        qkv_near[:, cols] = dot(give[kind], both).astype(BF16)
        send(
            qkv_near.at[:, cols],
            qkv_near_in.at[:, cols],
            qkv_out_sem.at[1],
            qkv_in_sem.at[1, g],
            {"kv": peers[kind]},
        )

    settled = [None] * GROUPS

    def qkv_last_step(g):
        phase(f"qkv_last{g}")
        cols, kind = qkv_cols(g), KINDS[g]
        drain(qkv_near_in.at[:, cols], qkv_in_sem.at[1, g])
        known = jnp.concatenate([qkv_own[:, cols], qkv_near_in[:, cols]], axis=0)
        both = dot(settle[kind], known)
        settled[g] = both[0:local, :]
        qkv_last[:, cols] = both[local:, :].astype(BF16)
        send(
            qkv_last.at[:, cols],
            qkv_last_in.at[:, cols],
            qkv_out_sem.at[2],
            qkv_in_sem.at[2, g],
            {"kv": peers[1 - kind]},
        )

    def qkv_total(g):
        phase(f"qkv_total{g}")
        cols = qkv_cols(g)
        drain(qkv_last_in.at[:, cols], qkv_in_sem.at[2, g])
        return settled[g] + qkv_last_in[:, cols].astype(F32)

    qkv_give(0)
    qkv_compute(0, core, qkv_own)
    qkv_give(1)
    qkv_give(2)
    qkv_near_step(0)
    qkv_compute(1, core, qkv_own)
    qkv_give(3)
    qkv_near_step(1)
    qkv_compute(2, core, qkv_own)
    qkv_near_step(2)
    qkv_compute(3, core, qkv_own)
    qkv_near_step(3)
    phase("state_low")
    loads[5].wait()
    drain(state_far, state_sem.at[2])
    state_low = jnp.concatenate(
        [state_keep[...].reshape(seqs * size, half_vw), state_far[...].reshape(seqs * size, half_vw)],
        axis=0,
    ).astype(BF16)
    for g in range(GROUPS):
        qkv_last_step(g)

    def token(values, t):
        return values[t * group_seqs : (t + 1) * group_seqs, :]

    def blocked(values):
        keep = lax.rem(iota(values.shape, 0), group_seqs)
        return jnp.concatenate(
            [jnp.where(keep == n, values, 0.0).astype(BF16) for n in range(group_seqs)], axis=1
        )

    totals = [qkv_total(0), None, None, None]
    phase("gates")
    extra = totals[0][:, 0:128]
    lane = iota((local, 128), 1)
    sq_lane = (lane == 2 * n_heads_all) | (lane == 2 * n_heads_all + 1)
    sq_own = jnp.sum(jnp.where(sq_lane, extra, 0.0), axis=1, keepdims=True)
    row_scale = lax.rsqrt(sq_own / D + EPSILON)
    scaled_extra = jnp.where(sq_lane, 0.0, extra * row_scale)
    lane_of = iota((128, half_vw), 0)
    head_of = iota((128, half_vw), 1) // size + first_head
    beta_pre = dot_exact(scaled_extra, (lane_of == head_of).astype(F32))
    alpha_pre = dot_exact(scaled_extra, (lane_of == head_of + n_heads_all).astype(F32))
    beta = jnp.where(live, 1.0 / (1.0 + jnp.exp(-beta_pre)), 0.0)
    pre = alpha_pre + bias
    softplus = jnp.maximum(pre, 0.0) + jnp.log(1.0 + jnp.exp(-jnp.abs(pre)))
    log_decay = jnp.where(live, -rate * softplus, 0.0)
    cumulative = [token(log_decay, 0)]
    for t in range(1, span):
        cumulative.append(cumulative[-1] + token(log_decay, t))

    def keyed(p, total):
        cols = slice(p * pair, (p + 1) * pair)
        k_raw = total[:, 0:pair] * row_scale
        keys = k_raw * lax.rsqrt(head_sum(k_raw * k_raw, size) + EPSILON)
        q_raw = total[:, pair : 2 * pair] * row_scale
        queries = q_raw * lax.rsqrt(head_sum(q_raw * q_raw, size) + EPSILON) * size ** (-0.5)
        products = []
        for h in range(2):
            at = slice(h * size, (h + 1) * size)
            both = jnp.concatenate([keys[:, at], queries[:, at]], axis=0)
            products.append(dot(blocked(both), state_low[:, p * pair + h * size : p * pair + (h + 1) * size]))
        products = jnp.concatenate(products, axis=1)
        sums = [c[:, cols] for c in cumulative]
        grown = [jnp.exp(c) for c in sums]
        key_weights = [
            [
                jnp.exp(sums[t] - sums[u]) * head_sum(token(keys, t) * token(keys, u), size)
                for u in range(t)
            ]
            for t in range(span)
        ]
        query_weights = [
            [
                jnp.exp(sums[t] - sums[u]) * head_sum(token(queries, t) * token(keys, u), size)
                for u in range(t + 1)
            ]
            for t in range(span)
        ]
        from_keys = [grown[t] * token(products, t) for t in range(span)]
        from_queries = [grown[t] * token(products, span + t) for t in range(span)]
        return keys, sums, key_weights, query_weights, from_keys, from_queries

    gain = jnp.concatenate([out_gain_ref[...]] * 2, axis=1)

    def solved(p, keyed_pair, total):
        keys, sums, key_weights, query_weights, from_keys, from_queries = keyed_pair
        cols = slice(p * pair, (p + 1) * pair)
        values = total * row_scale
        updates, attended = [], []
        for t in range(span):
            update = token(values, t) - from_keys[t]
            for u in range(t):
                update = update - key_weights[t][u] * updates[u]
            updates.append(token(beta, t)[:, cols] * update)
            result = from_queries[t]
            for u in range(t + 1):
                result = result + query_weights[t][u] * updates[u]
            attended.append(result)
        attended = jnp.concatenate(attended, axis=0)
        out = attended * lax.rsqrt(head_sum(attended * attended, size) / size + EPSILON) * gain
        return out.astype(BF16), updates

    def gather_start(index, piece_at):
        mine = piece_at(chip)
        for kind in (2, 0, 1):
            send(mine, mine, far_send.at[index], far_recv.at[index, kind], {"kv": peers[kind]})
        send(mine, mine, fwd_send.at[index], fwd_recv.at[index], {"kv": partner})

    def gather_pass(index, piece_at):
        for kind in range(3):
            got = piece_at(hops[kind])
            drain(got, far_recv.at[index, kind])
            send(got, got, fwd_send.at[index], fwd_recv.at[index], {"kv": partner})

    def gather_finish(index, sent_far, sent, received):
        drain(received, fwd_recv.at[index])
        drain(sent_far, far_send.at[index])
        drain(sent, fwd_send.at[index])

    def head_lanes(c, p):
        return block(c * 2 + p, pair)

    def head_piece(p):
        return lambda q: head_all.at[q, :, head_lanes(core, p)]

    def head_finish(p):
        gather_finish(
            p,
            head_all.at[0:3, :, head_lanes(core, p)],
            head_all.at[:, :, head_lanes(core, p)],
            head_all.at[:, :, head_lanes(other, p)],
        )

    pairs = [keyed(0, totals[0][:, 128:])]
    totals[1] = qkv_total(1)
    phase("keyed1")
    pairs.append(keyed(1, totals[1]))
    updates = []
    for p in range(2):
        total = qkv_total(2 + p)
        phase(f"solve{p}")
        out, update = solved(p, pairs[p], total)
        head_all[chip, :, head_lanes(core, p)] = out
        updates.append(update)
        phase(f"head_send{p}")
        gather_start(p, head_piece(p))

    def update_state(p):
        keys, sums = pairs[p][0], pairs[p][1]
        final = sums[-1]
        tails = jnp.concatenate(
            [token(keys, t) * jnp.exp(final - sums[t]) for t in range(span)], axis=0
        )
        all_updates = jnp.concatenate(updates[p], axis=0).astype(BF16)
        decay_all = jnp.exp(final)
        for h in range(2):
            at = slice(h * size, (h + 1) * size)
            to = slice(p * pair + h * size, p * pair + (h + 1) * size)
            rank = lax.dot_general(
                blocked(tails[:, at]),
                all_updates[:, at],
                (((0,), (0,)), ((), ())),
                preferred_element_type=F32,
            )
            for n in range(group_seqs):
                ref = state_keep if n < seqs else state_far
                i = n % seqs
                ref[i, :, to] = (
                    ref[i, :, to] * decay_all[n : n + 1, at] + rank[n * size : (n + 1) * size, :]
                )

    phase("update0")
    update_state(0)
    phase("head_pass0")
    gather_pass(0, head_piece(0))
    phase("update1")
    update_state(1)
    phase("head_pass1")
    gather_pass(1, head_piece(1))
    head_finish(0)
    head_finish(1)
    phase("state_return")
    send(state_far, state_back, state_sem.at[3], state_sem.at[4], {"kv": partner})
    phase("w_out")
    heads_every = head_all[...].reshape(slots, vw)
    packed = jnp.concatenate(
        [dot(pick_heads[c], heads_every[:, c * half_vw : (c + 1) * half_vw]) for c in range(2)],
        axis=1,
    ).astype(BF16)
    loads[6].wait()
    part = dot(packed, w_out[...])
    own_cols = tokens_ref.shape[1]

    def tp_scatter_start(index, part, part_ref, recv_ref, group):
        for j in range(n_tp):
            part_ref[j, group, :] = part[group, j * own_cols : (j + 1) * own_cols].astype(BF16)
        phase(f"scatter{index}")
        tp_start(
            index, lambda peer: part_ref.at[peer, group, :], lambda d: recv_ref.at[d - 1, group, :]
        )

    def tp_scatter_finish(index, part_ref, recv_ref, group):
        tp_finish(index, part_ref.at[0:rest, group, :], recv_ref.at[:, group, :])
        total = part_ref[tp, group, :].astype(F32)
        for d in range(1, n_tp):
            total = total + recv_ref[d - 1, group, :].astype(F32)
        return total

    cut = packs // 32 * 16
    groups = (slice(0, cut), slice(cut, packs))
    for i, group in enumerate(groups):
        tp_scatter_start(1 + i, part, attn_part, attn_recv, group)
    own_tokens = dot(picker, tokens_ref[...])
    for i, group in enumerate(groups):
        phase(f"middle{i}")
        middle = (own_tokens[group, :] + tp_scatter_finish(1 + i, attn_part, attn_recv, group)).astype(BF16)
        mid_all[tp, group, :] = middle
        phase(f"mid_send{i}")
        tp_start(3 + i, lambda peer: mid_all.at[tp, group, :], lambda d: mid_all.at[tp, group, :])
    phase("mid_wait")
    drain(wg_hbm, load_sem.at[6])
    drain(wu_hbm, load_sem.at[7])
    for i, group in enumerate(groups):
        tp_finish(3 + i, mid_all.at[0:rest, group, :], mid_all.at[0:rest, group, :])
    phase("norm_mid")
    middle_rows = jnp.concatenate([mid_all[j] for j in range(n_tp)], axis=1).astype(F32)
    normed_mid = (middle_rows * mix_gain_ref[...]).astype(BF16)
    rows_half = packs // 2

    def strip_cols(g):
        return slice(starts[g] * 128, (starts[g] + sizes[g]) * 128)

    def gu_compute(g, c, dest):
        count = 2 * sizes[g]
        weights = w_gu[pl.ds(c * (2 * per) + 2 * starts[g], count)].reshape(count * 128, width)
        product = dot_t(normed_mid, weights)
        wide = sizes[g] * 128
        for hh in range(2):
            for yy in range(2):
                dest[hh, yy, :, strip_cols(g)] = product[
                    hh * rows_half : (hh + 1) * rows_half, yy * wide : (yy + 1) * wide
                ].astype(BF16)

    def gu_give(g):
        phase(f"gu_give{g}")
        gu_compute(g, other, gu_send)
        cols = strip_cols(g)
        send(
            gu_send.at[:, :, :, cols],
            gu_pair.at[:, :, :, cols],
            gu_out_sem.at[0],
            gu_in_sem.at[0, g],
            {"kv": partner},
        )

    def gu_pairs(h, yy, cols):
        return gu_own[h, yy, :, cols].astype(F32) + gu_pair[h, yy, :, cols].astype(F32)

    def gu_near_step(g):
        phase(f"gu_near{g}")
        cols, kind = strip_cols(g), KINDS[g]
        drain(gu_pair.at[:, :, :, cols], gu_in_sem.at[0, g])
        for i in range(2):
            at = (1 - x, i) if kind == 0 else (i, 1 - y)
            gu_near[i, :, cols] = gu_pairs(*at, cols).astype(BF16)
        send(
            gu_near.at[:, :, cols],
            gu_near_in.at[:, :, cols],
            gu_out_sem.at[1],
            gu_in_sem.at[1, g],
            {"kv": peers[kind]},
        )

    def gu_last_step(g):
        phase(f"gu_last{g}")
        cols, kind = strip_cols(g), KINDS[g]
        drain(gu_near_in.at[:, :, cols], gu_in_sem.at[1, g])
        at = (x, 1 - y) if kind == 0 else (1 - x, y)
        inner = 1 - y if kind == 0 else 1 - x
        gu_last[:, cols] = (gu_pairs(*at, cols) + gu_near_in[inner, :, cols].astype(F32)).astype(BF16)
        send(
            gu_last.at[:, cols],
            gu_last_in.at[:, cols],
            gu_out_sem.at[2],
            gu_in_sem.at[2, g],
            {"kv": peers[1 - kind]},
        )

    def gu_total(g):
        phase(f"gu_total{g}")
        cols, kind = strip_cols(g), KINDS[g]
        drain(gu_last_in.at[:, cols], gu_in_sem.at[2, g])
        inner = y if kind == 0 else x
        return (
            gu_pairs(x, y, cols)
            + gu_near_in[inner, :, cols].astype(F32)
            + gu_last_in[:, cols].astype(F32)
        )

    gu_give(0)
    gu_compute(0, core, gu_own)
    gu_give(1)
    gu_near_step(0)
    gu_compute(1, core, gu_own)
    gu_give(2)
    gu_near_step(1)
    gu_compute(2, core, gu_own)
    gu_give(3)
    gu_near_step(2)
    gu_compute(3, core, gu_own)
    gu_near_step(3)
    phase("squares")
    squares = jnp.sum(middle_rows * middle_rows, axis=1, keepdims=True)
    same = iota((packs, 128), 0) == iota((packs, 128), 1)
    sq_all[kv] = jnp.sum(jnp.where(same, squares, 0.0), axis=0, keepdims=True)
    for step in range(1, n_kv):
        peer = lax.rem(kv + step, n_kv)
        send(sq_all.at[kv], sq_all.at[kv], sq_sem.at[0], sq_sem.at[1], {"kv": peer})
    for g in range(GROUPS):
        gu_last_step(g)
    phase("scale_mid")
    drain(sq_all.at[0 : n_kv - 1], sq_sem.at[1])
    drain(sq_all.at[0 : n_kv - 1], sq_sem.at[0])
    sq_row = sq_all[0]
    for j in range(1, n_kv):
        sq_row = sq_row + sq_all[j]
    own_row = iota((rows_half, 128), 0) + x * rows_half == iota((rows_half, 128), 1)
    sq_mid = jnp.sum(jnp.where(own_row, sq_row, 0.0), axis=1, keepdims=True)
    mid_scale = lax.rsqrt(sq_mid / D + EPSILON)
    lane = iota((rows_half, 128), 1)

    def hidden_of(parts):
        wide = jnp.concatenate(parts, axis=1) * mid_scale
        pieces = []
        for at in range(0, piece, 128):
            a = wide[:, 2 * at : 2 * at + 128]
            if 2 * at + 256 <= wide.shape[1]:
                b = wide[:, 2 * at + 128 : 2 * at + 256]
            else:
                b = jnp.zeros_like(a)
            gate = jnp.where(lane < STRIP, a, pltpu.roll(b, STRIP, 1))
            up = jnp.where(lane < STRIP, pltpu.roll(a, STRIP, 1), b)
            pieces.append(gate / (1.0 + jnp.exp(-gate)) * up)
        return jnp.concatenate(pieces, axis=1).astype(BF16)

    def hid_piece(k):
        return lambda q: hid_all.at[core, q, :, k * piece : (k + 1) * piece]

    def hid_start(k, g):
        lanes = slice(k * piece, (k + 1) * piece)
        hid_all[core, chip, :, lanes] = hidden_of([gu_total(g), gu_total(g + 1)])
        phase(f"hid_send{k}")
        gather_start(2 + k, hid_piece(k))

    def hid_finish(k):
        lanes = slice(k * piece, (k + 1) * piece)
        gather_finish(
            2 + k,
            hid_all.at[core, 0:3, :, lanes],
            hid_all.at[core, :, :, lanes],
            hid_all.at[other, :, :, lanes],
        )

    def down(k):
        lanes = slice(k * piece, (k + 1) * piece)
        hidden = jnp.concatenate(
            [
                jnp.concatenate(
                    [hid_all[c, 2 * yy + xx, :, lanes].astype(F32) for xx in range(2)], axis=0
                )
                for c in range(2)
                for yy in range(2)
            ],
            axis=1,
        ).astype(BF16)
        return dot(hidden, w_down[k * 4 * piece : (k + 1) * 4 * piece, :])

    hid_start(0, 0)
    hid_start(1, 2)
    phase("hid_pass0")
    gather_pass(2, hid_piece(0))
    drain(wd_hbm, load_sem.at[8])
    hid_finish(0)
    phase("down0")
    part = down(0)
    phase("hid_pass1")
    gather_pass(3, hid_piece(1))
    hid_finish(1)
    phase("down1")
    part = part + down(1)
    every = slice(0, packs)
    tp_scatter_start(5, part, down_part, down_recv, every)
    phase("drains")
    drain(qkv_send, qkv_out_sem.at[0])
    drain(qkv_near, qkv_out_sem.at[1])
    drain(qkv_last, qkv_out_sem.at[2])
    drain(gu_send, gu_out_sem.at[0])
    drain(gu_near, gu_out_sem.at[1])
    drain(gu_last, gu_out_sem.at[2])
    drain(state_far, state_sem.at[1])
    drain(state_far, state_sem.at[3])
    drain(state_back, state_sem.at[4])
    phase("down_wait")
    total = tp_scatter_finish(5, down_part, down_recv, every)
    phase("result")
    result = (mid_all[tp].astype(F32) + total).astype(BF16)
    mixed_ref[...] = lax.dot_general(
        picker, result, (((0,), (0,)), ((), ())), preferred_element_type=F32
    ).astype(BF16)
    phase(None)


def fused_layer(n_kv, n_tp, *args):
    tokens, lengths, state, attn_gain, w_query = args[:5]
    w_beta, w_out, w_gate = args[7], args[12], args[14]
    batch, span, own_cols = tokens.shape
    seqs, size, vw = state.shape
    heads = vw // size
    width = attn_gain.shape[0]
    ff = w_gate.shape[1]
    pack = min(batch * 7 // 4, batch * span)
    packs = (pack + 15) // 16 * 16
    half = batch // 2
    cap = (min(half * span, pack - half) + 15) // 16 * 16
    local = 2 * seqs * span
    chips = n_kv // 2
    strips = ff // STRIP
    per = (strips + 3) // 4
    sizes = strip_groups(per)
    piece = ((sizes[0] + sizes[1]) * STRIP + 127) // 128 * 128
    qkv_width = 128 + 3 * vw // 2
    rows_half = packs // 2
    strip_width = per * 128
    dims = (n_kv, n_tp, batch, span, seqs, heads, size, width, ff, packs, cap)
    operands = list(args)
    operands[0] = tokens.reshape(batch * span, own_cols)
    for at in (1, 3, 9, 10, 11, 13):
        operands[at] = operands[at].reshape(1, -1)
    for at in (7, 8):
        operands[at] = operands[at].T
    for at in (14, 15):
        operands[at] = operands[at].T.reshape(strips, STRIP, width)
    in_vmem = pl.BlockSpec(memory_space=pltpu.VMEM)
    in_hbm = pl.BlockSpec(memory_space=pltpu.HBM)
    dma = pltpu.SemaphoreType.DMA

    def buf(*shape):
        return pltpu.VMEM(shape, BF16)

    half_state = (seqs, size, vw // 2)
    mixed, keep, back = pl.pallas_call(
        lambda *refs: layer_kernel(dims, *refs),
        out_shape=(
            pltpu.VMEM((batch * span, own_cols), BF16),
            pltpu.VMEM(half_state, F32),
            pltpu.VMEM(half_state, F32),
        ),
        in_specs=[in_hbm] * len(operands),
        out_specs=(in_vmem, in_vmem, in_vmem),
        scratch_shapes=[
            pltpu.VMEM(half_state, F32),
            buf(batch * span, own_cols),
            pltpu.VMEM((1, batch), jnp.int32),
            pltpu.VMEM((1, width), F32),
            pltpu.VMEM((1, args[9].shape[0]), F32),
            pltpu.VMEM((1, args[10].shape[0]), F32),
            pltpu.VMEM((1, size), F32),
            pltpu.VMEM((1, width), F32),
            buf(3, width, vw),
            buf(w_beta.shape[1], width),
            buf(w_beta.shape[1], width),
            buf(*w_out.shape),
            buf(4 * per, 2, STRIP, width),
            buf(8 * piece, w_out.shape[1]),
            buf(n_tp, packs, own_cols),
            buf(packs, qkv_width),
            buf(packs, qkv_width),
            buf(packs, qkv_width),
            buf(cap, qkv_width),
            buf(cap, qkv_width),
            buf(local, qkv_width),
            buf(local, qkv_width),
            buf(chips, local, vw),
            buf(n_tp, packs, own_cols),
            buf(n_tp - 1, packs, own_cols),
            buf(n_tp, packs, own_cols),
            pltpu.VMEM((n_kv, 1, 128), F32),
            buf(2, 2, rows_half, strip_width),
            buf(2, 2, rows_half, strip_width),
            buf(2, 2, rows_half, strip_width),
            buf(2, rows_half, strip_width),
            buf(2, rows_half, strip_width),
            buf(rows_half, strip_width),
            buf(rows_half, strip_width),
            buf(2, chips, rows_half, 2 * piece),
            buf(n_tp, packs, own_cols),
            buf(n_tp - 1, packs, own_cols),
            dma((7,)),
            dma((9,)),
            dma((5,)),
            dma((6,)),
            dma((6,)),
            dma((3,)),
            dma((3, GROUPS)),
            dma((3,)),
            dma((3, GROUPS)),
            dma((4,)),
            dma((4, 3)),
            dma((4,)),
            dma((4,)),
            dma((2,)),
        ],
        compiler_params=pltpu.CompilerParams(
            collective_id=0, has_side_effects=True, vmem_limit_bytes=52 * 1024 * 1024
        ),
    )(*operands)
    return pl.pallas_call(
        finish_kernel,
        out_shape=(
            jax.ShapeDtypeStruct(tokens.shape, BF16),
            jax.ShapeDtypeStruct(state.shape, F32),
        ),
        in_specs=[in_vmem, in_vmem, in_vmem],
        out_specs=(in_hbm, in_hbm),
        scratch_shapes=[pltpu.VMEM(tokens.shape, BF16), dma((9,))],
        compiler_params=pltpu.CompilerParams(vmem_limit_bytes=4 * 1024 * 1024),
    )(mixed, keep, back)


def finish_kernel(mixed_ref, keep_ref, back_ref, mixed_out, state_out, mixed_rows, write_sem):
    core = lax.rem(lax.axis_index("kv"), 2)
    seqs, _, half = keep_ref.shape
    writes = []
    for i, (ref, at) in enumerate(((keep_ref, core), (back_ref, 1 - core))):
        lanes = pl.ds(pl.multiple_of(at * half, half), half)
        for j in range(4):
            rows = slice(j * seqs // 4, (j + 1) * seqs // 4)
            writes.append(
                pltpu.make_async_copy(
                    ref.at[rows], state_out.at[rows, :, lanes], write_sem.at[4 * i + j]
                )
            )
    for write in writes:
        write.start()
    mixed_rows[...] = mixed_ref[...].astype(F32).reshape(mixed_rows.shape).astype(BF16)
    writes.append(pltpu.make_async_copy(mixed_rows, mixed_out, write_sem.at[8]))
    writes[-1].start()
    for write in writes:
        write.wait()


def layer(*args):
    n_kv, n_tp = lax.axis_size("kv"), lax.axis_size("tp")
    tokens, state, w_gate = args[0], args[2], args[14]
    batch, span, own_cols = tokens.shape
    seqs, size, vw = state.shape
    pack = min(batch * 7 // 4, batch * span)
    aligned = own_cols % 128 == 0 and size % 128 == 0 and seqs == 8
    aligned = aligned and n_kv == 8 and n_tp == 4 and 2 * args[7].shape[1] + 2 <= 128
    aligned = aligned and pack % 16 == 0 and pack <= 128 and vw == 8 * size
    aligned = aligned and w_gate.shape[1] % STRIP == 0
    if aligned:
        return fused_layer(n_kv, n_tp, *args)
    return body(*args)


def solution(mesh):
    return jax.shard_map(
        layer,
        mesh=mesh,
        in_specs=(
            P(None, None, ("kv", "tp")),
            P(),
            P("kv", None, "tp"),
            P("kv"),
            P("kv", "tp"),
            P("kv", "tp"),
            P("kv", "tp"),
            P(),
            P(),
            P(),
            P(),
            P(),
            P("tp", "kv"),
            P("kv"),
            P("kv", "tp"),
            P("kv", "tp"),
            P("tp", "kv"),
        ),
        out_specs=(P(None, None, ("kv", "tp")), P("kv", None, "tp")),
        check_vma=False,
    )
```

```python
import jax
import jax.numpy as jnp
from jax import lax
from jax.experimental import pallas as pl
from jax.experimental.pallas import tpu as pltpu
from jax.sharding import PartitionSpec as P

MESH = pl.DeviceIdType.MESH
F32 = jnp.float32
BF16 = jnp.bfloat16

D = 4096
HEAD_DIM = 128


EPSILON = 1e-06


def unit_rows(vectors):
    return vectors * lax.rsqrt(jnp.sum(vectors * vectors, axis=-1, keepdims=True) + EPSILON)


def delta_block(queries, unit_keys, values_split, beta, log_decay, carried):
    highest = lax.Precision.HIGHEST
    seq_count, span_len, heads_here = beta.shape
    cumulative = jnp.cumsum(log_decay, axis=1)
    position = jnp.arange(span_len)
    inclusive = (position[:, None] >= position[None, :])[None, :, :, None]
    strict = (position[:, None] > position[None, :])[None, :, :, None]
    gap_matrix = cumulative[:, :, None, :] - cumulative[:, None, :, :]
    decay_matrix = jnp.where(inclusive, jnp.exp(jnp.where(inclusive, gap_matrix, 0.0)), 0.0)
    key_dots = jnp.einsum("nihd,njhd->nijh", unit_keys, unit_keys, precision=highest)
    query_dots = jnp.einsum("nihd,njhd->nijh", queries, unit_keys, precision=highest) * decay_matrix
    lower_part = jnp.where(strict, key_dots * decay_matrix * beta[:, :, None, :], 0.0)
    identity = jnp.eye(span_len, dtype=jnp.float32)
    inverse_rows = []
    for step in range(span_len):
        row_now = jnp.broadcast_to(identity[step][None, :, None], (seq_count, span_len, heads_here))
        for prior in range(step):
            row_now = row_now - lower_part[:, step, prior, :][:, None, :] * inverse_rows[prior]
        inverse_rows.append(row_now)
    inverse = jnp.stack(inverse_rows, axis=1)
    beta_value = beta[..., None] * values_split
    beta_key = (beta * jnp.exp(cumulative))[..., None] * unit_keys
    base_update = jnp.einsum("nich,nche->nihe", inverse, beta_value, precision=highest)
    key_weights = jnp.einsum("nich,nchd->nihd", inverse, beta_key, precision=highest)
    corrected = base_update - jnp.einsum("nihd,ndhe->nihe", key_weights, carried, precision=highest)
    decayed_queries = queries * jnp.exp(cumulative)[..., None]
    attended = jnp.einsum("nihd,ndhe->nihe", decayed_queries, carried, precision=highest)
    attended = attended + jnp.einsum("nijh,njhe->nihe", query_dots, corrected, precision=highest)
    block_total = cumulative[:, -1, :]
    key_tail = unit_keys * jnp.exp(block_total[:, None, :] - cumulative)[..., None]
    updated = carried * jnp.exp(block_total)[:, None, :, None]
    updated = updated + jnp.einsum("nihd,nihe->ndhe", key_tail, corrected, precision=highest)
    return (attended, updated)


def body(
    tokens,
    lengths,
    state,
    attn_gain,
    w_query,
    w_key,
    w_value,
    w_beta,
    w_alpha,
    decay_rate,
    decay_bias,
    out_gain,
    w_out,
    mix_gain,
    w_gate,
    w_up,
    w_down,
):
    kv_index = lax.axis_index("kv")
    tp_index = lax.axis_index("tp")
    kv_count = lax.axis_size("kv")
    batch_all, span_len, own_cols = tokens.shape
    row_count = batch_all * span_len
    seq_count = state.shape[0]
    local_rows = seq_count * span_len
    head_size = state.shape[1]
    heads_here = state.shape[2] // head_size
    block_width = attn_gain.shape[0]
    flat_rows = tokens.reshape(row_count, own_cols)
    live_all = (jnp.arange(span_len, dtype=jnp.int32)[None, :] < lengths[:, None]).reshape(
        row_count, 1
    )
    gathered = lax.all_gather(flat_rows, "tp", axis=1, tiled=True).astype(jnp.float32)
    squares_in = jnp.sum(gathered * gathered, axis=1)
    normed_in = (gathered * attn_gain).astype(jnp.bfloat16)
    beta_rows = lax.dynamic_slice_in_dim(w_beta, kv_index * block_width, block_width, 0)
    alpha_rows = lax.dynamic_slice_in_dim(w_alpha, kv_index * block_width, block_width, 0)
    query_part = jnp.dot(normed_in, w_query, preferred_element_type=jnp.float32)
    key_part = jnp.dot(normed_in, w_key, preferred_element_type=jnp.float32)
    value_part = jnp.dot(normed_in, w_value, preferred_element_type=jnp.float32)
    beta_part = jnp.dot(normed_in, beta_rows, preferred_element_type=jnp.float32)
    alpha_part = jnp.dot(normed_in, alpha_rows, preferred_element_type=jnp.float32)
    squares_all = lax.psum(squares_in, "kv")
    squares_own = lax.dynamic_slice_in_dim(squares_all, kv_index * local_rows, local_rows, 0)
    query_sum, key_sum, value_sum, beta_sum, alpha_sum = (
        lax.psum_scatter(
            query_part.astype(jnp.bfloat16), "kv", scatter_dimension=0, tiled=True
        ).astype(jnp.float32),
        lax.psum_scatter(
            key_part.astype(jnp.bfloat16), "kv", scatter_dimension=0, tiled=True
        ).astype(jnp.float32),
        lax.psum_scatter(
            value_part.astype(jnp.bfloat16), "kv", scatter_dimension=0, tiled=True
        ).astype(jnp.float32),
        lax.psum_scatter(
            beta_part.astype(jnp.bfloat16), "kv", scatter_dimension=0, tiled=True
        ).astype(jnp.float32),
        lax.psum_scatter(
            alpha_part.astype(jnp.bfloat16), "kv", scatter_dimension=0, tiled=True
        ).astype(jnp.float32),
    )
    row_scale = lax.rsqrt(squares_own / D + EPSILON)[:, None]
    head_start = tp_index * heads_here
    lengths_own = lax.dynamic_slice_in_dim(lengths, kv_index * seq_count, seq_count, 0)
    live_own = (jnp.arange(span_len, dtype=jnp.int32)[None, :] < lengths_own[:, None])[..., None]
    beta_heads = lax.dynamic_slice_in_dim(beta_sum, head_start, heads_here, 1) * row_scale
    alpha_heads = lax.dynamic_slice_in_dim(alpha_sum, head_start, heads_here, 1) * row_scale
    rate_here = lax.dynamic_slice_in_dim(decay_rate, head_start, heads_here, 0)
    bias_here = lax.dynamic_slice_in_dim(decay_bias, head_start, heads_here, 0)
    beta = jnp.where(
        live_own, jax.nn.sigmoid(beta_heads).reshape(seq_count, span_len, heads_here), 0.0
    )
    log_decay = -rate_here * jax.nn.softplus(alpha_heads + bias_here)
    log_decay = jnp.where(live_own, log_decay.reshape(seq_count, span_len, heads_here), 0.0)
    split_shape = (seq_count, span_len, heads_here, head_size)
    queries = unit_rows((query_sum * row_scale).reshape(split_shape)) * HEAD_DIM ** (-0.5)
    unit_keys = unit_rows((key_sum * row_scale).reshape(split_shape))
    values_split = (value_sum * row_scale).reshape(split_shape)
    carried = state.reshape(seq_count, head_size, heads_here, head_size)
    attended, updated = delta_block(queries, unit_keys, values_split, beta, log_decay, carried)
    head_out = (
        attended
        * lax.rsqrt(jnp.mean(attended * attended, axis=-1, keepdims=True) + EPSILON)
        * out_gain
    )
    head_out = head_out.astype(jnp.bfloat16).reshape(local_rows, heads_here * head_size)
    pack_rows = min((batch_all * 7 // 4 + kv_count - 1) // kv_count * kv_count, row_count)
    live_flat = live_all.reshape(row_count).astype(jnp.int32)
    slot_index = jnp.cumsum(live_flat) - 1
    picker = (
        (slot_index[None, :] == jnp.arange(pack_rows, dtype=jnp.int32)[:, None])
        & (live_flat[None, :] > 0)
    ).astype(jnp.bfloat16)
    heads_every = lax.all_gather(head_out, "kv", axis=0, tiled=True)
    packed_heads = jnp.dot(picker, heads_every, preferred_element_type=jnp.float32).astype(
        jnp.bfloat16
    )
    attn_part = jnp.dot(packed_heads, w_out, preferred_element_type=jnp.float32)
    base_rows = jnp.dot(picker, flat_rows, preferred_element_type=jnp.float32)
    attn_own = lax.psum_scatter(
        attn_part.astype(jnp.bfloat16), "tp", scatter_dimension=1, tiled=True
    ).astype(jnp.float32)
    middle = (base_rows + attn_own).astype(jnp.bfloat16)
    middle_rows = lax.all_gather(middle, "tp", axis=1, tiled=True).astype(jnp.float32)
    squares_mid = jnp.sum(middle_rows * middle_rows, axis=1)
    normed_mid = (middle_rows * mix_gain).astype(jnp.bfloat16)
    gate_part = jnp.dot(normed_mid, w_gate, preferred_element_type=jnp.float32)
    up_part = jnp.dot(normed_mid, w_up, preferred_element_type=jnp.float32)
    squares_total = lax.psum(squares_mid, "kv")
    gate_sum, up_sum = (
        lax.psum(gate_part.astype(jnp.bfloat16), "kv").astype(jnp.float32),
        lax.psum(up_part.astype(jnp.bfloat16), "kv").astype(jnp.float32),
    )
    mid_scale = lax.rsqrt(squares_total / D + EPSILON)[:, None]
    hidden = (jax.nn.silu(gate_sum * mid_scale) * (up_sum * mid_scale)).astype(jnp.bfloat16)
    down_part = jnp.dot(hidden, w_down, preferred_element_type=jnp.float32)
    down_own = lax.psum_scatter(
        down_part.astype(jnp.bfloat16), "tp", scatter_dimension=1, tiled=True
    ).astype(jnp.float32)
    result_rows = middle.astype(jnp.float32) + down_own
    result_rows = jnp.dot(
        picker.astype(jnp.float32).T,
        result_rows,
        precision=lax.Precision.HIGHEST,
        preferred_element_type=jnp.float32,
    )
    mixed = (
        jnp.where(live_all, result_rows, 0.0)
        .astype(jnp.bfloat16)
        .reshape(batch_all, span_len, own_cols)
    )
    return (mixed, updated.reshape(seq_count, head_size, heads_here * head_size))


def iota(shape, axis):
    return lax.broadcasted_iota(jnp.int32, shape, axis)


def dot(a, b):
    return jnp.dot(a, b, preferred_element_type=F32)


def dot_t(a, b):
    return lax.dot_general(a, b, (((1,), (1,)), ((), ())), preferred_element_type=F32)


def dot_exact(a, b):
    return jnp.dot(a, b, precision=lax.Precision.HIGHEST, preferred_element_type=F32)


def head_sum(x, size):
    pieces = []
    for h in range(x.shape[1] // size):
        total = jnp.sum(x[:, h * size : (h + 1) * size], axis=1, keepdims=True)
        pieces.append(jnp.broadcast_to(total, (x.shape[0], size)))
    return jnp.concatenate(pieces, axis=1)


def high_low(x):
    high = x.astype(BF16)
    return high.astype(F32), x - high.astype(F32)


class Phases:
    def __init__(self):
        self.scope = None

    def __call__(self, name):
        if self.scope is not None:
            self.scope.__exit__(None, None, None)
            self.scope = None
        if name:
            self.scope = jax.named_scope(name)
            self.scope.__enter__()


GROUPS = 6
KINDS = (0, 1) * (GROUPS // 2)
PIECES = GROUPS // 2
STRIP = 64


def strip_groups(per):
    sizes = [per // GROUPS] * GROUPS
    for at in range(per % GROUPS):
        sizes[at] += 1
    return sizes


def piece_width(sizes):
    widest = max(sizes[2 * k] + sizes[2 * k + 1] for k in range(PIECES))
    return (widest * STRIP + 127) // 128 * 128


def role_of(core, chip):
    return lax.rem(core + lax.rem(chip, 2) + chip // 2, 2)


def layer_kernel(
    dims,
    tokens_hbm,
    lengths_hbm,
    state_hbm,
    attn_gain_hbm,
    wq_hbm,
    wk_hbm,
    wv_hbm,
    wb_hbm,
    wa_hbm,
    rate_hbm,
    bias_hbm,
    out_gain_hbm,
    wo_hbm,
    mix_gain_hbm,
    wg_hbm,
    wu_hbm,
    wd_hbm,
    mixed_ref,
    state_keep,
    state_back,
    state_far,
    tokens_ref,
    lengths_ref,
    attn_gain_ref,
    rate_ref,
    bias_ref,
    out_gain_ref,
    mix_gain_ref,
    w_qkv,
    w_beta,
    w_alpha,
    w_out,
    w_gu,
    w_down,
    tok_all,
    tok_pair,
    gain_pair,
    qkv_sum,
    qkv_own,
    qkv_near,
    qkv_near_in,
    qkv_last,
    qkv_last_in,
    head_all,
    attn_part,
    attn_recv,
    mid_all,
    mid_pair,
    sq_all,
    gu_sum,
    gu_near,
    gu_near_in,
    gu_last,
    gu_last_in,
    hid_all,
    down_part,
    down_recv,
    small_sem,
    load_sem,
    pair_out,
    pair_in,
    tp_send,
    tp_recv,
    qkv_out_sem,
    qkv_in_sem,
    far_send,
    far_recv,
    fwd_send,
    fwd_recv,
    sq_sem,
):
    n_kv, n_tp, batch, span, seqs, heads, size, width, ff, packs, cap = dims
    phase = Phases()
    phase("loads")
    kv = lax.axis_index("kv")
    tp = lax.axis_index("tp")
    core = lax.rem(kv, 2)
    chip = kv // 2
    other = 1 - core
    x = lax.rem(chip, 2)
    y = chip // 2
    partner = chip * 2 + other
    chips = n_kv // 2
    slots = batch * span
    group_seqs = 2 * seqs
    local = group_seqs * span
    vw = heads * size
    half_vw = vw // 2
    pair = 2 * size
    hops = (y * 2 + 1 - x, (1 - y) * 2 + x, (1 - y) * 2 + 1 - x)
    peers = [hop * 2 + other for hop in hops]
    role = role_of(core, chip)
    other_role = 1 - role
    upper = tp // 2
    tp_peers = (3 - 3 * upper, 2 - upper, tp + 1 - 2 * lax.rem(tp, 2))

    barrier = pltpu.get_barrier_semaphore()
    for peer in [partner, *peers]:
        pl.semaphore_signal(barrier, inc=1, device_id={"kv": peer}, device_id_type=MESH)
    for peer in tp_peers:
        pl.semaphore_signal(
            barrier, inc=1, device_id={"kv": partner, "tp": peer}, device_id_type=MESH
        )

    def move(source, dest, sem):
        copy = pltpu.make_async_copy(source, dest, sem)
        copy.start()
        return copy

    def send(source, dest, out_sem, in_sem, device):
        pltpu.make_async_remote_copy(
            src_ref=source,
            dst_ref=dest,
            send_sem=out_sem,
            recv_sem=in_sem,
            device_id=device,
            device_id_type=MESH,
        ).start()

    def drain(ref, sem):
        pltpu.make_async_copy(ref, ref, sem).wait()

    smalls = [
        move(source, dest, small_sem.at[i])
        for i, (source, dest) in enumerate(
            (
                (lengths_hbm, lengths_ref),
                (tokens_hbm, tokens_ref),
                (attn_gain_hbm, attn_gain_ref),
                (rate_hbm, rate_ref),
                (bias_hbm, bias_ref),
                (out_gain_hbm, out_gain_ref),
                (mix_gain_hbm, mix_gain_ref),
            )
        )
    ]

    for load in smalls[0:2]:
        load.wait()

    phase("pick")
    lengths_row = lengths_ref[...].astype(F32)
    row = iota((8, 1), 0)

    def chosen(owner):
        owner_x, owner_y = lax.rem(owner, 2), owner // 2
        return (
            (row == 0)
            | ((row == 1) & (owner_x == x))
            | ((row == 2) & (owner_x != x))
            | ((row == 3) & (owner_y == y))
            | ((row == 4) & (owner_y != y))
        )

    slot_seq = iota((batch, slots), 1) // span
    spread = (slot_seq == iota((batch, slots), 0)).astype(BF16)
    before = (slot_seq > iota((batch, slots), 0)).astype(BF16)
    length_of = dot(jnp.broadcast_to(lengths_row, (8, batch)).astype(BF16), spread)
    counted = jnp.where(chosen(iota((8, batch), 1) // group_seqs), lengths_row, 0.0)
    step = lax.rem(iota((8, slots), 1), span).astype(F32)
    members = (step < length_of) & chosen(iota((8, slots), 1) // (group_seqs * span))
    ranks = jnp.where(members, dot(counted.astype(BF16), before) + step, -1.0)
    picker = (iota((packs, slots), 0).astype(F32) == ranks[0:1, :]).astype(BF16)
    tok_all[tp] = dot(picker, tokens_ref[...]).astype(BF16)
    phase("barrier")
    pl.semaphore_wait(barrier, 1 + len(peers) + (n_tp - 1))

    def tp_start(index, source_at, dest_at):
        for peer in tp_peers:
            d = lax.rem(peer - tp + n_tp, n_tp)
            send(source_at(peer), dest_at(d), tp_send.at[index], tp_recv.at[index], {"tp": peer})

    def tp_finish(index, sent, received):
        drain(received, tp_recv.at[index])
        drain(sent, tp_send.at[index])

    rest = n_tp - 1
    to_partner = {"kv": partner}

    def pair_send(index, source, dest):
        send(source, dest, pair_out.at[index], pair_in.at[index], to_partner)

    def cross_start(index, pair_index, own_ref, pair_ref, group):
        source, dest = own_ref.at[tp, group, :], pair_ref.at[tp, group, :]
        for peer in tp_peers:
            device = {"kv": partner, "tp": peer}
            send(source, dest, tp_send.at[index], tp_recv.at[index], device)
        pair_send(pair_index, source, dest)

    def cross_pass(index, pair_index, own_ref, pair_ref, group):
        drain(pair_ref.at[0:rest, group, :], tp_recv.at[index])
        for peer in tp_peers:
            pair_send(pair_index, pair_ref.at[peer, group, :], own_ref.at[peer, group, :])
        drain(own_ref.at[0:rest, group, :], tp_send.at[index])

    every = slice(0, packs)
    phase("token_send")
    cross_start(0, 2, tok_all, tok_pair, every)
    phase("big_loads")
    def block(index, extent):
        return pl.ds(pl.multiple_of(index * extent, extent), extent)

    mine, theirs = block(role, half_vw), block(other_role, half_vw)
    pair_send(0, attn_gain_hbm, gain_pair.at[0])
    pair_send(0, mix_gain_hbm, gain_pair.at[1])
    for m, source in ((1, wk_hbm), (0, wq_hbm), (2, wv_hbm)):
        pair_send(1, source.at[:, theirs], w_qkv.at[1, m])
        move(source.at[:, mine], w_qkv.at[0, m], load_sem.at[0])
    strips = ff // STRIP
    per = (strips + 3) // 4
    missing = 4 * per - strips
    sizes = strip_groups(per)
    starts = [sum(sizes[:g]) for g in range(GROUPS)]
    loads = [
        move(wb_hbm.at[:, block(chip, 2 * width)], w_beta, load_sem.at[1]),
        move(wa_hbm.at[:, block(chip, 2 * width)], w_alpha, load_sem.at[2]),
        move(state_hbm.at[:, :, mine], state_keep, load_sem.at[3]),
        move(wo_hbm, w_out, load_sem.at[4]),
    ]

    def strip_moves(r):
        for g in range(GROUPS):
            for yy in range(2):
                source = (r * 2 + yy) * per + starts[g]
                if g == GROUPS - 1 and yy == 1:
                    source = source - missing * r
                dest = 2 * starts[g] + yy * sizes[g]
                for m, ref in enumerate((wg_hbm, wu_hbm)):
                    yield ref.at[pl.ds(source, sizes[g])], pl.ds(dest, sizes[g]), m

    for source, rows, m in strip_moves(role):
        move(source, w_gu.at[0, rows, m], load_sem.at[5])
    piece = piece_width(sizes)
    for i in range(4):
        for g in range(GROUPS):
            low = (i * per + starts[g]) * STRIP
            extent = sizes[g] * STRIP
            lost = missing * STRIP if i == 3 and g == GROUPS - 1 else 0
            dest = (g // 2 * 4 + i) * piece + (g % 2) * sizes[g - 1] * STRIP
            count = extent - lost
            if lost:
                w_down[dest : dest + lost, :] = jnp.zeros((lost, w_down.shape[1]), BF16)
            if count > 0:
                move(
                    wd_hbm.at[low : low + count, :],
                    w_down.at[dest + lost : dest + extent, :],
                    load_sem.at[6],
                )
            end = (g // 2 * 4 + i + 1) * piece
            if g % 2 and dest + extent < end:
                w_down[dest + extent : end, :] = jnp.zeros((end - dest - extent, w_down.shape[1]), BF16)
    phase("picks")
    for load in smalls[2:]:
        load.wait()
    half_rows = [
        (iota((cap, slots), 0).astype(F32) == ranks[1 + i : 2 + i, :]).astype(BF16) for i in range(4)
    ]
    keep_rows, give_rows = half_rows[0::2], half_rows[1::2]
    give = [dot_t(rows, picker).astype(BF16) for rows in give_rows]

    def slot_of(q, c, shape, axis, period=None):
        r = lax.rem(iota(shape, axis), period or shape[axis])
        s = lax.rem(r, group_seqs)
        seq = q * group_seqs + lax.rem(c + s // seqs, 2) * seqs + lax.rem(s, seqs)
        return seq * span + r // group_seqs

    def place(q, c):
        return (iota((local, slots), 1) == slot_of(q, c, (local, slots), 0)).astype(BF16)

    own_place = place(chip, core)
    settle = []
    for kind in range(2):
        both = jnp.concatenate([own_place, place(hops[1 - kind], other)], axis=0)
        known = jnp.concatenate([picker, keep_rows[kind]], axis=0)
        settle.append(dot_t(both, known).astype(BF16))

    def order(r):
        column = iota((slots, slots), 1)
        q = column // local
        return (iota((slots, slots), 0) == slot_of(q, role_of(r, q), (slots, slots), 1, local)).astype(BF16)

    pick_heads = [dot(picker, order(r)).astype(BF16) for r in range(2)]
    n_heads_all = wb_hbm.shape[0]
    core_heads = heads // 2
    first_head = tp * heads + role * core_heads
    per_head = (
        iota((n_heads_all, half_vw), 0) == iota((n_heads_all, half_vw), 1) // size + first_head
    ).astype(F32)
    rate = dot_exact(jnp.broadcast_to(rate_ref[...], (8, n_heads_all)), per_head)[0:1, :]
    bias = dot_exact(jnp.broadcast_to(bias_ref[...], (8, n_heads_all)), per_head)[0:1, :]
    slot_seq = slot_of(chip, core, (local, batch), 0) // span
    own_len = jnp.sum(
        jnp.where(iota((local, batch), 1) == slot_seq, lengths_row, 0.0), axis=1, keepdims=True
    )
    live = (iota((local, 1), 0) // group_seqs).astype(F32) < own_len
    drain(w_qkv.at[0], load_sem.at[0])
    for load in loads[0:2]:
        load.wait()
    drain(gain_pair, pair_in.at[0])
    drain(gain_pair, pair_out.at[0])

    phase("token_wait")
    cross_pass(0, 7, tok_all, tok_pair, every)

    def columns(ref):
        return jnp.concatenate([ref[j] for j in range(n_tp)], axis=1).astype(F32)

    def norm_in(ref, gain, c):
        gathered = columns(ref)
        normed = (gathered * gain).astype(BF16)
        lanes = block(c, width)
        sums = (
            dot_t(normed, w_beta[:, lanes]),
            dot_t(normed, w_alpha[:, lanes]),
            jnp.sum(gathered * gathered, axis=1, keepdims=True),
        )
        return normed, sums

    phase("norm")
    drain(w_qkv.at[1], pair_in.at[1])
    drain(tok_pair.at[0], pair_in.at[2])
    normed_pair, sums_pair = norm_in(tok_pair, gain_pair[0], other)

    widths = (128 + pair,) + (pair,) * (GROUPS - 1)
    offsets = [sum(widths[:g]) for g in range(GROUPS + 1)]

    def qkv_cols(g):
        return slice(offsets[g], offsets[g + 1])

    def qkv_dot(normed, i, g):
        lanes = slice(KINDS[g] * pair, (KINDS[g] + 1) * pair)
        return dot(normed, w_qkv[i, (1, 0, 2)[g // 2], :, lanes])

    def qkv_near_step(g):
        phase(f"qkv_near{g}")
        cols, kind = qkv_cols(g), KINDS[g]
        at = slice(g * pair, (g + 1) * pair)
        both = (qkv_sum[:, at] + qkv_dot(normed_own, 0, g)).astype(BF16)
        if g == 0:
            both = jnp.concatenate([extra.astype(BF16), both], axis=1)
        qkv_own[:, cols] = both
        qkv_near[:, cols] = dot(give[kind], both).astype(BF16)
        send(
            qkv_near.at[:, cols],
            qkv_near_in.at[:, cols],
            qkv_out_sem.at[0],
            qkv_in_sem.at[0, g],
            {"kv": peers[kind]},
        )

    settled = [None] * GROUPS

    def qkv_last_step(g):
        phase(f"qkv_last{g}")
        cols, kind = qkv_cols(g), KINDS[g]
        drain(qkv_near_in.at[:, cols], qkv_in_sem.at[0, g])
        known = jnp.concatenate([qkv_own[:, cols], qkv_near_in[:, cols]], axis=0)
        both = dot(settle[kind], known)
        settled[g] = both[0:local, :]
        qkv_last[:, cols] = both[local:, :].astype(BF16)
        send(
            qkv_last.at[:, cols],
            qkv_last_in.at[:, cols],
            qkv_out_sem.at[1],
            qkv_in_sem.at[1, g],
            {"kv": peers[1 - kind]},
        )

    def qkv_total(g):
        phase(f"qkv_total{g}")
        cols = qkv_cols(g)
        drain(qkv_last_in.at[:, cols], qkv_in_sem.at[1, g])
        return settled[g] + qkv_last_in[:, cols].astype(F32)

    for g in range(GROUPS):
        qkv_sum[:, g * pair : (g + 1) * pair] = qkv_dot(normed_pair, 1, g)
    phase("token_pair_wait")
    drain(tok_all.at[0:rest], pair_in.at[7])
    phase("bulk_send")
    pair_send(3, state_hbm.at[:, :, theirs], state_far)
    phase("norm_pair")
    normed_own, sums_own = norm_in(tok_all, attn_gain_ref[...], core)
    beta_sum, alpha_sum, squares = [a + b for a, b in zip(sums_own, sums_pair)]
    square_high, square_low = high_low(squares)
    blank = jnp.zeros((packs, 128 - 2 * n_heads_all - 2), F32)
    extra = jnp.concatenate([beta_sum, alpha_sum, square_high, square_low, blank], axis=1)
    for g in range(GROUPS):
        qkv_near_step(g)
    for g in range(GROUPS):
        qkv_last_step(g)
    phase("state_low")
    loads[2].wait()
    drain(state_far, pair_in.at[3])
    for source, rows, m in strip_moves(other_role):
        pair_send(4, source, w_gu.at[1, rows, m])
    state_low = [
        ref[...].reshape(seqs * size, half_vw).astype(BF16) for ref in (state_keep, state_far)
    ]

    def token(values, t):
        return values[t * group_seqs : (t + 1) * group_seqs, :]

    def grouped(values, group):
        return jnp.concatenate(
            [
                values[at + group * seqs : at + (group + 1) * seqs, :]
                for at in range(0, values.shape[0], group_seqs)
            ],
            axis=0,
        )

    def blocked(values):
        keep = lax.rem(iota(values.shape, 0), seqs)
        return jnp.concatenate(
            [jnp.where(keep == n, values, 0.0).astype(BF16) for n in range(seqs)], axis=1
        )

    total = qkv_total(0)
    keys_raw = [total[:, 128:], qkv_total(1)]
    phase("gates")
    extra = total[:, 0:128]
    lane = iota((local, 128), 1)
    sq_lane = (lane == 2 * n_heads_all) | (lane == 2 * n_heads_all + 1)
    sq_own = jnp.sum(jnp.where(sq_lane, extra, 0.0), axis=1, keepdims=True)
    row_scale = lax.rsqrt(sq_own / D + EPSILON)
    scaled_extra = jnp.where(sq_lane, 0.0, extra * row_scale)
    lane_of = iota((128, half_vw), 0)
    head_of = iota((128, half_vw), 1) // size + first_head
    beta_pre = dot_exact(scaled_extra, (lane_of == head_of).astype(F32))
    alpha_pre = dot_exact(scaled_extra, (lane_of == head_of + n_heads_all).astype(F32))
    beta = jnp.where(live, 1.0 / (1.0 + jnp.exp(-beta_pre)), 0.0)
    pre = alpha_pre + bias
    softplus = jnp.maximum(pre, 0.0) + jnp.log(1.0 + jnp.exp(-jnp.abs(pre)))
    log_decay = jnp.where(live, -rate * softplus, 0.0)
    cumulative = [token(log_decay, 0)]
    for t in range(1, span):
        cumulative.append(cumulative[-1] + token(log_decay, t))

    def keyed(p, k_raw):
        k_raw = k_raw * row_scale
        keys = k_raw * lax.rsqrt(head_sum(k_raw * k_raw, size) + EPSILON)
        sums = [c[:, p * pair : (p + 1) * pair] for c in cumulative]
        key_weights = [
            [
                jnp.exp(sums[t] - sums[u]) * head_sum(token(keys, t) * token(keys, u), size)
                for u in range(t)
            ]
            for t in range(span)
        ]
        return keys, sums, key_weights

    def queried(p, keyed_pair, q_raw):
        keys, sums, key_weights = keyed_pair
        q_raw = q_raw * row_scale
        queries = q_raw * lax.rsqrt(head_sum(q_raw * q_raw, size) + EPSILON) * size ** (-0.5)
        products = []
        for group in range(2):
            heads_here = []
            for h in range(2):
                at = slice(h * size, (h + 1) * size)
                both = grouped(jnp.concatenate([keys[:, at], queries[:, at]], axis=0), group)
                held = state_low[group][:, p * pair + h * size : p * pair + (h + 1) * size]
                heads_here.append(dot(blocked(both), held))
            products.append(jnp.concatenate(heads_here, axis=1))

        def product(t):
            return jnp.concatenate([g[t * seqs : (t + 1) * seqs, :] for g in products], axis=0)

        grown = [jnp.exp(c) for c in sums]
        query_weights = [
            [
                jnp.exp(sums[t] - sums[u]) * head_sum(token(queries, t) * token(keys, u), size)
                for u in range(t + 1)
            ]
            for t in range(span)
        ]
        from_keys = [grown[t] * product(t) for t in range(span)]
        from_queries = [grown[t] * product(span + t) for t in range(span)]
        return keys, sums, key_weights, query_weights, from_keys, from_queries

    gain = jnp.concatenate([out_gain_ref[...]] * 2, axis=1)

    def solved(p, keyed_pair, total):
        keys, sums, key_weights, query_weights, from_keys, from_queries = keyed_pair
        cols = slice(p * pair, (p + 1) * pair)
        values = total * row_scale
        updates, attended = [], []
        for t in range(span):
            update = token(values, t) - from_keys[t]
            for u in range(t):
                update = update - key_weights[t][u] * updates[u]
            updates.append(token(beta, t)[:, cols] * update)
            result = from_queries[t]
            for u in range(t + 1):
                result = result + query_weights[t][u] * updates[u]
            attended.append(result)
        attended = jnp.concatenate(attended, axis=0)
        out = attended * lax.rsqrt(head_sum(attended * attended, size) / size + EPSILON) * gain
        return out.astype(BF16), updates

    def gather_start(index, piece_at):
        mine = piece_at(chip, role)
        for kind in (2, 0, 1):
            send(mine, mine, far_send.at[index], far_recv.at[index, kind], {"kv": peers[kind]})
        send(mine, mine, fwd_send.at[index], fwd_recv.at[index], {"kv": partner})

    def gather_pass(index, piece_at):
        for kind in range(3):
            got = piece_at(hops[kind], other_role if kind == 2 else role)
            drain(got, far_recv.at[index, kind])
            send(got, got, fwd_send.at[index], fwd_recv.at[index], {"kv": partner})

    def gather_finish(index, sent_far, sent, received):
        drain(received, fwd_recv.at[index])
        drain(sent_far, far_send.at[index])
        drain(sent, fwd_send.at[index])

    def head_lanes(c, p):
        return block(c * 2 + p, pair)

    def head_piece(p):
        return lambda q, r: head_all.at[q, :, head_lanes(r, p)]

    def head_finish(p):
        gather_finish(
            p,
            head_all.at[0:3, :, head_lanes(role, p)],
            head_all.at[:, :, head_lanes(role, p)],
            head_all.at[:, :, head_lanes(other_role, p)],
        )

    keyed_pairs = [keyed(p, keys_raw[p]) for p in range(2)]
    queries_raw = [qkv_total(2), qkv_total(3)]
    phase("queried")
    pairs = [queried(p, keyed_pairs[p], queries_raw[p]) for p in range(2)]
    values_raw = [qkv_total(4), qkv_total(5)]
    phase("solve")
    updates = []
    for p in range(2):
        out, update = solved(p, pairs[p], values_raw[p])
        head_all[chip, :, head_lanes(role, p)] = out
        updates.append(update)
    phase("head_send")
    for p in range(2):
        gather_start(p, head_piece(p))

    def update_state(p):
        keys, sums = pairs[p][0], pairs[p][1]
        final = sums[-1]
        tails = jnp.concatenate(
            [token(keys, t) * jnp.exp(final - sums[t]) for t in range(span)], axis=0
        )
        all_updates = jnp.concatenate(updates[p], axis=0)
        decay_all = jnp.exp(final)
        for h in range(2):
            at = slice(h * size, (h + 1) * size)
            to = slice(p * pair + h * size, p * pair + (h + 1) * size)
            for group, ref in enumerate((state_keep, state_far)):
                rank = lax.dot_general(
                    blocked(grouped(tails[:, at], group)),
                    grouped(all_updates[:, at], group).astype(BF16),
                    (((0,), (0,)), ((), ())),
                    preferred_element_type=F32,
                )
                for n in range(seqs):
                    decay = decay_all[group * seqs + n : group * seqs + n + 1, at]
                    ref[n, :, to] = ref[n, :, to] * decay + rank[n * size : (n + 1) * size, :]

    phase("update0")
    update_state(0)
    update_state(1)
    phase("head_pass0")
    gather_pass(0, head_piece(0))
    phase("head_pass1")
    gather_pass(1, head_piece(1))
    phase("head_wait")
    loads[3].wait()
    head_finish(0)
    head_finish(1)
    phase("state_return")
    pair_send(5, state_far, state_back)
    phase("w_out")
    heads_every = head_all[...].reshape(slots, vw)
    packed = jnp.concatenate(
        [dot(pick_heads[r], heads_every[:, r * half_vw : (r + 1) * half_vw]) for r in range(2)],
        axis=1,
    ).astype(BF16)
    part = dot(packed, w_out[...])
    own_cols = tokens_ref.shape[1]

    def tp_scatter_start(index, part, part_ref, recv_ref, group):
        for j in range(n_tp):
            part_ref[j, group, :] = part[group, j * own_cols : (j + 1) * own_cols].astype(BF16)
        phase(f"scatter{index}")
        tp_start(
            index, lambda peer: part_ref.at[peer, group, :], lambda d: recv_ref.at[d - 1, group, :]
        )

    def tp_scatter_finish(index, part_ref, recv_ref, group):
        tp_finish(index, part_ref.at[0:rest, group, :], recv_ref.at[:, group, :])
        total = part_ref[tp, group, :].astype(F32)
        for d in range(1, n_tp):
            total = total + recv_ref[d - 1, group, :].astype(F32)
        return total

    cuts = (0, packs // 48 * 16, packs - packs // 48 * 16, packs)
    groups = [slice(cuts[i], cuts[i + 1]) for i in range(3)]
    for i, group in enumerate(groups):
        tp_scatter_start(1 + i, part, attn_part, attn_recv, group)
    own_tokens = dot(picker, tokens_ref[...])
    for i, group in enumerate(groups):
        phase(f"middle{i}")
        middle = (own_tokens[group, :] + tp_scatter_finish(1 + i, attn_part, attn_recv, group)).astype(BF16)
        mid_all[tp, group, :] = middle
        phase(f"mid_send{i}")
        cross_start(4 + i, 6, mid_all, mid_pair, group)
    phase("mid_wait")
    drain(qkv_near, qkv_out_sem.at[0])
    drain(qkv_last, qkv_out_sem.at[1])
    drain(w_gu.at[0], load_sem.at[5])
    drain(w_gu.at[1], pair_in.at[4])
    for i, group in enumerate(groups):
        cross_pass(4 + i, 8, mid_all, mid_pair, group)
    phase("norm_mid")
    drain(mid_pair.at[0], pair_in.at[6])
    normed_mid_pair = (columns(mid_pair) * gain_pair[1]).astype(BF16)
    rows_half = packs // 2

    def strip_cols(g):
        return slice(starts[g] * 128, (starts[g] + sizes[g]) * 128)

    def gu_parts(g, normed, i):
        weights = w_gu[i, 2 * starts[g] : 2 * (starts[g] + sizes[g])]
        product = dot_t(normed, weights.reshape(2 * sizes[g] * 128, width))
        wide = sizes[g] * 128
        for hh in range(2):
            for yy in range(2):
                rows = slice(hh * rows_half, (hh + 1) * rows_half)
                yield (hh, yy), product[rows, yy * wide : (yy + 1) * wide]

    def gu_own(g):
        for (hh, yy), part in gu_parts(g, normed_mid_pair, 1):
            gu_sum[hh, yy, :, strip_cols(g)] = part

    def gu_near_step(g):
        phase(f"gu_near{g}")
        cols, kind = strip_cols(g), KINDS[g]
        for (hh, yy), part in gu_parts(g, normed_mid, 0):
            gu_sum[hh, yy, :, cols] = gu_sum[hh, yy, :, cols] + part
        for i in range(2):
            at = (1 - x, i) if kind == 0 else (i, 1 - y)
            gu_near[i, :, cols] = gu_sum[*at, :, cols].astype(BF16)
        send(
            gu_near.at[:, :, cols],
            gu_near_in.at[:, :, cols],
            qkv_out_sem.at[0],
            qkv_in_sem.at[0, g],
            {"kv": peers[kind]},
        )

    def gu_last_step(g):
        phase(f"gu_last{g}")
        cols, kind = strip_cols(g), KINDS[g]
        drain(gu_near_in.at[:, :, cols], qkv_in_sem.at[0, g])
        at = (x, 1 - y) if kind == 0 else (1 - x, y)
        inner = 1 - y if kind == 0 else 1 - x
        gu_last[:, cols] = (gu_sum[*at, :, cols] + gu_near_in[inner, :, cols].astype(F32)).astype(BF16)
        send(
            gu_last.at[:, cols],
            gu_last_in.at[:, cols],
            qkv_out_sem.at[1],
            qkv_in_sem.at[1, g],
            {"kv": peers[1 - kind]},
        )

    def gu_total(g):
        phase(f"gu_total{g}")
        cols, kind = strip_cols(g), KINDS[g]
        drain(gu_last_in.at[:, cols], qkv_in_sem.at[1, g])
        inner = y if kind == 0 else x
        return (
            gu_sum[x, y, :, cols]
            + gu_near_in[inner, :, cols].astype(F32)
            + gu_last_in[:, cols].astype(F32)
        )

    for g in range(3):
        gu_own(g)
    phase("mid_pair_wait")
    drain(mid_all.at[0:rest], pair_in.at[8])
    middle_rows = columns(mid_all)
    normed_mid = (middle_rows * mix_gain_ref[...]).astype(BF16)
    for g in range(GROUPS):
        gu_near_step(g)
        if g + 3 < GROUPS:
            gu_own(g + 3)
    phase("squares")
    squares = jnp.sum(middle_rows * middle_rows, axis=1, keepdims=True)
    same = iota((packs, 128), 0) == iota((packs, 128), 1)
    sq_all[kv] = jnp.sum(jnp.where(same, squares, 0.0), axis=0, keepdims=True)
    for step in range(1, n_kv):
        peer = lax.rem(kv + step, n_kv)
        send(sq_all.at[kv], sq_all.at[kv], sq_sem.at[0], sq_sem.at[1], {"kv": peer})
    for g in range(GROUPS):
        gu_last_step(g)
    phase("scale_mid")
    drain(sq_all.at[0 : n_kv - 1], sq_sem.at[1])
    drain(sq_all.at[0 : n_kv - 1], sq_sem.at[0])
    sq_row = sq_all[0]
    for j in range(1, n_kv):
        sq_row = sq_row + sq_all[j]
    own_row = iota((rows_half, 128), 0) + x * rows_half == iota((rows_half, 128), 1)
    sq_mid = jnp.sum(jnp.where(own_row, sq_row, 0.0), axis=1, keepdims=True)
    mid_scale = lax.rsqrt(sq_mid / D + EPSILON)
    lane = iota((rows_half, 128), 1)

    def hidden_of(parts):
        wide = jnp.concatenate(parts, axis=1) * mid_scale
        pieces = []
        for at in range(0, 2 * piece, 256):
            a, b = [
                wide[:, to : to + 128] if to < wide.shape[1] else jnp.zeros((rows_half, 128), F32)
                for to in (at, at + 128)
            ]
            gate = jnp.where(lane < STRIP, a, pltpu.roll(b, STRIP, 1))
            up = jnp.where(lane < STRIP, pltpu.roll(a, STRIP, 1), b)
            pieces.append(gate / (1.0 + jnp.exp(-gate)) * up)
        return jnp.concatenate(pieces, axis=1).astype(BF16)

    def hid_piece(k):
        return lambda q, r: hid_all.at[r, q, :, k * piece : (k + 1) * piece]

    def hid_start(k):
        lanes = slice(k * piece, (k + 1) * piece)
        hid_all[role, chip, :, lanes] = hidden_of([gu_total(2 * k), gu_total(2 * k + 1)])
        phase(f"hid_send{k}")
        gather_start(k, hid_piece(k))

    def hid_finish(k):
        lanes = slice(k * piece, (k + 1) * piece)
        gather_finish(
            k,
            hid_all.at[role, 0:3, :, lanes],
            hid_all.at[role, :, :, lanes],
            hid_all.at[other_role, :, :, lanes],
        )

    def hid_rows(k, r, yy):
        lanes = slice(k * piece, (k + 1) * piece)
        return jnp.concatenate(
            [hid_all[r, 2 * yy + xx, :, lanes].astype(F32) for xx in range(2)], axis=0
        ).astype(BF16)

    def down_rows(k, r, yy, count):
        return w_down[pl.ds((4 * k + 2 * r + yy) * piece, count * piece), :]

    for k in range(PIECES):
        hid_start(k)
    phase("down_loads")
    drain(wd_hbm, load_sem.at[6])
    part = None
    for k in range(PIECES):
        phase(f"hid_pass{k}")
        gather_pass(k, hid_piece(k))
        phase(f"down_own{k}")
        own_part = dot(hid_rows(k, role, y), down_rows(k, role, y, 1))
        part = own_part if part is None else part + own_part
    for k in range(PIECES):
        hid_finish(k)
        phase(f"down{k}")
        part = part + dot(hid_rows(k, role, 1 - y), down_rows(k, role, 1 - y, 1))
        other_rows = jnp.concatenate([hid_rows(k, other_role, yy) for yy in range(2)], axis=1)
        part = part + dot(other_rows, down_rows(k, other_role, 0, 2))
    tp_scatter_start(7, part, down_part, down_recv, every)
    phase("drains")
    drain(gu_near, qkv_out_sem.at[0])
    drain(gu_last, qkv_out_sem.at[1])
    drain(w_qkv.at[1], pair_out.at[1])
    drain(tok_all.at[0], pair_out.at[2])
    drain(tok_all.at[0:rest], pair_out.at[7])
    drain(state_far, pair_out.at[3])
    drain(w_gu.at[1], pair_out.at[4])
    drain(state_far, pair_out.at[5])
    drain(state_back, pair_in.at[5])
    drain(mid_all.at[0], pair_out.at[6])
    drain(mid_all.at[0:rest], pair_out.at[8])
    phase("down_wait")
    total = tp_scatter_finish(7, down_part, down_recv, every)
    phase("result")
    result = (mid_all[tp].astype(F32) + total).astype(BF16)
    mixed_ref[...] = lax.dot_general(
        picker, result, (((0,), (0,)), ((), ())), preferred_element_type=F32
    ).astype(BF16)
    phase(None)


def fused_layer(n_kv, n_tp, *args):
    tokens, lengths, state, attn_gain, w_query = args[:5]
    w_beta, w_out, w_gate = args[7], args[12], args[14]
    batch, span, own_cols = tokens.shape
    seqs, size, vw = state.shape
    heads = vw // size
    width = attn_gain.shape[0]
    ff = w_gate.shape[1]
    pack = min(batch * 7 // 4, batch * span)
    packs = (pack + 15) // 16 * 16
    half = batch // 2
    cap = (min(half * span, pack - half) + 15) // 16 * 16
    local = 2 * seqs * span
    chips = n_kv // 2
    strips = ff // STRIP
    per = (strips + 3) // 4
    sizes = strip_groups(per)
    piece = piece_width(sizes)
    qkv_width = 128 + 3 * vw // 2
    rows_half = packs // 2
    strip_width = per * 128
    dims = (n_kv, n_tp, batch, span, seqs, heads, size, width, ff, packs, cap)
    operands = list(args)
    operands[0] = tokens.reshape(batch * span, own_cols)
    for at in (1, 3, 9, 10, 11, 13):
        operands[at] = operands[at].reshape(1, -1)
    for at in (7, 8):
        operands[at] = operands[at].T
    for at in (14, 15):
        operands[at] = operands[at].T.reshape(strips, STRIP, width)
    in_vmem = pl.BlockSpec(memory_space=pltpu.VMEM)
    in_hbm = pl.BlockSpec(memory_space=pltpu.HBM)
    dma = pltpu.SemaphoreType.DMA

    def buf(*shape):
        return pltpu.VMEM(shape, BF16)

    half_state = (seqs, size, vw // 2)
    mixed, keep, back = pl.pallas_call(
        lambda *refs: layer_kernel(dims, *refs),
        out_shape=(
            pltpu.VMEM((batch * span, own_cols), BF16),
            pltpu.VMEM(half_state, F32),
            pltpu.VMEM(half_state, F32),
        ),
        in_specs=[in_hbm] * len(operands),
        out_specs=(in_vmem, in_vmem, in_vmem),
        scratch_shapes=[
            pltpu.VMEM(half_state, F32),
            buf(batch * span, own_cols),
            pltpu.VMEM((1, batch), jnp.int32),
            pltpu.VMEM((1, width), F32),
            pltpu.VMEM((1, args[9].shape[0]), F32),
            pltpu.VMEM((1, args[10].shape[0]), F32),
            pltpu.VMEM((1, size), F32),
            pltpu.VMEM((1, width), F32),
            buf(2, 3, width, vw // 2),
            buf(w_beta.shape[1], 2 * width),
            buf(w_beta.shape[1], 2 * width),
            buf(*w_out.shape),
            buf(2, 2 * per, 2, STRIP, width),
            buf(4 * PIECES * piece, w_out.shape[1]),
            buf(n_tp, packs, own_cols),
            buf(n_tp, packs, own_cols),
            pltpu.VMEM((2, 1, width), F32),
            pltpu.VMEM((packs, 3 * vw // 2), F32),
            buf(packs, qkv_width),
            buf(cap, qkv_width),
            buf(cap, qkv_width),
            buf(local, qkv_width),
            buf(local, qkv_width),
            buf(chips, local, vw),
            buf(n_tp, packs, own_cols),
            buf(n_tp - 1, packs, own_cols),
            buf(n_tp, packs, own_cols),
            buf(n_tp, packs, own_cols),
            pltpu.VMEM((n_kv, 1, 128), F32),
            pltpu.VMEM((2, 2, rows_half, strip_width), F32),
            buf(2, rows_half, strip_width),
            buf(2, rows_half, strip_width),
            buf(rows_half, strip_width),
            buf(rows_half, strip_width),
            buf(2, chips, rows_half, PIECES * piece),
            buf(n_tp, packs, own_cols),
            buf(n_tp - 1, packs, own_cols),
            dma((7,)),
            dma((7,)),
            dma((9,)),
            dma((9,)),
            dma((8,)),
            dma((8,)),
            dma((2,)),
            dma((2, GROUPS)),
            dma((PIECES,)),
            dma((PIECES, 3)),
            dma((PIECES,)),
            dma((PIECES,)),
            dma((2,)),
        ],
        compiler_params=pltpu.CompilerParams(
            collective_id=0, has_side_effects=True, vmem_limit_bytes=52 * 1024 * 1024
        ),
    )(*operands)
    return pl.pallas_call(
        finish_kernel,
        out_shape=(
            jax.ShapeDtypeStruct(tokens.shape, BF16),
            jax.ShapeDtypeStruct(state.shape, F32),
        ),
        in_specs=[in_vmem, in_vmem, in_vmem],
        out_specs=(in_hbm, in_hbm),
        scratch_shapes=[pltpu.VMEM(tokens.shape, BF16), dma((9,))],
        compiler_params=pltpu.CompilerParams(vmem_limit_bytes=4 * 1024 * 1024),
    )(mixed, keep, back)


def finish_kernel(mixed_ref, keep_ref, back_ref, mixed_out, state_out, mixed_rows, write_sem):
    kv = lax.axis_index("kv")
    role = role_of(lax.rem(kv, 2), kv // 2)
    seqs, _, half = keep_ref.shape
    writes = []
    for i, (ref, at) in enumerate(((keep_ref, role), (back_ref, 1 - role))):
        lanes = pl.ds(pl.multiple_of(at * half, half), half)
        for j in range(4):
            rows = slice(j * seqs // 4, (j + 1) * seqs // 4)
            writes.append(
                pltpu.make_async_copy(
                    ref.at[rows], state_out.at[rows, :, lanes], write_sem.at[4 * i + j]
                )
            )
    for write in writes:
        write.start()
    mixed_rows[...] = mixed_ref[...].astype(F32).reshape(mixed_rows.shape).astype(BF16)
    writes.append(pltpu.make_async_copy(mixed_rows, mixed_out, write_sem.at[8]))
    writes[-1].start()
    for write in writes:
        write.wait()


def layer(*args):
    n_kv, n_tp = lax.axis_size("kv"), lax.axis_size("tp")
    tokens, state, w_gate = args[0], args[2], args[14]
    batch, span, own_cols = tokens.shape
    seqs, size, vw = state.shape
    pack = min(batch * 7 // 4, batch * span)
    aligned = own_cols % 128 == 0 and size % 128 == 0 and seqs == 8
    aligned = aligned and n_kv == 8 and n_tp == 4 and 2 * args[7].shape[1] + 2 <= 128
    aligned = aligned and pack % 16 == 0 and pack <= 128 and vw == 8 * size
    aligned = aligned and w_gate.shape[1] % STRIP == 0
    if aligned:
        return fused_layer(n_kv, n_tp, *args)
    return body(*args)


def solution(mesh):
    return jax.shard_map(
        layer,
        mesh=mesh,
        in_specs=(
            P(None, None, ("kv", "tp")),
            P(),
            P("kv", None, "tp"),
            P("kv"),
            P("kv", "tp"),
            P("kv", "tp"),
            P("kv", "tp"),
            P(),
            P(),
            P(),
            P(),
            P(),
            P("tp", "kv"),
            P("kv"),
            P("kv", "tp"),
            P("kv", "tp"),
            P("tp", "kv"),
        ),
        out_specs=(P(None, None, ("kv", "tp")), P("kv", None, "tp")),
        check_vma=False,
    )
```

```python
import jax
import jax.numpy as jnp
from jax import lax
from jax.experimental import pallas as pl
from jax.experimental.pallas import tpu as pltpu
from jax.sharding import PartitionSpec as P

MESH = pl.DeviceIdType.MESH
F32 = jnp.float32
BF16 = jnp.bfloat16

D = 4096
HEAD_DIM = 128


EPSILON = 1e-06


def unit_rows(vectors):
    return vectors * lax.rsqrt(jnp.sum(vectors * vectors, axis=-1, keepdims=True) + EPSILON)


def delta_block(queries, unit_keys, values_split, beta, log_decay, carried):
    highest = lax.Precision.HIGHEST
    seq_count, span_len, heads_here = beta.shape
    cumulative = jnp.cumsum(log_decay, axis=1)
    position = jnp.arange(span_len)
    inclusive = (position[:, None] >= position[None, :])[None, :, :, None]
    strict = (position[:, None] > position[None, :])[None, :, :, None]
    gap_matrix = cumulative[:, :, None, :] - cumulative[:, None, :, :]
    decay_matrix = jnp.where(inclusive, jnp.exp(jnp.where(inclusive, gap_matrix, 0.0)), 0.0)
    key_dots = jnp.einsum("nihd,njhd->nijh", unit_keys, unit_keys, precision=highest)
    query_dots = jnp.einsum("nihd,njhd->nijh", queries, unit_keys, precision=highest) * decay_matrix
    lower_part = jnp.where(strict, key_dots * decay_matrix * beta[:, :, None, :], 0.0)
    identity = jnp.eye(span_len, dtype=jnp.float32)
    inverse_rows = []
    for step in range(span_len):
        row_now = jnp.broadcast_to(identity[step][None, :, None], (seq_count, span_len, heads_here))
        for prior in range(step):
            row_now = row_now - lower_part[:, step, prior, :][:, None, :] * inverse_rows[prior]
        inverse_rows.append(row_now)
    inverse = jnp.stack(inverse_rows, axis=1)
    beta_value = beta[..., None] * values_split
    beta_key = (beta * jnp.exp(cumulative))[..., None] * unit_keys
    base_update = jnp.einsum("nich,nche->nihe", inverse, beta_value, precision=highest)
    key_weights = jnp.einsum("nich,nchd->nihd", inverse, beta_key, precision=highest)
    corrected = base_update - jnp.einsum("nihd,ndhe->nihe", key_weights, carried, precision=highest)
    decayed_queries = queries * jnp.exp(cumulative)[..., None]
    attended = jnp.einsum("nihd,ndhe->nihe", decayed_queries, carried, precision=highest)
    attended = attended + jnp.einsum("nijh,njhe->nihe", query_dots, corrected, precision=highest)
    block_total = cumulative[:, -1, :]
    key_tail = unit_keys * jnp.exp(block_total[:, None, :] - cumulative)[..., None]
    updated = carried * jnp.exp(block_total)[:, None, :, None]
    updated = updated + jnp.einsum("nihd,nihe->ndhe", key_tail, corrected, precision=highest)
    return (attended, updated)


def body(
    tokens,
    lengths,
    state,
    attn_gain,
    w_query,
    w_key,
    w_value,
    w_beta,
    w_alpha,
    decay_rate,
    decay_bias,
    out_gain,
    w_out,
    mix_gain,
    w_gate,
    w_up,
    w_down,
):
    kv_index = lax.axis_index("kv")
    tp_index = lax.axis_index("tp")
    kv_count = lax.axis_size("kv")
    batch_all, span_len, own_cols = tokens.shape
    row_count = batch_all * span_len
    seq_count = state.shape[0]
    local_rows = seq_count * span_len
    head_size = state.shape[1]
    heads_here = state.shape[2] // head_size
    block_width = attn_gain.shape[0]
    flat_rows = tokens.reshape(row_count, own_cols)
    live_all = (jnp.arange(span_len, dtype=jnp.int32)[None, :] < lengths[:, None]).reshape(
        row_count, 1
    )
    gathered = lax.all_gather(flat_rows, "tp", axis=1, tiled=True).astype(jnp.float32)
    squares_in = jnp.sum(gathered * gathered, axis=1)
    normed_in = (gathered * attn_gain).astype(jnp.bfloat16)
    beta_rows = lax.dynamic_slice_in_dim(w_beta, kv_index * block_width, block_width, 0)
    alpha_rows = lax.dynamic_slice_in_dim(w_alpha, kv_index * block_width, block_width, 0)
    query_part = jnp.dot(normed_in, w_query, preferred_element_type=jnp.float32)
    key_part = jnp.dot(normed_in, w_key, preferred_element_type=jnp.float32)
    value_part = jnp.dot(normed_in, w_value, preferred_element_type=jnp.float32)
    beta_part = jnp.dot(normed_in, beta_rows, preferred_element_type=jnp.float32)
    alpha_part = jnp.dot(normed_in, alpha_rows, preferred_element_type=jnp.float32)
    squares_all = lax.psum(squares_in, "kv")
    squares_own = lax.dynamic_slice_in_dim(squares_all, kv_index * local_rows, local_rows, 0)
    query_sum, key_sum, value_sum, beta_sum, alpha_sum = (
        lax.psum_scatter(
            query_part.astype(jnp.bfloat16), "kv", scatter_dimension=0, tiled=True
        ).astype(jnp.float32),
        lax.psum_scatter(
            key_part.astype(jnp.bfloat16), "kv", scatter_dimension=0, tiled=True
        ).astype(jnp.float32),
        lax.psum_scatter(
            value_part.astype(jnp.bfloat16), "kv", scatter_dimension=0, tiled=True
        ).astype(jnp.float32),
        lax.psum_scatter(
            beta_part.astype(jnp.bfloat16), "kv", scatter_dimension=0, tiled=True
        ).astype(jnp.float32),
        lax.psum_scatter(
            alpha_part.astype(jnp.bfloat16), "kv", scatter_dimension=0, tiled=True
        ).astype(jnp.float32),
    )
    row_scale = lax.rsqrt(squares_own / D + EPSILON)[:, None]
    head_start = tp_index * heads_here
    lengths_own = lax.dynamic_slice_in_dim(lengths, kv_index * seq_count, seq_count, 0)
    live_own = (jnp.arange(span_len, dtype=jnp.int32)[None, :] < lengths_own[:, None])[..., None]
    beta_heads = lax.dynamic_slice_in_dim(beta_sum, head_start, heads_here, 1) * row_scale
    alpha_heads = lax.dynamic_slice_in_dim(alpha_sum, head_start, heads_here, 1) * row_scale
    rate_here = lax.dynamic_slice_in_dim(decay_rate, head_start, heads_here, 0)
    bias_here = lax.dynamic_slice_in_dim(decay_bias, head_start, heads_here, 0)
    beta = jnp.where(
        live_own, jax.nn.sigmoid(beta_heads).reshape(seq_count, span_len, heads_here), 0.0
    )
    log_decay = -rate_here * jax.nn.softplus(alpha_heads + bias_here)
    log_decay = jnp.where(live_own, log_decay.reshape(seq_count, span_len, heads_here), 0.0)
    split_shape = (seq_count, span_len, heads_here, head_size)
    queries = unit_rows((query_sum * row_scale).reshape(split_shape)) * HEAD_DIM ** (-0.5)
    unit_keys = unit_rows((key_sum * row_scale).reshape(split_shape))
    values_split = (value_sum * row_scale).reshape(split_shape)
    carried = state.reshape(seq_count, head_size, heads_here, head_size)
    attended, updated = delta_block(queries, unit_keys, values_split, beta, log_decay, carried)
    head_out = (
        attended
        * lax.rsqrt(jnp.mean(attended * attended, axis=-1, keepdims=True) + EPSILON)
        * out_gain
    )
    head_out = head_out.astype(jnp.bfloat16).reshape(local_rows, heads_here * head_size)
    pack_rows = min((batch_all * 7 // 4 + kv_count - 1) // kv_count * kv_count, row_count)
    live_flat = live_all.reshape(row_count).astype(jnp.int32)
    slot_index = jnp.cumsum(live_flat) - 1
    picker = (
        (slot_index[None, :] == jnp.arange(pack_rows, dtype=jnp.int32)[:, None])
        & (live_flat[None, :] > 0)
    ).astype(jnp.bfloat16)
    heads_every = lax.all_gather(head_out, "kv", axis=0, tiled=True)
    packed_heads = jnp.dot(picker, heads_every, preferred_element_type=jnp.float32).astype(
        jnp.bfloat16
    )
    attn_part = jnp.dot(packed_heads, w_out, preferred_element_type=jnp.float32)
    base_rows = jnp.dot(picker, flat_rows, preferred_element_type=jnp.float32)
    attn_own = lax.psum_scatter(
        attn_part.astype(jnp.bfloat16), "tp", scatter_dimension=1, tiled=True
    ).astype(jnp.float32)
    middle = (base_rows + attn_own).astype(jnp.bfloat16)
    middle_rows = lax.all_gather(middle, "tp", axis=1, tiled=True).astype(jnp.float32)
    squares_mid = jnp.sum(middle_rows * middle_rows, axis=1)
    normed_mid = (middle_rows * mix_gain).astype(jnp.bfloat16)
    gate_part = jnp.dot(normed_mid, w_gate, preferred_element_type=jnp.float32)
    up_part = jnp.dot(normed_mid, w_up, preferred_element_type=jnp.float32)
    squares_total = lax.psum(squares_mid, "kv")
    gate_sum, up_sum = (
        lax.psum(gate_part.astype(jnp.bfloat16), "kv").astype(jnp.float32),
        lax.psum(up_part.astype(jnp.bfloat16), "kv").astype(jnp.float32),
    )
    mid_scale = lax.rsqrt(squares_total / D + EPSILON)[:, None]
    hidden = (jax.nn.silu(gate_sum * mid_scale) * (up_sum * mid_scale)).astype(jnp.bfloat16)
    down_part = jnp.dot(hidden, w_down, preferred_element_type=jnp.float32)
    down_own = lax.psum_scatter(
        down_part.astype(jnp.bfloat16), "tp", scatter_dimension=1, tiled=True
    ).astype(jnp.float32)
    result_rows = middle.astype(jnp.float32) + down_own
    result_rows = jnp.dot(
        picker.astype(jnp.float32).T,
        result_rows,
        precision=lax.Precision.HIGHEST,
        preferred_element_type=jnp.float32,
    )
    mixed = (
        jnp.where(live_all, result_rows, 0.0)
        .astype(jnp.bfloat16)
        .reshape(batch_all, span_len, own_cols)
    )
    return (mixed, updated.reshape(seq_count, head_size, heads_here * head_size))


def iota(shape, axis):
    return lax.broadcasted_iota(jnp.int32, shape, axis)


def dot(a, b):
    return jnp.dot(a, b, preferred_element_type=F32)


def dot_t(a, b):
    return lax.dot_general(a, b, (((1,), (1,)), ((), ())), preferred_element_type=F32)


def dot_exact(a, b):
    return jnp.dot(a, b, precision=lax.Precision.HIGHEST, preferred_element_type=F32)


def head_sum(x, size):
    pieces = []
    for h in range(x.shape[1] // size):
        total = jnp.sum(x[:, h * size : (h + 1) * size], axis=1, keepdims=True)
        pieces.append(jnp.broadcast_to(total, (x.shape[0], size)))
    return jnp.concatenate(pieces, axis=1)


def high_low(x):
    high = x.astype(BF16)
    return high.astype(F32), x - high.astype(F32)


class Phases:
    def __init__(self):
        self.scope = None

    def __call__(self, name):
        if self.scope is not None:
            self.scope.__exit__(None, None, None)
            self.scope = None
        if name:
            self.scope = jax.named_scope(name)
            self.scope.__enter__()


GROUPS = 6
KINDS = (0, 1) * (GROUPS // 2)
PIECES = GROUPS // 2
STRIP = 64


def strip_groups(per):
    sizes = [per // GROUPS] * GROUPS
    for at in range(per % GROUPS):
        sizes[at] += 1
    return sizes


def piece_width(sizes):
    widest = max(sizes[2 * k] + sizes[2 * k + 1] for k in range(PIECES))
    return (widest * STRIP + 127) // 128 * 128


def role_of(core, chip):
    return lax.rem(core + lax.rem(chip, 2) + chip // 2, 2)


def layer_kernel(
    dims,
    tokens_hbm,
    lengths_hbm,
    state_hbm,
    attn_gain_hbm,
    wq_hbm,
    wk_hbm,
    wv_hbm,
    wb_hbm,
    wa_hbm,
    rate_hbm,
    bias_hbm,
    out_gain_hbm,
    wo_hbm,
    mix_gain_hbm,
    wg_hbm,
    wu_hbm,
    wd_hbm,
    mixed_ref,
    state_keep,
    state_back,
    state_far,
    tokens_ref,
    lengths_ref,
    attn_gain_ref,
    rate_ref,
    bias_ref,
    out_gain_ref,
    mix_gain_ref,
    w_qkv,
    w_beta,
    w_alpha,
    w_out,
    w_gu,
    w_down,
    tok_all,
    tok_pair,
    gain_pair,
    qkv_sum,
    qkv_own,
    qkv_near,
    qkv_near_in,
    qkv_last,
    qkv_last_in,
    head_all,
    attn_part,
    attn_recv,
    mid_all,
    mid_pair,
    sq_all,
    gu_sum,
    gu_near,
    gu_near_in,
    gu_last,
    gu_last_in,
    hid_all,
    down_part,
    down_recv,
    small_sem,
    load_sem,
    pair_out,
    pair_in,
    tp_send,
    tp_recv,
    qkv_out_sem,
    qkv_in_sem,
    far_send,
    far_recv,
    fwd_send,
    fwd_recv,
    sq_sem,
):
    n_kv, n_tp, batch, span, seqs, heads, size, width, ff, packs, cap = dims
    phase = Phases()
    phase("loads")
    kv = lax.axis_index("kv")
    tp = lax.axis_index("tp")
    core = lax.rem(kv, 2)
    chip = kv // 2
    other = 1 - core
    x = lax.rem(chip, 2)
    y = chip // 2
    partner = chip * 2 + other
    chips = n_kv // 2
    slots = batch * span
    group_seqs = 2 * seqs
    local = group_seqs * span
    vw = heads * size
    half_vw = vw // 2
    pair = 2 * size
    hops = (y * 2 + 1 - x, (1 - y) * 2 + x, (1 - y) * 2 + 1 - x)
    peers = [hop * 2 + other for hop in hops]
    role = role_of(core, chip)
    other_role = 1 - role
    upper = tp // 2
    tp_peers = (3 - 3 * upper, 2 - upper, tp + 1 - 2 * lax.rem(tp, 2))

    barrier = pltpu.get_barrier_semaphore()
    for peer in [partner, *peers]:
        pl.semaphore_signal(barrier, inc=1, device_id={"kv": peer}, device_id_type=MESH)
    for peer in tp_peers:
        pl.semaphore_signal(
            barrier, inc=1, device_id={"kv": partner, "tp": peer}, device_id_type=MESH
        )

    def move(source, dest, sem):
        copy = pltpu.make_async_copy(source, dest, sem)
        copy.start()
        return copy

    def send(source, dest, out_sem, in_sem, device):
        pltpu.make_async_remote_copy(
            src_ref=source,
            dst_ref=dest,
            send_sem=out_sem,
            recv_sem=in_sem,
            device_id=device,
            device_id_type=MESH,
        ).start()

    def drain(ref, sem):
        pltpu.make_async_copy(ref, ref, sem).wait()

    smalls = [
        move(source, dest, small_sem.at[i])
        for i, (source, dest) in enumerate(
            (
                (lengths_hbm, lengths_ref),
                (attn_gain_hbm, attn_gain_ref),
                (rate_hbm, rate_ref),
                (bias_hbm, bias_ref),
                (out_gain_hbm, out_gain_ref),
                (mix_gain_hbm, mix_gain_ref),
            )
        )
    ]

    tokens_each = slots // 8
    for at in range(0, slots, tokens_each):
        move(tokens_hbm.at[at : at + tokens_each], tokens_ref.at[at : at + tokens_each], small_sem.at[6])
    smalls[0].wait()

    phase("pick")
    lengths_row = lengths_ref[...].astype(F32)
    row = iota((8, 1), 0)

    def chosen(owner):
        owner_x, owner_y = lax.rem(owner, 2), owner // 2
        return (
            (row == 0)
            | ((row == 1) & (owner_x == x))
            | ((row == 2) & (owner_x != x))
            | ((row == 3) & (owner_y == y))
            | ((row == 4) & (owner_y != y))
        )

    slot_seq = iota((batch, slots), 1) // span
    spread = (slot_seq == iota((batch, slots), 0)).astype(BF16)
    before = (slot_seq > iota((batch, slots), 0)).astype(BF16)
    length_of = dot(jnp.broadcast_to(lengths_row, (8, batch)).astype(BF16), spread)
    counted = jnp.where(chosen(iota((8, batch), 1) // group_seqs), lengths_row, 0.0)
    step = lax.rem(iota((8, slots), 1), span).astype(F32)
    members = (step < length_of) & chosen(iota((8, slots), 1) // (group_seqs * span))
    ranks = jnp.where(members, dot(counted.astype(BF16), before) + step, -1.0)
    picker = (iota((packs, slots), 0).astype(F32) == ranks[0:1, :]).astype(BF16)
    drain(tokens_ref, small_sem.at[6])
    tok_all[tp] = dot(picker, tokens_ref[...]).astype(BF16)
    phase("barrier")
    pl.semaphore_wait(barrier, 1 + len(peers) + (n_tp - 1))

    def tp_start(index, source_at, dest_at):
        for peer in tp_peers:
            d = lax.rem(peer - tp + n_tp, n_tp)
            send(source_at(peer), dest_at(d), tp_send.at[index], tp_recv.at[index], {"tp": peer})

    def tp_finish(index, sent, received):
        drain(received, tp_recv.at[index])
        drain(sent, tp_send.at[index])

    rest = n_tp - 1
    to_partner = {"kv": partner}

    def pair_send(index, source, dest):
        send(source, dest, pair_out.at[index], pair_in.at[index], to_partner)

    def cross_start(index, pair_index, own_ref, pair_ref, group):
        source, dest = own_ref.at[tp, group, :], pair_ref.at[tp, group, :]
        for peer in tp_peers:
            device = {"kv": partner, "tp": peer}
            send(source, dest, tp_send.at[index], tp_recv.at[index], device)
        pair_send(pair_index, source, dest)

    def cross_pass(index, pair_index, own_ref, pair_ref, group):
        drain(pair_ref.at[0:rest, group, :], tp_recv.at[index])
        for peer in tp_peers:
            pair_send(pair_index, pair_ref.at[peer, group, :], own_ref.at[peer, group, :])
        drain(own_ref.at[0:rest, group, :], tp_send.at[index])

    every = slice(0, packs)
    phase("token_send")
    cross_start(0, 2, tok_all, tok_pair, every)
    phase("big_loads")
    def block(index, extent):
        return pl.ds(pl.multiple_of(index * extent, extent), extent)

    mine, theirs = block(role, half_vw), block(other_role, half_vw)
    pair_send(0, attn_gain_hbm, gain_pair.at[0])
    pair_send(0, mix_gain_hbm, gain_pair.at[1])
    for m, source in ((1, wk_hbm), (0, wq_hbm), (2, wv_hbm)):
        pair_send(1, source.at[:, theirs], w_qkv.at[1, m])
        move(source.at[:, mine], w_qkv.at[0, m], load_sem.at[0])
    strips = ff // STRIP
    per = (strips + 3) // 4
    missing = 4 * per - strips
    sizes = strip_groups(per)
    starts = [sum(sizes[:g]) for g in range(GROUPS)]
    loads = [
        move(wb_hbm.at[:, block(chip, 2 * width)], w_beta, load_sem.at[1]),
        move(wa_hbm.at[:, block(chip, 2 * width)], w_alpha, load_sem.at[2]),
        move(state_hbm.at[:, :, mine], state_keep, load_sem.at[3]),
        move(wo_hbm, w_out, load_sem.at[4]),
    ]

    def strip_moves(r):
        for g in range(GROUPS):
            for yy in range(2):
                source = (r * 2 + yy) * per + starts[g]
                if g == GROUPS - 1 and yy == 1:
                    source = source - missing * r
                dest = 2 * starts[g] + yy * sizes[g]
                for m, ref in enumerate((wg_hbm, wu_hbm)):
                    yield ref.at[pl.ds(source, sizes[g])], pl.ds(dest, sizes[g]), m

    for source, rows, m in strip_moves(role):
        move(source, w_gu.at[0, rows, m], load_sem.at[5])
    piece = piece_width(sizes)
    for i in range(4):
        for g in range(GROUPS):
            low = (i * per + starts[g]) * STRIP
            extent = sizes[g] * STRIP
            lost = missing * STRIP if i == 3 and g == GROUPS - 1 else 0
            dest = (g // 2 * 4 + i) * piece + (g % 2) * sizes[g - 1] * STRIP
            count = extent - lost
            if lost:
                w_down[dest : dest + lost, :] = jnp.zeros((lost, w_down.shape[1]), BF16)
            if count > 0:
                move(
                    wd_hbm.at[low : low + count, :],
                    w_down.at[dest + lost : dest + extent, :],
                    load_sem.at[6],
                )
            end = (g // 2 * 4 + i + 1) * piece
            if g % 2 and dest + extent < end:
                w_down[dest + extent : end, :] = jnp.zeros((end - dest - extent, w_down.shape[1]), BF16)
    phase("picks")
    for load in smalls[1:]:
        load.wait()
    half_rows = [
        (iota((cap, slots), 0).astype(F32) == ranks[1 + i : 2 + i, :]).astype(BF16) for i in range(4)
    ]
    keep_rows, give_rows = half_rows[0::2], half_rows[1::2]
    give = [dot_t(rows, picker).astype(BF16) for rows in give_rows]

    def slot_of(q, c, shape, axis, period=None):
        r = lax.rem(iota(shape, axis), period or shape[axis])
        s = lax.rem(r, group_seqs)
        seq = q * group_seqs + lax.rem(c + s // seqs, 2) * seqs + lax.rem(s, seqs)
        return seq * span + r // group_seqs

    def place(q, c):
        return (iota((local, slots), 1) == slot_of(q, c, (local, slots), 0)).astype(BF16)

    own_place = place(chip, core)
    settle = []
    for kind in range(2):
        both = jnp.concatenate([own_place, place(hops[1 - kind], other)], axis=0)
        known = jnp.concatenate([picker, keep_rows[kind]], axis=0)
        settle.append(dot_t(both, known).astype(BF16))

    def order(r):
        column = iota((slots, slots), 1)
        q = column // local
        return (iota((slots, slots), 0) == slot_of(q, role_of(r, q), (slots, slots), 1, local)).astype(BF16)

    pick_heads = [dot(picker, order(r)).astype(BF16) for r in range(2)]
    n_heads_all = wb_hbm.shape[0]
    core_heads = heads // 2
    first_head = tp * heads + role * core_heads
    per_head = (
        iota((n_heads_all, half_vw), 0) == iota((n_heads_all, half_vw), 1) // size + first_head
    ).astype(F32)
    rate = dot_exact(jnp.broadcast_to(rate_ref[...], (8, n_heads_all)), per_head)[0:1, :]
    bias = dot_exact(jnp.broadcast_to(bias_ref[...], (8, n_heads_all)), per_head)[0:1, :]
    slot_seq = slot_of(chip, core, (local, batch), 0) // span
    own_len = jnp.sum(
        jnp.where(iota((local, batch), 1) == slot_seq, lengths_row, 0.0), axis=1, keepdims=True
    )
    live = (iota((local, 1), 0) // group_seqs).astype(F32) < own_len
    drain(w_qkv.at[0], load_sem.at[0])
    for load in loads[0:2]:
        load.wait()
    drain(gain_pair, pair_in.at[0])
    drain(gain_pair, pair_out.at[0])

    phase("token_wait")
    cross_pass(0, 7, tok_all, tok_pair, every)

    def columns(ref):
        return jnp.concatenate([ref[j] for j in range(n_tp)], axis=1).astype(F32)

    def norm_in(ref, gain, c):
        gathered = columns(ref)
        normed = (gathered * gain).astype(BF16)
        lanes = block(c, width)
        sums = (
            dot_t(normed, w_beta[:, lanes]),
            dot_t(normed, w_alpha[:, lanes]),
            jnp.sum(gathered * gathered, axis=1, keepdims=True),
        )
        return normed, sums

    phase("norm")
    drain(w_qkv.at[1], pair_in.at[1])
    drain(tok_pair.at[0], pair_in.at[2])
    normed_pair, sums_pair = norm_in(tok_pair, gain_pair[0], other)

    widths = (128 + pair,) + (pair,) * (GROUPS - 1)
    offsets = [sum(widths[:g]) for g in range(GROUPS + 1)]

    def qkv_cols(g):
        return slice(offsets[g], offsets[g + 1])

    def qkv_dot(normed, i, g):
        lanes = slice(KINDS[g] * pair, (KINDS[g] + 1) * pair)
        return dot(normed, w_qkv[i, (1, 0, 2)[g // 2], :, lanes])

    def qkv_near_step(g):
        phase(f"qkv_near{g}")
        cols, kind = qkv_cols(g), KINDS[g]
        at = slice(g * pair, (g + 1) * pair)
        both = (qkv_sum[:, at] + qkv_dot(normed_own, 0, g)).astype(BF16)
        if g == 0:
            both = jnp.concatenate([extra.astype(BF16), both], axis=1)
        qkv_own[:, cols] = both
        qkv_near[:, cols] = dot(give[kind], both).astype(BF16)
        send(
            qkv_near.at[:, cols],
            qkv_near_in.at[:, cols],
            qkv_out_sem.at[0],
            qkv_in_sem.at[0, g],
            {"kv": peers[kind]},
        )

    settled = [None] * GROUPS

    def qkv_last_step(g):
        phase(f"qkv_last{g}")
        cols, kind = qkv_cols(g), KINDS[g]
        drain(qkv_near_in.at[:, cols], qkv_in_sem.at[0, g])
        known = jnp.concatenate([qkv_own[:, cols], qkv_near_in[:, cols]], axis=0)
        both = dot(settle[kind], known)
        settled[g] = both[0:local, :]
        qkv_last[:, cols] = both[local:, :].astype(BF16)
        send(
            qkv_last.at[:, cols],
            qkv_last_in.at[:, cols],
            qkv_out_sem.at[1],
            qkv_in_sem.at[1, g],
            {"kv": peers[1 - kind]},
        )

    def qkv_total(g):
        phase(f"qkv_total{g}")
        cols = qkv_cols(g)
        drain(qkv_last_in.at[:, cols], qkv_in_sem.at[1, g])
        return settled[g] + qkv_last_in[:, cols].astype(F32)

    for g in range(GROUPS):
        qkv_sum[:, g * pair : (g + 1) * pair] = qkv_dot(normed_pair, 1, g)
    phase("token_pair_wait")
    drain(tok_all.at[0:rest], pair_in.at[7])
    phase("bulk_send")
    pair_send(3, state_hbm.at[:, :, theirs], state_far)
    phase("norm_pair")
    normed_own, sums_own = norm_in(tok_all, attn_gain_ref[...], core)
    beta_sum, alpha_sum, squares = [a + b for a, b in zip(sums_own, sums_pair)]
    square_high, square_low = high_low(squares)
    blank = jnp.zeros((packs, 128 - 2 * n_heads_all - 2), F32)
    extra = jnp.concatenate([beta_sum, alpha_sum, square_high, square_low, blank], axis=1)
    for g in range(GROUPS):
        qkv_near_step(g)
    for g in range(GROUPS):
        qkv_last_step(g)
    phase("state_low")
    loads[2].wait()
    drain(state_far, pair_in.at[3])
    for source, rows, m in strip_moves(other_role):
        pair_send(4, source, w_gu.at[1, rows, m])
    state_low = [
        ref[...].reshape(seqs * size, half_vw).astype(BF16) for ref in (state_keep, state_far)
    ]

    def token(values, t):
        return values[t * group_seqs : (t + 1) * group_seqs, :]

    def grouped(values, group):
        return jnp.concatenate(
            [
                values[at + group * seqs : at + (group + 1) * seqs, :]
                for at in range(0, values.shape[0], group_seqs)
            ],
            axis=0,
        )

    def blocked(values):
        keep = lax.rem(iota(values.shape, 0), seqs)
        return jnp.concatenate(
            [jnp.where(keep == n, values, 0.0).astype(BF16) for n in range(seqs)], axis=1
        )

    total = qkv_total(0)
    keys_raw = [total[:, 128:], qkv_total(1)]
    phase("gates")
    extra = total[:, 0:128]
    lane = iota((local, 128), 1)
    sq_lane = (lane == 2 * n_heads_all) | (lane == 2 * n_heads_all + 1)
    sq_own = jnp.sum(jnp.where(sq_lane, extra, 0.0), axis=1, keepdims=True)
    row_scale = lax.rsqrt(sq_own / D + EPSILON)
    scaled_extra = jnp.where(sq_lane, 0.0, extra * row_scale)
    lane_of = iota((128, half_vw), 0)
    head_of = iota((128, half_vw), 1) // size + first_head
    beta_pre = dot_exact(scaled_extra, (lane_of == head_of).astype(F32))
    alpha_pre = dot_exact(scaled_extra, (lane_of == head_of + n_heads_all).astype(F32))
    beta = jnp.where(live, 1.0 / (1.0 + jnp.exp(-beta_pre)), 0.0)
    pre = alpha_pre + bias
    softplus = jnp.maximum(pre, 0.0) + jnp.log(1.0 + jnp.exp(-jnp.abs(pre)))
    log_decay = jnp.where(live, -rate * softplus, 0.0)
    cumulative = [token(log_decay, 0)]
    for t in range(1, span):
        cumulative.append(cumulative[-1] + token(log_decay, t))

    def keyed(p, k_raw):
        k_raw = k_raw * row_scale
        keys = k_raw * lax.rsqrt(head_sum(k_raw * k_raw, size) + EPSILON)
        sums = [c[:, p * pair : (p + 1) * pair] for c in cumulative]
        key_weights = [
            [
                jnp.exp(sums[t] - sums[u]) * head_sum(token(keys, t) * token(keys, u), size)
                for u in range(t)
            ]
            for t in range(span)
        ]
        return keys, sums, key_weights

    def queried(p, keyed_pair, q_raw):
        keys, sums, key_weights = keyed_pair
        q_raw = q_raw * row_scale
        queries = q_raw * lax.rsqrt(head_sum(q_raw * q_raw, size) + EPSILON) * size ** (-0.5)
        products = []
        for group in range(2):
            heads_here = []
            for h in range(2):
                at = slice(h * size, (h + 1) * size)
                both = grouped(jnp.concatenate([keys[:, at], queries[:, at]], axis=0), group)
                held = state_low[group][:, p * pair + h * size : p * pair + (h + 1) * size]
                heads_here.append(dot(blocked(both), held))
            products.append(jnp.concatenate(heads_here, axis=1))

        def product(t):
            return jnp.concatenate([g[t * seqs : (t + 1) * seqs, :] for g in products], axis=0)

        grown = [jnp.exp(c) for c in sums]
        query_weights = [
            [
                jnp.exp(sums[t] - sums[u]) * head_sum(token(queries, t) * token(keys, u), size)
                for u in range(t + 1)
            ]
            for t in range(span)
        ]
        from_keys = [grown[t] * product(t) for t in range(span)]
        from_queries = [grown[t] * product(span + t) for t in range(span)]
        return keys, sums, key_weights, query_weights, from_keys, from_queries

    gain = jnp.concatenate([out_gain_ref[...]] * 2, axis=1)

    def solved(p, keyed_pair, total):
        keys, sums, key_weights, query_weights, from_keys, from_queries = keyed_pair
        cols = slice(p * pair, (p + 1) * pair)
        values = total * row_scale
        updates, attended = [], []
        for t in range(span):
            update = token(values, t) - from_keys[t]
            for u in range(t):
                update = update - key_weights[t][u] * updates[u]
            updates.append(token(beta, t)[:, cols] * update)
            result = from_queries[t]
            for u in range(t + 1):
                result = result + query_weights[t][u] * updates[u]
            attended.append(result)
        attended = jnp.concatenate(attended, axis=0)
        out = attended * lax.rsqrt(head_sum(attended * attended, size) / size + EPSILON) * gain
        return out.astype(BF16), updates

    def gather_start(index, piece_at):
        mine = piece_at(chip, role)
        for kind in (2, 1, 0):
            send(mine, mine, far_send.at[index], far_recv.at[index, kind], {"kv": peers[kind]})
        send(mine, mine, fwd_send.at[index], fwd_recv.at[index], {"kv": partner})

    def gather_pass(index, piece_at):
        for kind in range(3):
            got = piece_at(hops[kind], other_role if kind == 2 else role)
            drain(got, far_recv.at[index, kind])
            send(got, got, fwd_send.at[index], fwd_recv.at[index], {"kv": partner})

    def gather_finish(index, sent_far, sent, received):
        drain(received, fwd_recv.at[index])
        drain(sent_far, far_send.at[index])
        drain(sent, fwd_send.at[index])

    def head_lanes(c, p):
        return block(c * 2 + p, pair)

    def head_piece(p):
        return lambda q, r: head_all.at[q, :, head_lanes(r, p)]

    def head_finish(p):
        gather_finish(
            p,
            head_all.at[0:3, :, head_lanes(role, p)],
            head_all.at[:, :, head_lanes(role, p)],
            head_all.at[:, :, head_lanes(other_role, p)],
        )

    keyed_pairs = [keyed(p, keys_raw[p]) for p in range(2)]
    queries_raw = [qkv_total(2), qkv_total(3)]
    phase("queried")
    pairs = [queried(p, keyed_pairs[p], queries_raw[p]) for p in range(2)]
    values_raw = [qkv_total(4), qkv_total(5)]
    phase("solve")
    updates = []
    for p in range(2):
        out, update = solved(p, pairs[p], values_raw[p])
        head_all[chip, :, head_lanes(role, p)] = out
        updates.append(update)
    phase("head_send")
    for p in range(2):
        gather_start(p, head_piece(p))

    def update_state(p):
        keys, sums = pairs[p][0], pairs[p][1]
        final = sums[-1]
        tails = jnp.concatenate(
            [token(keys, t) * jnp.exp(final - sums[t]) for t in range(span)], axis=0
        )
        all_updates = jnp.concatenate(updates[p], axis=0)
        decay_all = jnp.exp(final)
        for h in range(2):
            at = slice(h * size, (h + 1) * size)
            to = slice(p * pair + h * size, p * pair + (h + 1) * size)
            for group, ref in enumerate((state_keep, state_far)):
                rank = lax.dot_general(
                    blocked(grouped(tails[:, at], group)),
                    grouped(all_updates[:, at], group).astype(BF16),
                    (((0,), (0,)), ((), ())),
                    preferred_element_type=F32,
                )
                for n in range(seqs):
                    decay = decay_all[group * seqs + n : group * seqs + n + 1, at]
                    ref[n, :, to] = ref[n, :, to] * decay + rank[n * size : (n + 1) * size, :]

    phase("update0")
    update_state(0)
    update_state(1)
    phase("head_pass0")
    gather_pass(0, head_piece(0))
    phase("head_pass1")
    gather_pass(1, head_piece(1))
    phase("head_wait")
    loads[3].wait()
    head_finish(0)
    head_finish(1)
    phase("state_return")
    pair_send(5, state_far, state_back)
    phase("w_out")
    heads_every = head_all[...].reshape(slots, vw)
    packed = jnp.concatenate(
        [dot(pick_heads[r], heads_every[:, r * half_vw : (r + 1) * half_vw]) for r in range(2)],
        axis=1,
    ).astype(BF16)
    part = dot(packed, w_out[...])
    own_cols = tokens_ref.shape[1]

    def tp_scatter_start(index, part, part_ref, recv_ref, group):
        for j in range(n_tp):
            part_ref[j, group, :] = part[group, j * own_cols : (j + 1) * own_cols].astype(BF16)
        phase(f"scatter{index}")
        tp_start(
            index, lambda peer: part_ref.at[peer, group, :], lambda d: recv_ref.at[d - 1, group, :]
        )

    def tp_scatter_finish(index, part_ref, recv_ref, group):
        tp_finish(index, part_ref.at[0:rest, group, :], recv_ref.at[:, group, :])
        total = part_ref[tp, group, :].astype(F32)
        for d in range(1, n_tp):
            total = total + recv_ref[d - 1, group, :].astype(F32)
        return total

    cuts = (0, packs // 48 * 16, packs - packs // 48 * 16, packs)
    groups = [slice(cuts[i], cuts[i + 1]) for i in range(3)]
    for i, group in enumerate(groups):
        tp_scatter_start(1 + i, part, attn_part, attn_recv, group)
    own_tokens = dot(picker, tokens_ref[...])
    for i, group in enumerate(groups):
        phase(f"middle{i}")
        middle = (own_tokens[group, :] + tp_scatter_finish(1 + i, attn_part, attn_recv, group)).astype(BF16)
        mid_all[tp, group, :] = middle
        phase(f"mid_send{i}")
        cross_start(4 + i, 6, mid_all, mid_pair, group)
    phase("mid_wait")
    drain(qkv_near, qkv_out_sem.at[0])
    drain(qkv_last, qkv_out_sem.at[1])
    drain(w_gu.at[0], load_sem.at[5])
    drain(w_gu.at[1], pair_in.at[4])
    for i, group in enumerate(groups):
        cross_pass(4 + i, 8, mid_all, mid_pair, group)
    phase("norm_mid")
    drain(mid_pair.at[0], pair_in.at[6])
    normed_mid_pair = (columns(mid_pair) * gain_pair[1]).astype(BF16)
    rows_half = packs // 2

    def strip_cols(g):
        return slice(starts[g] * 128, (starts[g] + sizes[g]) * 128)

    def gu_parts(g, normed, i):
        weights = w_gu[i, 2 * starts[g] : 2 * (starts[g] + sizes[g])]
        product = dot_t(normed, weights.reshape(2 * sizes[g] * 128, width))
        wide = sizes[g] * 128
        for hh in range(2):
            for yy in range(2):
                rows = slice(hh * rows_half, (hh + 1) * rows_half)
                yield (hh, yy), product[rows, yy * wide : (yy + 1) * wide]

    def gu_own(g):
        for (hh, yy), part in gu_parts(g, normed_mid_pair, 1):
            gu_sum[hh, yy, :, strip_cols(g)] = part

    def gu_near_step(g):
        phase(f"gu_near{g}")
        cols, kind = strip_cols(g), KINDS[g]
        for (hh, yy), part in gu_parts(g, normed_mid, 0):
            gu_sum[hh, yy, :, cols] = gu_sum[hh, yy, :, cols] + part
        for i in range(2):
            at = (1 - x, i) if kind == 0 else (i, 1 - y)
            gu_near[i, :, cols] = gu_sum[*at, :, cols].astype(BF16)
        send(
            gu_near.at[:, :, cols],
            gu_near_in.at[:, :, cols],
            qkv_out_sem.at[0],
            qkv_in_sem.at[0, g],
            {"kv": peers[kind]},
        )

    def gu_last_step(g):
        phase(f"gu_last{g}")
        cols, kind = strip_cols(g), KINDS[g]
        drain(gu_near_in.at[:, :, cols], qkv_in_sem.at[0, g])
        at = (x, 1 - y) if kind == 0 else (1 - x, y)
        inner = 1 - y if kind == 0 else 1 - x
        gu_last[:, cols] = (gu_sum[*at, :, cols] + gu_near_in[inner, :, cols].astype(F32)).astype(BF16)
        send(
            gu_last.at[:, cols],
            gu_last_in.at[:, cols],
            qkv_out_sem.at[1],
            qkv_in_sem.at[1, g],
            {"kv": peers[1 - kind]},
        )

    def gu_total(g):
        phase(f"gu_total{g}")
        cols, kind = strip_cols(g), KINDS[g]
        drain(gu_last_in.at[:, cols], qkv_in_sem.at[1, g])
        inner = y if kind == 0 else x
        return (
            gu_sum[x, y, :, cols]
            + gu_near_in[inner, :, cols].astype(F32)
            + gu_last_in[:, cols].astype(F32)
        )

    for g in range(3):
        gu_own(g)
    phase("mid_pair_wait")
    drain(mid_all.at[0:rest], pair_in.at[8])
    middle_rows = columns(mid_all)
    normed_mid = (middle_rows * mix_gain_ref[...]).astype(BF16)
    for g in range(GROUPS):
        gu_near_step(g)
        if g + 3 < GROUPS:
            gu_own(g + 3)
    phase("squares")
    squares = jnp.sum(middle_rows * middle_rows, axis=1, keepdims=True)
    same = iota((packs, 128), 0) == iota((packs, 128), 1)
    sq_all[kv] = jnp.sum(jnp.where(same, squares, 0.0), axis=0, keepdims=True)
    for step in range(1, n_kv):
        peer = lax.rem(kv + step, n_kv)
        send(sq_all.at[kv], sq_all.at[kv], sq_sem.at[0], sq_sem.at[1], {"kv": peer})
    for g in range(GROUPS):
        gu_last_step(g)
    phase("scale_mid")
    drain(sq_all.at[0 : n_kv - 1], sq_sem.at[1])
    drain(sq_all.at[0 : n_kv - 1], sq_sem.at[0])
    sq_row = sq_all[0]
    for j in range(1, n_kv):
        sq_row = sq_row + sq_all[j]
    own_row = iota((rows_half, 128), 0) + x * rows_half == iota((rows_half, 128), 1)
    sq_mid = jnp.sum(jnp.where(own_row, sq_row, 0.0), axis=1, keepdims=True)
    mid_scale = lax.rsqrt(sq_mid / D + EPSILON)
    lane = iota((rows_half, 128), 1)

    def hidden_of(parts):
        wide = jnp.concatenate(parts, axis=1) * mid_scale
        pieces = []
        for at in range(0, 2 * piece, 256):
            a, b = [
                wide[:, to : to + 128] if to < wide.shape[1] else jnp.zeros((rows_half, 128), F32)
                for to in (at, at + 128)
            ]
            gate = jnp.where(lane < STRIP, a, pltpu.roll(b, STRIP, 1))
            up = jnp.where(lane < STRIP, pltpu.roll(a, STRIP, 1), b)
            pieces.append(gate / (1.0 + jnp.exp(-gate)) * up)
        return jnp.concatenate(pieces, axis=1).astype(BF16)

    def hid_piece(k):
        return lambda q, r: hid_all.at[r, q, :, k * piece : (k + 1) * piece]

    def hid_start(k):
        lanes = slice(k * piece, (k + 1) * piece)
        hid_all[role, chip, :, lanes] = hidden_of([gu_total(2 * k), gu_total(2 * k + 1)])
        phase(f"hid_send{k}")
        gather_start(k, hid_piece(k))

    def hid_finish(k):
        lanes = slice(k * piece, (k + 1) * piece)
        gather_finish(
            k,
            hid_all.at[role, 0:3, :, lanes],
            hid_all.at[role, :, :, lanes],
            hid_all.at[other_role, :, :, lanes],
        )

    def hid_rows(k, r, yy):
        lanes = slice(k * piece, (k + 1) * piece)
        return jnp.concatenate(
            [hid_all[r, 2 * yy + xx, :, lanes].astype(F32) for xx in range(2)], axis=0
        ).astype(BF16)

    def down_rows(k, r, yy, count):
        return w_down[pl.ds((4 * k + 2 * r + yy) * piece, count * piece), :]

    for k in range(PIECES):
        hid_start(k)
    phase("down_loads")
    drain(wd_hbm, load_sem.at[6])
    part = None
    for k in range(PIECES):
        phase(f"hid_pass{k}")
        gather_pass(k, hid_piece(k))
        phase(f"down_own{k}")
        own_part = dot(hid_rows(k, role, y), down_rows(k, role, y, 1))
        part = own_part if part is None else part + own_part
    for k in range(PIECES):
        hid_finish(k)
        phase(f"down{k}")
        part = part + dot(hid_rows(k, role, 1 - y), down_rows(k, role, 1 - y, 1))
        other_rows = jnp.concatenate([hid_rows(k, other_role, yy) for yy in range(2)], axis=1)
        part = part + dot(other_rows, down_rows(k, other_role, 0, 2))
    tp_scatter_start(7, part, down_part, down_recv, every)
    phase("drains")
    drain(gu_near, qkv_out_sem.at[0])
    drain(gu_last, qkv_out_sem.at[1])
    drain(w_qkv.at[1], pair_out.at[1])
    drain(tok_all.at[0], pair_out.at[2])
    drain(tok_all.at[0:rest], pair_out.at[7])
    drain(state_far, pair_out.at[3])
    drain(w_gu.at[1], pair_out.at[4])
    drain(state_far, pair_out.at[5])
    drain(state_back, pair_in.at[5])
    drain(mid_all.at[0], pair_out.at[6])
    drain(mid_all.at[0:rest], pair_out.at[8])
    phase("down_wait")
    total = tp_scatter_finish(7, down_part, down_recv, every)
    phase("result")
    result = (mid_all[tp].astype(F32) + total).astype(BF16)
    mixed_ref[...] = lax.dot_general(
        picker, result, (((0,), (0,)), ((), ())), preferred_element_type=F32
    ).astype(BF16)
    phase(None)


def fused_layer(n_kv, n_tp, *args):
    tokens, lengths, state, attn_gain, w_query = args[:5]
    w_beta, w_out, w_gate = args[7], args[12], args[14]
    batch, span, own_cols = tokens.shape
    seqs, size, vw = state.shape
    heads = vw // size
    width = attn_gain.shape[0]
    ff = w_gate.shape[1]
    pack = min(batch * 7 // 4, batch * span)
    packs = (pack + 15) // 16 * 16
    half = batch // 2
    cap = (min(half * span, pack - half) + 15) // 16 * 16
    local = 2 * seqs * span
    chips = n_kv // 2
    strips = ff // STRIP
    per = (strips + 3) // 4
    sizes = strip_groups(per)
    piece = piece_width(sizes)
    qkv_width = 128 + 3 * vw // 2
    rows_half = packs // 2
    strip_width = per * 128
    dims = (n_kv, n_tp, batch, span, seqs, heads, size, width, ff, packs, cap)
    operands = list(args)
    operands[0] = tokens.reshape(batch * span, own_cols)
    for at in (1, 3, 9, 10, 11, 13):
        operands[at] = operands[at].reshape(1, -1)
    for at in (7, 8):
        operands[at] = operands[at].T
    for at in (14, 15):
        operands[at] = operands[at].T.reshape(strips, STRIP, width)
    in_vmem = pl.BlockSpec(memory_space=pltpu.VMEM)
    in_hbm = pl.BlockSpec(memory_space=pltpu.HBM)
    dma = pltpu.SemaphoreType.DMA

    def buf(*shape):
        return pltpu.VMEM(shape, BF16)

    half_state = (seqs, size, vw // 2)
    mixed, keep, back = pl.pallas_call(
        lambda *refs: layer_kernel(dims, *refs),
        out_shape=(
            pltpu.VMEM((batch * span, own_cols), BF16),
            pltpu.VMEM(half_state, F32),
            pltpu.VMEM(half_state, F32),
        ),
        in_specs=[in_hbm] * len(operands),
        out_specs=(in_vmem, in_vmem, in_vmem),
        scratch_shapes=[
            pltpu.VMEM(half_state, F32),
            buf(batch * span, own_cols),
            pltpu.VMEM((1, batch), jnp.int32),
            pltpu.VMEM((1, width), F32),
            pltpu.VMEM((1, args[9].shape[0]), F32),
            pltpu.VMEM((1, args[10].shape[0]), F32),
            pltpu.VMEM((1, size), F32),
            pltpu.VMEM((1, width), F32),
            buf(2, 3, width, vw // 2),
            buf(w_beta.shape[1], 2 * width),
            buf(w_beta.shape[1], 2 * width),
            buf(*w_out.shape),
            buf(2, 2 * per, 2, STRIP, width),
            buf(4 * PIECES * piece, w_out.shape[1]),
            buf(n_tp, packs, own_cols),
            buf(n_tp, packs, own_cols),
            pltpu.VMEM((2, 1, width), F32),
            pltpu.VMEM((packs, 3 * vw // 2), F32),
            buf(packs, qkv_width),
            buf(cap, qkv_width),
            buf(cap, qkv_width),
            buf(local, qkv_width),
            buf(local, qkv_width),
            buf(chips, local, vw),
            buf(n_tp, packs, own_cols),
            buf(n_tp - 1, packs, own_cols),
            buf(n_tp, packs, own_cols),
            buf(n_tp, packs, own_cols),
            pltpu.VMEM((n_kv, 1, 128), F32),
            pltpu.VMEM((2, 2, rows_half, strip_width), F32),
            buf(2, rows_half, strip_width),
            buf(2, rows_half, strip_width),
            buf(rows_half, strip_width),
            buf(rows_half, strip_width),
            buf(2, chips, rows_half, PIECES * piece),
            buf(n_tp, packs, own_cols),
            buf(n_tp - 1, packs, own_cols),
            dma((7,)),
            dma((7,)),
            dma((9,)),
            dma((9,)),
            dma((8,)),
            dma((8,)),
            dma((2,)),
            dma((2, GROUPS)),
            dma((PIECES,)),
            dma((PIECES, 3)),
            dma((PIECES,)),
            dma((PIECES,)),
            dma((2,)),
        ],
        compiler_params=pltpu.CompilerParams(
            collective_id=0, has_side_effects=True, vmem_limit_bytes=52 * 1024 * 1024
        ),
    )(*operands)
    return pl.pallas_call(
        finish_kernel,
        out_shape=(
            jax.ShapeDtypeStruct(tokens.shape, BF16),
            jax.ShapeDtypeStruct(state.shape, F32),
        ),
        in_specs=[in_vmem, in_vmem, in_vmem],
        out_specs=(in_hbm, in_hbm),
        scratch_shapes=[pltpu.VMEM(tokens.shape, BF16), dma((9,))],
        compiler_params=pltpu.CompilerParams(vmem_limit_bytes=4 * 1024 * 1024),
    )(mixed, keep, back)


def finish_kernel(mixed_ref, keep_ref, back_ref, mixed_out, state_out, mixed_rows, write_sem):
    kv = lax.axis_index("kv")
    role = role_of(lax.rem(kv, 2), kv // 2)
    seqs, _, half = keep_ref.shape
    writes = []
    for i, (ref, at) in enumerate(((keep_ref, role), (back_ref, 1 - role))):
        lanes = pl.ds(pl.multiple_of(at * half, half), half)
        for j in range(4):
            rows = slice(j * seqs // 4, (j + 1) * seqs // 4)
            writes.append(
                pltpu.make_async_copy(
                    ref.at[rows], state_out.at[rows, :, lanes], write_sem.at[4 * i + j]
                )
            )
    for write in writes:
        write.start()
    mixed_rows[...] = mixed_ref[...].astype(F32).reshape(mixed_rows.shape).astype(BF16)
    writes.append(pltpu.make_async_copy(mixed_rows, mixed_out, write_sem.at[8]))
    writes[-1].start()
    for write in writes:
        write.wait()


def layer(*args):
    n_kv, n_tp = lax.axis_size("kv"), lax.axis_size("tp")
    tokens, state, w_gate = args[0], args[2], args[14]
    batch, span, own_cols = tokens.shape
    seqs, size, vw = state.shape
    pack = min(batch * 7 // 4, batch * span)
    aligned = own_cols % 128 == 0 and size % 128 == 0 and seqs == 8
    aligned = aligned and n_kv == 8 and n_tp == 4 and 2 * args[7].shape[1] + 2 <= 128
    aligned = aligned and pack % 16 == 0 and pack <= 128 and vw == 8 * size
    aligned = aligned and w_gate.shape[1] % STRIP == 0
    if aligned:
        return fused_layer(n_kv, n_tp, *args)
    return body(*args)


def solution(mesh):
    return jax.shard_map(
        layer,
        mesh=mesh,
        in_specs=(
            P(None, None, ("kv", "tp")),
            P(),
            P("kv", None, "tp"),
            P("kv"),
            P("kv", "tp"),
            P("kv", "tp"),
            P("kv", "tp"),
            P(),
            P(),
            P(),
            P(),
            P(),
            P("tp", "kv"),
            P("kv"),
            P("kv", "tp"),
            P("kv", "tp"),
            P("tp", "kv"),
        ),
        out_specs=(P(None, None, ("kv", "tp")), P("kv", None, "tp")),
        check_vma=False,
    )
```
